512 devices in a mesh: sp: 128 (over z, x, core), tp: 4 (over y).
Axes of the slice: x: 4, y: 4, z: 16, core: 2. Of those that a mesh axis runs over, the one named last changes fastest.
Arguments:
- stream: bfloat16 [16384, 2048], P('sp', 'tp')
- norm_gain: float32 [2048], P('tp'), may hold values from 0.1 to 1.9
- w_value: bfloat16 [2048, 512], P(None, 'tp'), may hold values from -0.125 to 0.125
- w_mix: bfloat16 [2048, 512], P(None, 'tp'), may hold values from -0.125 to 0.125
- w_gate: bfloat16 [2048, 512], P(None, 'tp'), may hold values from -0.125 to 0.125
- w_state: bfloat16 [2048, 512], P(None, 'tp'), may hold values from -0.125 to 0.125
- conv_taps: float32 [3, 512], P(None, 'tp'), may hold values from -3 to 3
- skip_gain: float32 [512], P('tp'), may hold values from -3 to 3
- decay_rate: float32 [2, 32, 64], P(None, 'tp'), as said below
- turn_rate: float32 [2, 32, 64], P(None, 'tp'), may hold values from 0.25 to 1.5
- input_real: float32 [2, 32, 64, 16], P(None, 'tp')
- input_imag: float32 [2, 32, 64, 16], P(None, 'tp')
- read_real: float32 [2, 32, 16, 64], P(None, 'tp'), may hold values from -0.75 to 0.75
- read_imag: float32 [2, 32, 16, 64], P(None, 'tp'), may hold values from -0.75 to 0.75
- initial_state: float32 [2, 2, 32, 64], P(None, None, 'tp'), may hold values from -5 to 5
- intervals: float32 [16384], P('sp'), as said below
- proj_conv: bfloat16 [512, 2048], P('tp'), may hold values from -0.1875 to 0.1875
- proj_state: bfloat16 [512, 2048], P('tp'), may hold values from -0.1875 to 0.1875
Outputs:
- mixed: bfloat16 [16384, 2048], P('sp', 'tp')
The draws below stay inside these ranges and needn't reach their ends.
Inputs may be any that keep to these rules, and one draw needn't show every extreme that they name: `decay_rate`: Positive. `intervals`: Positive.
All inputs are finite; a program needn't handle non-finite values.
Results may differ from the reference program's by a relative error of at most 0.024.
Values may be sent and summed in bfloat16 or wider, within the bound.
No kernel may reach another device: no remote copies, remote signals or barrier semaphores. Data moves between devices by JAX's collectives and lax.ppermute only.
A program may use at most 64 MiB of HBM per device.

```python
import math
import jax
import jax.numpy as jnp
from jax import lax

D = 2048
CONV_W = 512
SSM_W = 512
GSIZE = 16
STATE = 64
MIXER_GROUPS = 32
TOK_DEV = 128
TOKEN_COUNT = 16384
N_TP = 4


def rate_table(key):
    slow_share = 0.5
    slow_flags = jax.random.uniform(jax.random.fold_in(key, 101), (2, MIXER_GROUPS, 1)) < slow_share
    quantile = jax.random.uniform(jax.random.fold_in(key, 102), (2, MIXER_GROUPS, STATE))
    slow_rates = jnp.exp(math.log(0.4) + quantile * math.log(0.9 / 0.4)) / TOKEN_COUNT
    fast_rates = jnp.exp(math.log(0.01) + quantile * math.log(1.0 / 30.0 / 0.01))
    return jnp.where(slow_flags, slow_rates, fast_rates).astype(jnp.float32)


def driven_matrix(key, salt):
    decay_rates = rate_table(key)
    normal_part = jnp.clip(jax.random.normal(jax.random.fold_in(key, salt), (2, MIXER_GROUPS, STATE, GSIZE)), -5.0, 5.0)
    return (normal_part * jnp.sqrt(decay_rates / GSIZE)[..., None]).astype(jnp.float32)


def draw_decay_rate(key, part):
    return rate_table(key)


def draw_input_real(key, part):
    return driven_matrix(key, 103)


def draw_input_imag(key, part):
    return driven_matrix(key, 104)


def draw_intervals(key, part):
    blocks = TOKEN_COUNT // TOK_DEV
    factor = jnp.exp(jax.random.uniform(jax.random.fold_in(key, 1), (blocks, 1), minval=math.log(0.5), maxval=math.log(2.0)))
    jitter = jax.random.uniform(jax.random.fold_in(key, 2), (blocks, TOK_DEV), minval=0.5, maxval=1.5)
    evenly_spaced = (factor * jitter).reshape(TOKEN_COUNT)
    spike_locations = jax.random.randint(jax.random.fold_in(key, 3), (2,), 0, TOKEN_COUNT)
    slot_indices = jnp.arange(TOKEN_COUNT)
    spike_mask = (slot_indices == spike_locations[0]) | (slot_indices == spike_locations[1])
    return jnp.where(spike_mask, 0.5 * TOKEN_COUNT, evenly_spaced).astype(jnp.float32)


def draw_stream(key, part):
    normal_part = jnp.clip(jax.random.normal(jax.random.fold_in(key, 11), (TOKEN_COUNT, D)), -5.0, 5.0)
    rise = 3.0
    row_scale = jnp.exp(jax.random.uniform(jax.random.fold_in(key, 12), (TOKEN_COUNT, 1), minval=math.log(0.3), maxval=math.log(3.0)))
    column_scale = jnp.exp(jax.random.uniform(jax.random.fold_in(key, 13), (1, D), minval=math.log(0.5), maxval=math.log(1.6)))
    column_block = (jnp.arange(D) // (D // N_TP)).astype(jnp.float32)
    trend = rise ** (column_block / max(N_TP - 1, 1))
    return (normal_part * row_scale * column_scale * trend[None, :]).astype(jnp.bfloat16)


def steps_of(key, extent, split, least, top_value):
    gain, own = 1.0, jax.random.fold_in(key, 6)
    for axis_at, parts in split:
        steps = jnp.exp(jax.random.uniform(jax.random.fold_in(own, axis_at), (parts,), jnp.float32, least / len(split), top_value / len(split)))
        gain = gain * jnp.repeat(steps, extent[axis_at] // parts).reshape([-1 if axis == axis_at else 1 for axis in range(len(extent))])
    return gain


def noise(key, shape, deviation, most, shards=(), held_as=jnp.bfloat16):
    loudness = steps_of(key, shape, shards, -0.22, 0.18) if shards else 1.0
    drawn = jax.random.normal(key, shape, jnp.float32) * deviation * loudness
    return jnp.minimum(jnp.maximum(drawn, -most), most).astype(held_as)


def setup_inputs(seed: int = 0) -> dict:
    keys = jax.random.split(jax.random.key(seed), 19)
    return {
        "stream": draw_stream(jax.random.fold_in(keys[18], 71), 0),
        "norm_gain": jnp.clip(1.0 + 0.18 * jax.random.normal(keys[1], (D,), jnp.float32), 0.1, 1.9),
        "w_value": noise(keys[2], (D, CONV_W), D ** -0.5, 0.125, ((1, 4),)),
        "w_mix": noise(keys[3], (D, CONV_W), D ** -0.5, 0.125, ((1, 4),)),
        "w_gate": noise(keys[4], (D, CONV_W), D ** -0.5, 0.125, ((1, 4),)),
        "w_state": noise(keys[5], (D, SSM_W), D ** -0.5, 0.125, ((1, 4),)),
        "conv_taps": noise(keys[6], (3, CONV_W), 0.5, 3.0, ((1, 4),), jnp.float32),
        "skip_gain": noise(keys[7], (SSM_W,), 0.5, 3.0, ((0, 4),), jnp.float32),
        "decay_rate": draw_decay_rate(jax.random.fold_in(keys[18], 71), 0),
        "turn_rate": jnp.clip(0.25 + 1.25 * jax.random.uniform(keys[9], (2, MIXER_GROUPS, STATE), jnp.float32) ** steps_of(keys[9], (2, MIXER_GROUPS, STATE), ((1, 4),), -0.2, 0.2), 0.25, 1.5),
        "input_real": draw_input_real(jax.random.fold_in(keys[18], 71), 0),
        "input_imag": draw_input_imag(jax.random.fold_in(keys[18], 71), 0),
        "read_real": noise(keys[12], (2, MIXER_GROUPS, GSIZE, STATE), STATE ** -0.5, 0.75, ((1, 4),), jnp.float32),
        "read_imag": noise(keys[13], (2, MIXER_GROUPS, GSIZE, STATE), STATE ** -0.5, 0.75, ((1, 4),), jnp.float32),
        "initial_state": noise(keys[14], (2, 2, MIXER_GROUPS, STATE), 1.0, 5.0, ((2, 4),), jnp.float32),
        "intervals": draw_intervals(jax.random.fold_in(keys[18], 71), 0),
        "proj_conv": noise(keys[16], (CONV_W, D), (CONV_W + SSM_W) ** -0.5, 0.1875, ((0, 4),)),
        "proj_state": noise(keys[17], (SSM_W, D), (CONV_W + SSM_W) ** -0.5, 0.1875, ((0, 4),)),
    }


EPSILON = 1e-06
HIGH = lax.Precision.HIGHEST

def step_factors(decay_rate, turn_rate, interval):
    damping = -decay_rate * interval
    angle = turn_rate * interval
    magnitude = jnp.exp(damping)
    factor_re = magnitude * jnp.cos(angle)
    factor_im = magnitude * jnp.sin(angle)
    half_sine = jnp.sin(0.5 * angle)
    lift_re = jnp.expm1(damping) * jnp.cos(angle) - 2.0 * half_sine * half_sine
    denominator = decay_rate * decay_rate + turn_rate * turn_rate
    gain_real = (turn_rate * factor_im - decay_rate * lift_re) / denominator
    gain_im = -(decay_rate * factor_im + turn_rate * lift_re) / denominator
    return (factor_re, factor_im, gain_real, gain_im)

def state_direction(inputs, intervals, decay_rate, turn_rate, input_real, input_imag, read_real, read_imag, start_re, start_im, backward):
    block_count = TOKEN_COUNT // TOK_DEV
    input_blocks = inputs.reshape(block_count, TOK_DEV, MIXER_GROUPS, GSIZE)
    interval_blocks = intervals.reshape(block_count, TOK_DEV)

    def advance_block(boundary, block_items):
        block_inputs, block_steps = block_items
        factor_re, factor_im, gain_real, gain_im = step_factors(decay_rate, turn_rate, block_steps[:, None, None])
        driven_re = jnp.einsum('tgh,gph->tgp', block_inputs, input_real, precision=HIGH)
        driven_im = jnp.einsum('tgh,gph->tgp', block_inputs, input_imag, precision=HIGH)
        push_re = gain_real * driven_re - gain_im * driven_im
        push_im = gain_real * driven_im + gain_im * driven_re

        def advance_position(current, step_items):
            step_re, step_im, add_re, add_im = step_items
            new_re = step_re * current[0] - step_im * current[1] + add_re
            new_im = step_re * current[1] + step_im * current[0] + add_im
            return ((new_re, new_im), (new_re, new_im))
        boundary, history = lax.scan(advance_position, boundary, (factor_re, factor_im, push_re, push_im), reverse=backward)
        reading = jnp.einsum('ghp,tgp->tgh', read_real, history[0], precision=HIGH)
        reading = reading - jnp.einsum('ghp,tgp->tgh', read_imag, history[1], precision=HIGH)
        return (boundary, reading)
    _, readings = lax.scan(advance_block, (start_re, start_im), (input_blocks, interval_blocks), reverse=backward)
    return readings.reshape(TOKEN_COUNT, MIXER_GROUPS, GSIZE)

def reference(stream, norm_gain, w_value, w_mix, w_gate, w_state, conv_taps, skip_gain, decay_rate, turn_rate, input_real, input_imag, read_real, read_imag, initial_state, intervals, proj_conv, proj_state):
    widened = stream.astype(jnp.float32)
    inv_rms = lax.rsqrt(lax.optimization_barrier(jnp.mean(widened * widened, axis=1, keepdims=True)) + EPSILON)
    normed = (widened * inv_rms * norm_gain).astype(jnp.bfloat16)
    conv_value = jnp.dot(normed, w_value, preferred_element_type=jnp.float32).astype(jnp.bfloat16)
    conv_mix = jnp.dot(normed, w_mix, preferred_element_type=jnp.float32).astype(jnp.bfloat16)
    conv_gate = jnp.dot(normed, w_gate, preferred_element_type=jnp.float32).astype(jnp.bfloat16)
    state_input = jnp.dot(normed, w_state, preferred_element_type=jnp.float32).astype(jnp.bfloat16)
    source = (conv_mix.astype(jnp.float32) * conv_value.astype(jnp.float32)).astype(jnp.bfloat16)
    padded = jnp.pad(source.astype(jnp.float32), ((1, 1), (0, 0)))
    filtered = conv_taps[0] * padded[:-2] + conv_taps[1] * padded[1:-1] + conv_taps[2] * padded[2:]
    conv_out = (conv_gate.astype(jnp.float32) * filtered).astype(jnp.bfloat16)
    state_float = state_input.astype(jnp.float32).reshape(TOKEN_COUNT, MIXER_GROUPS, GSIZE)
    responses = skip_gain.reshape(MIXER_GROUPS, GSIZE) * state_float
    for direction in range(2):
        responses = responses + state_direction(state_float, intervals, decay_rate[direction], turn_rate[direction], input_real[direction], input_imag[direction], read_real[direction], read_imag[direction], initial_state[direction, 0], initial_state[direction, 1], direction == 1)
    state_out = jax.nn.gelu(responses.reshape(TOKEN_COUNT, SSM_W)).astype(jnp.bfloat16)
    total = jnp.dot(conv_out, proj_conv, preferred_element_type=jnp.float32)
    total = total + jnp.dot(state_out, proj_state, preferred_element_type=jnp.float32)
    return total.astype(jnp.bfloat16)
```

```python
import jax
import jax.numpy as jnp
from jax import lax
from jax.experimental import pallas as pl
from jax.experimental.pallas import tpu as pltpu
from jax.sharding import Mesh
from jax.sharding import PartitionSpec as P

D = 2048
SP = ("sp_0", "sp_1", "sp_2")
EPSILON = 1e-06
F32 = jnp.float32
BF16 = jnp.bfloat16
CHUNKS = 8


def sin_cos(angle):
    turns = jnp.floor(angle * 0.6366197723675814 + 0.5)
    rest = ((angle - turns * 1.5703125) - turns * 4.837512969970703125e-4) - turns * 7.54978995489188216e-8
    rest = jnp.clip(rest, -0.8, 0.8)
    square = rest * rest
    sine = rest + rest * square * (
        -1.6666654611e-1 + square * (8.3321608736e-3 - 1.9515295891e-4 * square)
    )
    cosine = 1.0 - 0.5 * square + square * square * (
        4.166664568298827e-2 + square * (-1.388731625493765e-3 + 2.443315711809948e-5 * square)
    )
    quadrant = turns.astype(jnp.int32)
    odd = (quadrant & 1) == 1
    s = jnp.where(odd, cosine, sine)
    c = jnp.where(odd, sine, cosine)
    s = jnp.where((quadrant & 2) == 2, -s, s)
    c = jnp.where(((quadrant + 1) & 2) == 2, -c, c)
    return s, c


def exp_less_one(x):
    series = x * (1.0 + x * (1 / 2 + x * (1 / 6 + x * (1 / 24 + x * (1 / 120 + x * (1 / 720 + x * (1 / 5040 + x * (1 / 40320))))))))
    return jnp.where(x > -0.5, series, jnp.exp(x) - 1.0)


def moved(elapsed, decay, turn):
    magnitude = jnp.exp(-decay * elapsed)
    s, c = sin_cos(turn * elapsed)
    return magnitude * c, magnitude * s


def cmul(ar, ai, br, bi):
    return ar * br - ai * bi, ar * bi + ai * br


def iota(shape, dim):
    return lax.broadcasted_iota(jnp.int32, shape, dim)


def dot(a, b, dims=((1,), (0,))):
    return lax.dot_general(a, b, (dims, ((), ())), preferred_element_type=F32)


def halves(x):
    high = x.astype(BF16)
    return high, (x - high.astype(F32)).astype(BF16)


def scan_chunks(fr, fi, lr, li, backward):
    rows = iota(fr.shape, 0)
    for k in (1, 2, 4):
        shift = CHUNKS - k if backward else k
        outside = rows >= CHUNKS - k if backward else rows < k
        sfr = jnp.where(outside, 1.0, pltpu.roll(fr, shift, 0))
        sfi = jnp.where(outside, 0.0, pltpu.roll(fi, shift, 0))
        if lr is not None:
            slr = jnp.where(outside, 0.0, pltpu.roll(lr, shift, 0))
            sli = jnp.where(outside, 0.0, pltpu.roll(li, shift, 0))
            ar, ai = cmul(fr, fi, slr, sli)
            lr, li = lr + ar, li + ai
        fr, fi = cmul(fr, fi, sfr, sfi)
    return fr, fi, lr, li


def one_later(x, backward, fill):
    rows = iota(x.shape, 0)
    if backward:
        return jnp.where(rows == CHUNKS - 1, fill, pltpu.roll(x, CHUNKS - 1, 0))
    return jnp.where(rows == 0, fill, pltpu.roll(x, 1, 0))


def pack_kernel(stream, gain, out):
    n = stream.shape[0]
    per = n // CHUNKS
    row, col = iota((n, n), 0), iota((n, n), 1)
    order = jnp.where(col == (row % CHUNKS) * per + row // CHUNKS, 1.0, 0.0).astype(BF16)
    x = dot(order, stream[...]).astype(BF16)
    g = gain[...]
    high = g.astype(BF16)
    left = g - high.astype(F32)
    mid = left.astype(BF16)
    low = (left - mid.astype(F32)).astype(BF16)
    row = iota((16, g.shape[1]), 0)
    tail = jnp.where(row == 0, high.astype(F32), jnp.where(row == 1, mid.astype(F32), jnp.where(row == 2, low.astype(F32), 0.0)))
    tail = tail.astype(BF16)
    for k in range(out.shape[0]):
        out[k, 0:n, :] = x
        out[k, n : n + 16, :] = tail


def prepare_kernel(intervals, decay, turn, in_re, in_im, rd_re, rd_im, fr_o, fi_o, gr_o, gi_o, pr_o, pi_o, br_o, bi_o, in_hi, in_lo, rd_hi, rd_lo, total):
    n = intervals.shape[1]
    per = n // CHUNKS
    row, col = iota((n, n), 0), iota((n, n), 1)
    steps = jnp.sum(jnp.where(col == (row % CHUNKS) * per + row // CHUNKS, intervals[...], 0.0), axis=1, keepdims=True)
    total[...] = jnp.broadcast_to(jnp.sum(intervals[...], axis=1, keepdims=True), total.shape)
    width = decay.shape[1]
    half = width // 2
    for tile in range(width // 128):
        lanes = slice(tile * 128, tile * 128 + 128)
        rate, turning = decay[:, lanes], turn[:, lanes]
        damping = -rate * steps
        s, c = sin_cos(0.5 * (turning * steps))
        magnitude = jnp.exp(damping)
        twice = 2.0 * s * s
        cosine = 1.0 - twice
        fr = magnitude * cosine
        fi = magnitude * (2.0 * s * c)
        lift = exp_less_one(damping) * cosine - twice
        inverse = 1.0 / (rate * rate + turning * turning)
        fr_o[:, lanes] = fr
        fi_o[:, lanes] = fi
        gr_o[:, lanes] = (turning * fi - rate * lift) * inverse
        gi_o[:, lanes] = -(rate * fi + turning * lift) * inverse
        backward = tile * 128 >= half
        cr = ci = None
        for i in reversed(range(per)) if backward else range(per):
            at = slice(i * CHUNKS, i * CHUNKS + CHUNKS)
            r, m = fr[at], fi[at]
            cr, ci = (r, m) if cr is None else cmul(r, m, cr, ci)
            pr_o[at, lanes] = cr
            pi_o[at, lanes] = ci
        br, bi, _, _ = scan_chunks(cr, ci, None, None, backward)
        br_o[:, lanes] = one_later(br, backward, 1.0)
        bi_o[:, lanes] = one_later(bi, backward, 0.0)
    channels = rd_re.shape[0] // 2
    groups = half // rd_re.shape[1]
    wide = channels // groups
    states = rd_re.shape[1]
    spread = jnp.where(iota((wide, channels), 1) % wide == iota((wide, channels), 0), 1.0, 0.0).astype(BF16)
    mine = iota((channels, width), 0) // wide == (iota((channels, width), 1) % half) // states
    for at, ref in enumerate((in_re, in_im)):
        for piece, out in zip(halves(ref[...]), (in_hi, in_lo)):
            full = dot(spread, piece, ((0,), (1,)))
            out[:, at * width : (at + 1) * width] = jnp.where(mine, full, 0.0).astype(BF16)
    spread = jnp.where(iota((states, half), 1) % states == iota((states, half), 0), 1.0, 0.0).astype(BF16)
    mine = iota((half, channels), 0) // states == iota((half, channels), 1) // wide
    for at, ref in enumerate((rd_re, rd_im)):
        for d in range(2):
            both = ref[d * channels : (d + 1) * channels, :]
            both = -both if at == 1 else both
            for piece, out in zip(halves(both), (rd_hi, rd_lo)):
                full = dot(spread, piece, ((0,), (1,)))
                place = at * width + d * half
                out[place : place + half, :] = jnp.where(mine, full, 0.0).astype(BF16)


def local_kernel(rows, w_value, w_mix, w_gate, w_state, fr, fi, gr, gi, pr, pi, in_hi, in_lo, total, hr_o, hi_o, cr_o, ci_o, source_o, gate_o, input_o, message):
    parts, n, share = rows.shape[0], rows.shape[1] - 16, rows.shape[2]
    per = n // CHUNKS
    squares = 0.0
    for k in range(parts):
        x = rows[k, 0:n, :].astype(F32)
        squares = squares + jnp.sum(x * x, axis=1, keepdims=True)
    inv_rms = lax.rsqrt(squares / D + EPSILON)
    value = mix = gate = state = 0.0
    for k in range(parts):
        tail = rows[k, n : n + 16, :].astype(F32)
        gain = (tail[0:1] + tail[1:2]) + tail[2:3]
        normed = ((rows[k, 0:n, :].astype(F32) * inv_rms) * gain).astype(BF16)
        at = slice(k * share, k * share + share)
        value = value + dot(normed, w_value[at, :])
        mix = mix + dot(normed, w_mix[at, :])
        gate = gate + dot(normed, w_gate[at, :])
        state = state + dot(normed, w_state[at, :])
    source = (mix.astype(BF16).astype(F32) * value.astype(BF16).astype(F32)).astype(BF16).astype(F32)
    source_o[...] = source
    gate_o[...] = gate.astype(BF16).astype(F32)
    state = state.astype(BF16)
    input_o[...] = state.astype(F32)
    width = fr.shape[1]
    half = width // 2
    edges = []
    for tile in range(width // 128):
        lanes = slice(tile * 128, tile * 128 + 128)
        other = slice(width + tile * 128, width + tile * 128 + 128)
        driven_re = dot(state, in_hi[:, lanes]) + dot(state, in_lo[:, lanes])
        driven_im = dot(state, in_hi[:, other]) + dot(state, in_lo[:, other])
        push_re, push_im = cmul(gr[:, lanes], gi[:, lanes], driven_re, driven_im)
        backward = tile * 128 >= half
        hr = hi = None
        for i in reversed(range(per)) if backward else range(per):
            at = slice(i * CHUNKS, i * CHUNKS + CHUNKS)
            if hr is None:
                hr, hi = push_re[at], push_im[at]
            else:
                ar, ai = cmul(fr[at, lanes], fi[at, lanes], hr, hi)
                hr, hi = ar + push_re[at], ai + push_im[at]
            hr_o[at, lanes] = hr
            hi_o[at, lanes] = hi
        end = slice(0, CHUNKS) if backward else slice(n - CHUNKS, n)
        _, _, lr, li = scan_chunks(pr[end, lanes], pi[end, lanes], hr, hi, backward)
        cr_o[:, lanes] = one_later(lr, backward, 0.0)
        ci_o[:, lanes] = one_later(li, backward, 0.0)
        edge = 0 if backward else CHUNKS - 1
        edges.append((lr[edge : edge + 1], li[edge : edge + 1]))
    for k in range(message.shape[0]):
        for tile, (r, m) in enumerate(edges):
            message[k, tile : tile + 1, :] = r
            message[k, 8 + tile : 9 + tile, :] = m
        message[k, 16:17, :] = total[0:1, :]
        message[k, 17:18, :] = source[0:1]
        message[k, 18:19, :] = source[n - 1 : n]
        message[k, 19:24, :] = jnp.zeros((5, 128), F32)


def plane_kernel(place, got, decay, turn, inner, message):
    size = got.shape[0]
    here, plane = place[0], place[1]
    rate, turning = decay[...], turn[...]
    forward = iota((8, 128), 0) < 4
    hr = hi = spent = jnp.zeros((8, 128), F32)
    ir = ii = before = hr
    for k in range(size):
        m = size - 1 - k
        mine = (forward & (here == k)) | (jnp.logical_not(forward) & (here == m))
        ir = jnp.where(mine, hr, ir)
        ii = jnp.where(mine, hi, ii)
        before = jnp.where(mine, spent, before)
        elapsed = jnp.where(forward, got[k, 16:17, :], got[m, 16:17, :])
        ar, ai = moved(elapsed, rate, turning)
        ar, ai = cmul(ar, ai, hr, hi)
        hr = ar + jnp.where(forward, got[k, 0:8, :], got[m, 0:8, :])
        hi = ai + jnp.where(forward, got[k, 8:16, :], got[m, 8:16, :])
        spent = spent + elapsed
    wr, wi = moved(before, rate, turning)
    inner[0:8, :] = ir
    inner[8:16, :] = ii
    inner[16:24, :] = wr
    inner[24:32, :] = wi
    previous = following = jnp.zeros((1, 128), F32)
    for k in range(size):
        previous = jnp.where(here - 1 == k, got[k, 18:19, :], previous)
        following = jnp.where(here + 1 == k, got[k, 17:18, :], following)
    inner[32:40, :] = jnp.broadcast_to(previous, (8, 128))
    inner[40:48, :] = jnp.broadcast_to(following, (8, 128))
    swapped = pltpu.roll(hi, 4, 0)
    later = jnp.where(forward, hr, swapped)
    earlier = jnp.where(forward, swapped, hr)
    row = iota((8, 128), 0)
    note_later = jnp.where(row == 0, spent, jnp.where(row == 1, got[size - 1, 18:19, :], 0.0))
    note_earlier = jnp.where(row == 0, spent, jnp.where(row == 1, got[0, 17:18, :], 0.0))
    for k in range(message.shape[0]):
        message[k, 0:8, :] = jnp.where(plane < k, later, earlier)
        message[k, 8:16, :] = jnp.where(plane < k, note_later, note_earlier)


def finish_kernel(place, got, inner, decay, turn, init_re, init_im, hr_i, hi_i, cr_i, ci_i, pr, pi, br, bi, rd_hi, rd_lo, source, gate, state, taps, skip, proj_conv, proj_state, out):
    size = got.shape[0]
    here, plane, last = place[0], place[1], place[2]
    rate, turning = decay[...], turn[...]
    forward = iota((8, 128), 0) < 4
    hr, hi = init_re[...], init_im[...]
    for k in range(size):
        m = size - 1 - k
        active = (forward & (plane > k)) | (jnp.logical_not(forward) & (plane < m))
        elapsed = jnp.where(forward, got[k, 8:9, :], got[m, 8:9, :])
        ar, ai = moved(elapsed, rate, turning)
        ar, ai = cmul(ar, ai, hr, hi)
        a, b = got[k, 0:8, :], got[m, 0:8, :]
        hr = jnp.where(active, ar + jnp.where(forward, a, b), hr)
        hi = jnp.where(active, ai + pltpu.roll(jnp.where(forward, b, a), 4, 0), hi)
    ar, ai = cmul(inner[16:24, :], inner[24:32, :], hr, hi)
    inc_re = ar + inner[0:8, :]
    inc_im = ai + inner[8:16, :]
    n, width = hr_i.shape
    per = n // CHUNKS
    response = state[...] * skip[...]
    for tile in range(width // 128):
        lanes = slice(tile * 128, tile * 128 + 128)
        er, ei = cmul(br[:, lanes], bi[:, lanes], inc_re[tile : tile + 1], inc_im[tile : tile + 1])
        er = er + cr_i[:, lanes]
        ei = ei + ci_i[:, lanes]
        er = jnp.concatenate([er] * per, axis=0)
        ei = jnp.concatenate([ei] * per, axis=0)
        ar, ai = cmul(pr[:, lanes], pi[:, lanes], er, ei)
        full = jnp.concatenate([ar + hr_i[:, lanes], ai + hi_i[:, lanes]], axis=1)
        high, low = halves(full)
        other = slice(width + tile * 128, width + tile * 128 + 128)
        r_hi = jnp.concatenate([rd_hi[lanes, :], rd_hi[other, :]], axis=0)
        r_lo = jnp.concatenate([rd_lo[lanes, :], rd_lo[other, :]], axis=0)
        response = response + ((dot(low, r_hi) + dot(high, r_lo)) + dot(high, r_hi))
    state_out = jax.nn.gelu(response).astype(BF16)
    previous, following = inner[32:33, :], inner[40:41, :]
    for k in range(size):
        previous = jnp.where((here == 0) & (plane - 1 == k), got[k, 9:10, :], previous)
        following = jnp.where((here == last) & (plane + 1 == k), got[k, 9:10, :], following)
    x = source[...]
    row = iota((CHUNKS, x.shape[1]), 0)
    head = jnp.where(row == 0, previous, pltpu.roll(x[n - CHUNKS :], 1, 0))
    foot = jnp.where(row == CHUNKS - 1, following, pltpu.roll(x[:CHUNKS], CHUNKS - 1, 0))
    before = jnp.concatenate([head, x[: n - CHUNKS]], axis=0)
    after = jnp.concatenate([x[CHUNKS:], foot], axis=0)
    filtered = taps[0:1, :] * before + taps[1:2, :] * x + taps[2:3, :] * after
    conv_out = (gate[...] * filtered).astype(BF16)
    row, col = iota((n, n), 0), iota((n, n), 1)
    order = jnp.where(row == (col % CHUNKS) * per + col // CHUNKS, 1.0, 0.0).astype(BF16)
    conv_out = dot(order, conv_out).astype(BF16)
    state_out = dot(order, state_out).astype(BF16)
    share = out.shape[2]
    for k in range(out.shape[0]):
        at = slice(k * share, k * share + share)
        out[k] = (dot(conv_out, proj_conv[:, at]) + dot(state_out, proj_state[:, at])).astype(BF16)


def exchange(x, axis):
    return lax.all_to_all(x, axis, split_axis=0, concat_axis=0, tiled=True)


VMEM = pl.BlockSpec(memory_space=pltpu.VMEM)
SMEM = pl.BlockSpec(memory_space=pltpu.SMEM)


def call(kernel, shapes, *args, scalars=0, flops=10**7, name=None):
    return pl.pallas_call(
        kernel,
        out_shape=[jax.ShapeDtypeStruct(s, d) for s, d in shapes],
        in_specs=[SMEM] * scalars + [VMEM] * (len(args) - scalars),
        out_specs=[VMEM] * len(shapes),
        compiler_params=pltpu.CompilerParams(vmem_limit_bytes=24 * 2**20),
        cost_estimate=pl.CostEstimate(flops=flops, bytes_accessed=10**6, transcendentals=0),
        name=name,
    )(*args)


def per_device(
    stream,
    norm_gain,
    w_value,
    w_mix,
    w_gate,
    w_state,
    conv_taps,
    skip_gain,
    decay_rate,
    turn_rate,
    input_real,
    input_imag,
    read_real,
    read_imag,
    initial_state,
    intervals,
    proj_conv,
    proj_state,
):
    n, share = stream.shape
    parts = lax.axis_size("tp")
    inner_axes = SP[1:]
    inside = lax.axis_size(inner_axes)
    planes = lax.axis_size(SP[0])
    channels = w_value.shape[1]
    width = decay_rate.size
    here = lax.axis_index(inner_axes)
    plane = lax.axis_index(SP[0])
    place = jnp.stack([here, plane, jnp.full_like(here, inside - 1)]).astype(jnp.int32)

    (packed,) = call(pack_kernel, [((parts, n + 16, share), BF16)], stream, norm_gain.reshape(1, -1), name="pack")
    rows = exchange(packed, "tp")

    states = (n, width)
    table = call(
        prepare_kernel,
        [(states, F32)] * 6
        + [((CHUNKS, width), F32)] * 2
        + [((channels, 2 * width), BF16)] * 2
        + [((2 * width, channels), BF16)] * 2
        + [((8, 128), F32)],
        intervals.reshape(1, n),
        decay_rate.reshape(1, width),
        turn_rate.reshape(1, width),
        input_real.reshape(width, -1),
        input_imag.reshape(width, -1),
        read_real.reshape(2 * channels, -1),
        read_imag.reshape(2 * channels, -1),
        flops=3 * 10**9,
        name="prepare",
    )
    fr, fi, gr, gi, pr, pi, br, bi, in_hi, in_lo, rd_hi, rd_lo, total = table

    hr, hi, cr, ci, source, gate, state, message = call(
        local_kernel,
        [(states, F32)] * 2
        + [((CHUNKS, width), F32)] * 2
        + [((n, channels), F32)] * 3
        + [((inside, 24, 128), F32)],
        rows, w_value, w_mix, w_gate, w_state, fr, fi, gr, gi, pr, pi, in_hi, in_lo, total,
        name="local",
    )
    decay = decay_rate.reshape(8, 128)
    turn = turn_rate.reshape(8, 128)
    inner, message = call(
        plane_kernel,
        [((48, 128), F32), ((planes, 16, 128), F32)],
        place, exchange(message, inner_axes), decay, turn,
        scalars=1,
        name="plane",
    )
    got = exchange(message, SP[0])
    (partial,) = call(
        finish_kernel,
        [((parts, n, share), BF16)],
        place, got, inner, decay, turn,
        initial_state[:, 0].reshape(8, 128), initial_state[:, 1].reshape(8, 128),
        hr, hi, cr, ci, pr, pi, br, bi, rd_hi, rd_lo, source, gate, state,
        conv_taps, skip_gain.reshape(1, -1), proj_conv, proj_state,
        scalars=1,
        name="finish",
    )
    arrived = exchange(partial, "tp")
    return arrived.astype(F32).sum(axis=0).astype(BF16)


def solution(mesh):
    finer = Mesh(mesh.devices.reshape(16, 4, 2, mesh.shape["tp"]), ("sp_0", "sp_1", "sp_2", "tp"))
    return jax.shard_map(
        per_device,
        mesh=finer,
        in_specs=(
            P(SP, "tp"),
            P("tp"),
            P(None, "tp"),
            P(None, "tp"),
            P(None, "tp"),
            P(None, "tp"),
            P(None, "tp"),
            P("tp"),
            P(None, "tp", None),
            P(None, "tp", None),
            P(None, "tp", None, None),
            P(None, "tp", None, None),
            P(None, "tp", None, None),
            P(None, "tp", None, None),
            P(None, None, "tp", None),
            P(SP),
            P("tp", None),
            P("tp", None),
        ),
        out_specs=P(SP, "tp"),
        check_vma=False,
    )
```

```python
import jax
import jax.numpy as jnp
from jax import lax
from jax.experimental import pallas as pl
from jax.experimental.pallas import tpu as pltpu
from jax.sharding import Mesh
from jax.sharding import PartitionSpec as P

D = 2048
SP = ("sp_0", "sp_1", "sp_2")
EPSILON = 1e-06
F32 = jnp.float32
BF16 = jnp.bfloat16
CHUNKS = 8


def sin_cos(angle):
    turns = jnp.floor(angle * 0.6366197723675814 + 0.5)
    rest = ((angle - turns * 1.5703125) - turns * 4.837512969970703125e-4) - turns * 7.54978995489188216e-8
    rest = jnp.clip(rest, -0.8, 0.8)
    square = rest * rest
    sine = rest + rest * square * (
        -1.6666654611e-1 + square * (8.3321608736e-3 - 1.9515295891e-4 * square)
    )
    cosine = 1.0 - 0.5 * square + square * square * (
        4.166664568298827e-2 + square * (-1.388731625493765e-3 + 2.443315711809948e-5 * square)
    )
    quadrant = turns.astype(jnp.int32)
    odd = (quadrant & 1) == 1
    s = jnp.where(odd, cosine, sine)
    c = jnp.where(odd, sine, cosine)
    s = jnp.where((quadrant & 2) == 2, -s, s)
    c = jnp.where(((quadrant + 1) & 2) == 2, -c, c)
    return s, c


def exp_less_one(x):
    series = x * (1.0 + x * (1 / 2 + x * (1 / 6 + x * (1 / 24 + x * (1 / 120 + x * (1 / 720 + x * (1 / 5040 + x * (1 / 40320))))))))
    return jnp.where(x > -0.5, series, jnp.exp(x) - 1.0)


def moved(elapsed, decay, turn):
    magnitude = jnp.exp(-decay * elapsed)
    s, c = sin_cos(turn * elapsed)
    return magnitude * c, magnitude * s


def cmul(ar, ai, br, bi):
    return ar * br - ai * bi, ar * bi + ai * br


def iota(shape, dim):
    return lax.broadcasted_iota(jnp.int32, shape, dim)


def dot(a, b, dims=((1,), (0,))):
    return lax.dot_general(a, b, (dims, ((), ())), preferred_element_type=F32)


def halves(x):
    high = x.astype(BF16)
    return high, (x - high.astype(F32)).astype(BF16)


def scan_chunks(fr, fi, lr, li, backward):
    rows = iota(fr.shape, 0)
    for k in (1, 2, 4):
        shift = CHUNKS - k if backward else k
        outside = rows >= CHUNKS - k if backward else rows < k
        sfr = jnp.where(outside, 1.0, pltpu.roll(fr, shift, 0))
        sfi = jnp.where(outside, 0.0, pltpu.roll(fi, shift, 0))
        if lr is not None:
            slr = jnp.where(outside, 0.0, pltpu.roll(lr, shift, 0))
            sli = jnp.where(outside, 0.0, pltpu.roll(li, shift, 0))
            ar, ai = cmul(fr, fi, slr, sli)
            lr, li = lr + ar, li + ai
        fr, fi = cmul(fr, fi, sfr, sfi)
    return fr, fi, lr, li


def one_later(x, backward, fill):
    rows = iota(x.shape, 0)
    if backward:
        return jnp.where(rows == CHUNKS - 1, fill, pltpu.roll(x, CHUNKS - 1, 0))
    return jnp.where(rows == 0, fill, pltpu.roll(x, 1, 0))


def pack_kernel(place, stream, gain, out, gain_here, sems):
    n = stream.shape[0]
    copies = [pltpu.make_async_copy(stream, out.at[k, pl.ds(0, n)], sems.at[k]) for k in range(out.shape[0])]
    gain_copy = pltpu.make_async_copy(gain, gain_here, sems.at[out.shape[0]])
    gain_copy.start()
    for copy in copies:
        copy.start()
    gain_copy.wait()
    g = gain_here[...]
    high = g.astype(BF16)
    left = g - high.astype(F32)
    mid = left.astype(BF16)
    low = (left - mid.astype(F32)).astype(BF16)
    row = iota((16, g.shape[1]), 0)
    tail = jnp.where(row == 0, high.astype(F32), jnp.where(row == 1, mid.astype(F32), jnp.where(row == 2, low.astype(F32), 0.0)))
    tail = tail.astype(BF16)
    for k in range(out.shape[0]):
        out[k, n : n + 16, :] = tail
    for copy in copies:
        copy.wait()


def row_of(ref, d, q):
    return jnp.concatenate([ref[d, 2 * q : 2 * q + 1, :], ref[d, 2 * q + 1 : 2 * q + 2, :]], axis=1)


def doubled(x):
    return jnp.concatenate([x, x], axis=1)


def local_kernel(rows, w_value, w_mix, w_gate, w_state, intervals, decay, turn, in_re, in_im, init, hr_o, hi_o, cr_o, ci_o, pr_o, pi_o, br_o, bi_o, source_o, gate_o, input_o, consts, message):
    parts, n, share = rows.shape[0], rows.shape[1] - 16, rows.shape[2]
    per = n // CHUNKS
    channels = w_value.shape[1]
    row, col = iota((n, n), 0), iota((n, n), 1)
    ordered = col == (row % CHUNKS) * per + row // CHUNKS
    steps = jnp.sum(jnp.where(ordered, intervals[...], 0.0), axis=1, keepdims=True)
    total = jnp.sum(intervals[...], axis=1, keepdims=True)
    order = jnp.where(ordered, 1.0, 0.0).astype(BF16)

    squares = 0.0
    for k in range(parts):
        x = rows[k, 0:n, :].astype(F32)
        squares = squares + jnp.sum(x * x, axis=1, keepdims=True)
    inv_rms = lax.rsqrt(squares / D + EPSILON)
    first = second = 0.0
    for k in range(parts):
        tail = rows[k, n : n + 16, :].astype(F32)
        gain = (tail[0:1] + tail[1:2]) + tail[2:3]
        normed = ((rows[k, 0:n, :].astype(F32) * inv_rms) * gain).astype(BF16)
        at = slice(k * share, k * share + share)
        first = first + dot(normed, jnp.concatenate([w_value[at, :], w_mix[at, :]], axis=1))
        second = second + dot(normed, jnp.concatenate([w_gate[at, :], w_state[at, :]], axis=1))
    first = dot(order, first.astype(BF16))
    second = dot(order, second.astype(BF16))
    source = (first[:, :channels] * first[:, channels:]).astype(BF16).astype(F32)
    source_o[...] = source
    gate_o[...] = second[:, :channels]
    input_o[...] = second[:, channels:]
    state = second[:, channels:].astype(BF16)
    state = jnp.concatenate([state, state], axis=1)

    groups, states = decay.shape[1], decay.shape[2]
    wide = channels // groups
    pairs = groups // 2
    edges = []
    for d in range(2):
        backward = d == 1
        rates, turns = decay[d], turn[d]
        inverse = 1.0 / (rates * rates + turns * turns)
        inv_re = jnp.broadcast_to((-rates * inverse)[:, None, :], (groups, wide, states)).reshape(channels, states)
        inv_im = jnp.broadcast_to((-turns * inverse)[:, None, :], (groups, wide, states)).reshape(channels, states)
        at = slice(d * channels, d * channels + channels)
        scaled_re, scaled_im = cmul(in_re[at, :], in_im[at, :], inv_re, inv_im)
        scaled_re, scaled_im = doubled(scaled_re), doubled(scaled_im)
        for q in range(pairs):
            tile = d * pairs + q
            lanes = slice(tile * 128, tile * 128 + 128)
            rate, turning = row_of(decay, d, q), row_of(turn, d, q)
            consts[tile : tile + 1, :] = rate
            consts[8 + tile : 9 + tile, :] = turning
            consts[16 + tile : 17 + tile, :] = jnp.concatenate([init[d, 0, 2 * q : 2 * q + 1, :], init[d, 0, 2 * q + 1 : 2 * q + 2, :]], axis=1)
            consts[24 + tile : 25 + tile, :] = jnp.concatenate([init[d, 1, 2 * q : 2 * q + 1, :], init[d, 1, 2 * q + 1 : 2 * q + 2, :]], axis=1)
            mine = iota((channels, 128), 0) // wide == 2 * q + iota((channels, 128), 1) // states
            re_hi, re_lo = halves(jnp.where(mine, scaled_re, 0.0))
            im_hi, im_lo = halves(jnp.where(mine, scaled_im, 0.0))
            matrix = jnp.concatenate([jnp.concatenate([re_hi, re_lo], axis=0), jnp.concatenate([im_hi, im_lo], axis=0)], axis=1)
            driven = dot(state, matrix)
            damping = -rate * steps
            s, c = sin_cos((0.5 * turning) * steps)
            magnitude = jnp.exp(damping)
            twice = 2.0 * s * s
            cosine = 1.0 - twice
            fr = magnitude * cosine
            fi = magnitude * (2.0 * s * c)
            lift = exp_less_one(damping) * cosine - twice
            push_re, push_im = cmul(lift, fi, driven[:, :128], driven[:, 128:])
            cr = ci = hr = hi = None
            for i in reversed(range(per)) if backward else range(per):
                at = slice(i * CHUNKS, i * CHUNKS + CHUNKS)
                r, m = fr[at], fi[at]
                if cr is None:
                    cr, ci, hr, hi = r, m, push_re[at], push_im[at]
                else:
                    cr, ci = cmul(r, m, cr, ci)
                    ar, ai = cmul(r, m, hr, hi)
                    hr, hi = ar + push_re[at], ai + push_im[at]
                pr_o[at, lanes] = cr
                pi_o[at, lanes] = ci
                hr_o[at, lanes] = hr
                hi_o[at, lanes] = hi
            br, bi, lr, li = scan_chunks(cr, ci, hr, hi, backward)
            br_o[:, lanes] = one_later(br, backward, 1.0)
            bi_o[:, lanes] = one_later(bi, backward, 0.0)
            cr_o[:, lanes] = one_later(lr, backward, 0.0)
            ci_o[:, lanes] = one_later(li, backward, 0.0)
            edge = 0 if backward else CHUNKS - 1
            edges.append((lr[edge : edge + 1], li[edge : edge + 1]))
    for k in range(message.shape[0]):
        for tile, (r, m) in enumerate(edges):
            message[k, tile : tile + 1, :] = r
            message[k, 8 + tile : 9 + tile, :] = m
        message[k, 16:17, :] = jnp.broadcast_to(total, (1, 128))
        message[k, 17:18, :] = source[0:1]
        message[k, 18:19, :] = source[n - 1 : n]
        message[k, 19:24, :] = jnp.zeros((5, 128), F32)


def plane_kernel(place, got, consts, inner, message):
    size = got.shape[0]
    here, plane = place[0], place[1]
    rate, turning = consts[0:8, :], consts[8:16, :]
    forward = iota((8, 128), 0) < 4
    hr = hi = spent = jnp.zeros((8, 128), F32)
    ir = ii = before = hr
    for k in range(size):
        m = size - 1 - k
        mine = (forward & (here == k)) | (jnp.logical_not(forward) & (here == m))
        ir = jnp.where(mine, hr, ir)
        ii = jnp.where(mine, hi, ii)
        before = jnp.where(mine, spent, before)
        elapsed = jnp.where(forward, got[k, 16:17, :], got[m, 16:17, :])
        ar, ai = moved(elapsed, rate, turning)
        ar, ai = cmul(ar, ai, hr, hi)
        hr = ar + jnp.where(forward, got[k, 0:8, :], got[m, 0:8, :])
        hi = ai + jnp.where(forward, got[k, 8:16, :], got[m, 8:16, :])
        spent = spent + elapsed
    wr, wi = moved(before, rate, turning)
    inner[0:8, :] = ir
    inner[8:16, :] = ii
    inner[16:24, :] = wr
    inner[24:32, :] = wi
    previous = following = jnp.zeros((1, 128), F32)
    for k in range(size):
        previous = jnp.where(here - 1 == k, got[k, 18:19, :], previous)
        following = jnp.where(here + 1 == k, got[k, 17:18, :], following)
    inner[32:40, :] = jnp.broadcast_to(previous, (8, 128))
    inner[40:48, :] = jnp.broadcast_to(following, (8, 128))
    swapped = pltpu.roll(hi, 4, 0)
    later = jnp.where(forward, hr, swapped)
    earlier = jnp.where(forward, swapped, hr)
    row = iota((8, 128), 0)
    note_later = jnp.where(row == 0, spent, jnp.where(row == 1, got[size - 1, 18:19, :], 0.0))
    note_earlier = jnp.where(row == 0, spent, jnp.where(row == 1, got[0, 17:18, :], 0.0))
    for k in range(message.shape[0]):
        message[k, 0:8, :] = jnp.where(plane < k, later, earlier)
        message[k, 8:16, :] = jnp.where(plane < k, note_later, note_earlier)


def finish_kernel(place, got, inner, consts, hr_i, hi_i, cr_i, ci_i, pr, pi, br, bi, rd_re, rd_im, source, gate, state, taps, skip, proj_conv, proj_state, out):
    size = got.shape[0]
    here, plane, last = place[0], place[1], place[2]
    rate, turning = consts[0:8, :], consts[8:16, :]
    forward = iota((8, 128), 0) < 4
    hr, hi = consts[16:24, :], consts[24:32, :]
    for k in range(size):
        m = size - 1 - k
        active = (forward & (plane > k)) | (jnp.logical_not(forward) & (plane < m))
        elapsed = jnp.where(forward, got[k, 8:9, :], got[m, 8:9, :])
        ar, ai = moved(elapsed, rate, turning)
        ar, ai = cmul(ar, ai, hr, hi)
        a, b = got[k, 0:8, :], got[m, 0:8, :]
        hr = jnp.where(active, ar + jnp.where(forward, a, b), hr)
        hi = jnp.where(active, ai + pltpu.roll(jnp.where(forward, b, a), 4, 0), hi)
    ar, ai = cmul(inner[16:24, :], inner[24:32, :], hr, hi)
    inc_re = ar + inner[0:8, :]
    inc_im = ai + inner[8:16, :]
    n, width = hr_i.shape
    per = n // CHUNKS
    channels = rd_re.shape[0] // 2
    states = rd_re.shape[1]
    pairs = width // 256
    block = channels // pairs
    wide = block // 2
    responses = []
    for q in range(pairs):
        mine = iota((block, 128), 0) // wide == iota((block, 128), 1) // states
        full, matrix = [], []
        for d in range(2):
            tile = d * pairs + q
            lanes = slice(tile * 128, tile * 128 + 128)
            er, ei = cmul(br[:, lanes], bi[:, lanes], inc_re[tile : tile + 1], inc_im[tile : tile + 1])
            er = jnp.concatenate([er + cr_i[:, lanes]] * per, axis=0)
            ei = jnp.concatenate([ei + ci_i[:, lanes]] * per, axis=0)
            ar, ai = cmul(pr[:, lanes], pi[:, lanes], er, ei)
            full += [ar + hr_i[:, lanes], ai + hi_i[:, lanes]]
            at = slice(d * channels + q * block, d * channels + (q + 1) * block)
            matrix += [jnp.where(mine, doubled(rd_re[at, :]), 0.0), jnp.where(mine, -doubled(rd_im[at, :]), 0.0)]
        high, low = halves(jnp.concatenate(full, axis=1))
        r_hi, r_lo = halves(jnp.concatenate(matrix, axis=1))
        across = ((1,), (1,))
        responses.append((dot(low, r_hi, across) + dot(high, r_lo, across)) + dot(high, r_hi, across))
    response = state[...] * skip[...] + jnp.concatenate(responses, axis=1)
    state_out = jax.nn.gelu(response).astype(BF16)
    previous, following = inner[32:33, :], inner[40:41, :]
    for k in range(size):
        previous = jnp.where((here == 0) & (plane - 1 == k), got[k, 9:10, :], previous)
        following = jnp.where((here == last) & (plane + 1 == k), got[k, 9:10, :], following)
    x = source[...]
    row = iota((CHUNKS, x.shape[1]), 0)
    head = jnp.where(row == 0, previous, pltpu.roll(x[n - CHUNKS :], 1, 0))
    foot = jnp.where(row == CHUNKS - 1, following, pltpu.roll(x[:CHUNKS], CHUNKS - 1, 0))
    before = jnp.concatenate([head, x[: n - CHUNKS]], axis=0)
    after = jnp.concatenate([x[CHUNKS:], foot], axis=0)
    filtered = taps[0:1, :] * before + taps[1:2, :] * x + taps[2:3, :] * after
    conv_out = (gate[...] * filtered).astype(BF16)
    row, col = iota((n, n), 0), iota((n, n), 1)
    order = jnp.where(row == (col % CHUNKS) * per + col // CHUNKS, 1.0, 0.0).astype(BF16)
    conv_out = dot(order, conv_out).astype(BF16)
    state_out = dot(order, state_out).astype(BF16)
    share = out.shape[2]
    for k in range(out.shape[0]):
        at = slice(k * share, k * share + share)
        out[k] = (dot(conv_out, proj_conv[:, at]) + dot(state_out, proj_state[:, at])).astype(BF16)


def exchange(x, axis):
    return lax.all_to_all(x, axis, split_axis=0, concat_axis=0, tiled=True)


VMEM = pl.BlockSpec(memory_space=pltpu.VMEM)
HBM = pl.BlockSpec(memory_space=pltpu.HBM)
SMEM = pl.BlockSpec(memory_space=pltpu.SMEM)


def call(kernel, shapes, *args, specs=(), name=None):
    return pl.pallas_call(
        kernel,
        out_shape=[jax.ShapeDtypeStruct(s, d) for s, d in shapes],
        in_specs=[dict(specs).get(k, VMEM) for k in range(len(args))],
        out_specs=[VMEM] * len(shapes),
        compiler_params=pltpu.CompilerParams(vmem_limit_bytes=24 * 2**20),
        name=name,
    )(*args)


def per_device(
    stream,
    norm_gain,
    w_value,
    w_mix,
    w_gate,
    w_state,
    conv_taps,
    skip_gain,
    decay_rate,
    turn_rate,
    input_real,
    input_imag,
    read_real,
    read_imag,
    initial_state,
    intervals,
    proj_conv,
    proj_state,
):
    n, share = stream.shape
    parts = lax.axis_size("tp")
    inner_axes = SP[1:]
    inside = lax.axis_size(inner_axes)
    planes = lax.axis_size(SP[0])
    channels = w_value.shape[1]
    width = decay_rate.size
    here = lax.axis_index(inner_axes)
    plane = lax.axis_index(SP[0])
    place = jnp.stack([here, plane, jnp.full_like(here, inside - 1)]).astype(jnp.int32)

    packed = pl.pallas_call(
        pack_kernel,
        out_shape=jax.ShapeDtypeStruct((parts, n + 16, share), BF16),
        in_specs=[SMEM, HBM, HBM],
        out_specs=VMEM,
        scratch_shapes=[pltpu.VMEM((1, share), F32), pltpu.SemaphoreType.DMA((parts + 1,))],
        compiler_params=pltpu.CompilerParams(vmem_limit_bytes=4 * 2**20),
        cost_estimate=pl.CostEstimate(flops=10**9, bytes_accessed=3 * 10**7, transcendentals=0),
        name="pack",
    )(place, stream, norm_gain.reshape(1, -1))
    rows = exchange(packed, "tp")

    states = ((n, width), F32)
    chunks = ((CHUNKS, width), F32)
    mixed = ((n, channels), F32)
    hr, hi, cr, ci, pr, pi, br, bi, source, gate, state, consts, message = call(
        local_kernel,
        [states, states, chunks, chunks, states, states, chunks, chunks, mixed, mixed, mixed]
        + [((32, 128), F32), ((inside, 24, 128), F32)],
        rows, w_value, w_mix, w_gate, w_state, intervals.reshape(1, n), decay_rate, turn_rate,
        jnp.swapaxes(input_real, 2, 3).reshape(2 * channels, -1),
        jnp.swapaxes(input_imag, 2, 3).reshape(2 * channels, -1),
        initial_state,
        name="local",
    )
    inner, message = call(
        plane_kernel,
        [((48, 128), F32), ((planes, 16, 128), F32)],
        place, exchange(message, inner_axes), consts,
        specs={0: SMEM},
        name="plane",
    )
    got = exchange(message, SP[0])
    (partial,) = call(
        finish_kernel,
        [((parts, n, share), BF16)],
        place, got, inner, consts, hr, hi, cr, ci, pr, pi, br, bi,
        read_real.reshape(2 * channels, -1), read_imag.reshape(2 * channels, -1), source, gate, state,
        conv_taps, skip_gain.reshape(1, -1), proj_conv, proj_state,
        specs={0: SMEM},
        name="finish",
    )
    arrived = exchange(partial, "tp")
    return arrived.astype(F32).sum(axis=0).astype(BF16)


def solution(mesh):
    finer = Mesh(mesh.devices.reshape(16, 4, 2, mesh.shape["tp"]), ("sp_0", "sp_1", "sp_2", "tp"))
    return jax.shard_map(
        per_device,
        mesh=finer,
        in_specs=(
            P(SP, "tp"),
            P("tp"),
            P(None, "tp"),
            P(None, "tp"),
            P(None, "tp"),
            P(None, "tp"),
            P(None, "tp"),
            P("tp"),
            P(None, "tp", None),
            P(None, "tp", None),
            P(None, "tp", None, None),
            P(None, "tp", None, None),
            P(None, "tp", None, None),
            P(None, "tp", None, None),
            P(None, None, "tp", None),
            P(SP),
            P("tp", None),
            P("tp", None),
        ),
        out_specs=P(SP, "tp"),
        check_vma=False,
    )
```

```python
import jax
import jax.numpy as jnp
from jax import lax
from jax.experimental import pallas as pl
from jax.experimental.pallas import tpu as pltpu
from jax.sharding import Mesh
from jax.sharding import PartitionSpec as P

D = 2048
SP = ("sp_0", "sp_1", "sp_2")
EPSILON = 1e-06
F32 = jnp.float32
BF16 = jnp.bfloat16
CHUNKS = 8


def sin_cos(angle):
    turns = jnp.floor(angle * 0.6366197723675814 + 0.5)
    rest = ((angle - turns * 1.5703125) - turns * 4.837512969970703125e-4) - turns * 7.54978995489188216e-8
    rest = jnp.clip(rest, -0.8, 0.8)
    square = rest * rest
    sine = rest + rest * square * (
        -1.6666654611e-1 + square * (8.3321608736e-3 - 1.9515295891e-4 * square)
    )
    cosine = 1.0 - 0.5 * square + square * square * (
        4.166664568298827e-2 + square * (-1.388731625493765e-3 + 2.443315711809948e-5 * square)
    )
    quadrant = turns.astype(jnp.int32)
    odd = (quadrant & 1) == 1
    s = jnp.where(odd, cosine, sine)
    c = jnp.where(odd, sine, cosine)
    s = jnp.where((quadrant & 2) == 2, -s, s)
    c = jnp.where(((quadrant + 1) & 2) == 2, -c, c)
    return s, c


def exp_less_one(x):
    series = x * (1.0 + x * (1 / 2 + x * (1 / 6 + x * (1 / 24 + x * (1 / 120 + x * (1 / 720 + x * (1 / 5040 + x * (1 / 40320))))))))
    return jnp.where(x > -0.5, series, jnp.exp(x) - 1.0)


def moved(elapsed, decay, turn):
    magnitude = jnp.exp(-decay * elapsed)
    s, c = sin_cos(turn * elapsed)
    return magnitude * c, magnitude * s


def cmul(ar, ai, br, bi):
    return ar * br - ai * bi, ar * bi + ai * br


def iota(shape, dim):
    return lax.broadcasted_iota(jnp.int32, shape, dim)


def dot(a, b, dims=((1,), (0,))):
    return lax.dot_general(a, b, (dims, ((), ())), preferred_element_type=F32)


def halves(x):
    high = x.astype(BF16)
    return high, (x - high.astype(F32)).astype(BF16)


def scan_chunks(fr, fi, lr, li, backward):
    rows = iota(fr.shape, 0)
    for k in (1, 2, 4):
        shift = CHUNKS - k if backward else k
        outside = rows >= CHUNKS - k if backward else rows < k
        sfr = jnp.where(outside, 1.0, pltpu.roll(fr, shift, 0))
        sfi = jnp.where(outside, 0.0, pltpu.roll(fi, shift, 0))
        if lr is not None:
            slr = jnp.where(outside, 0.0, pltpu.roll(lr, shift, 0))
            sli = jnp.where(outside, 0.0, pltpu.roll(li, shift, 0))
            ar, ai = cmul(fr, fi, slr, sli)
            lr, li = lr + ar, li + ai
        fr, fi = cmul(fr, fi, sfr, sfi)
    return fr, fi, lr, li


def one_later(x, backward, fill):
    rows = iota(x.shape, 0)
    if backward:
        return jnp.where(rows == CHUNKS - 1, fill, pltpu.roll(x, CHUNKS - 1, 0))
    return jnp.where(rows == 0, fill, pltpu.roll(x, 1, 0))


def pack_kernel(stream, gain, intervals, taps, skip, out, notes, sems):
    n, share = stream.shape
    copies = [pltpu.make_async_copy(stream, out.at[k, pl.ds(0, n)], sems.at[k]) for k in range(out.shape[0])]
    for copy in copies:
        copy.start()
    row = iota((8, share), 0)
    tail = jnp.zeros((8, share), F32)
    for at, x in enumerate((gain[...], jnp.concatenate([intervals[...]] * (share // n), axis=1))):
        high = x.astype(BF16).astype(F32)
        mid = (x - high).astype(BF16).astype(F32)
        for p, piece in enumerate((high, mid, x - high - mid)):
            tail = jnp.where(row == 3 * at + p, piece, tail)
    for k in range(out.shape[0]):
        out[k, n : n + 8, :] = tail.astype(BF16)
    notes[0:3, :] = taps[...]
    notes[3:4, :] = skip[...]
    notes[4:8, :] = jnp.zeros((4, notes.shape[1]), F32)
    for copy in copies:
        copy.wait()


def row_of(ref, d, q):
    return jnp.concatenate([ref[d, 2 * q : 2 * q + 1, :], ref[d, 2 * q + 1 : 2 * q + 2, :]], axis=1)


def doubled(x):
    return jnp.concatenate([x, x], axis=1)


def local_kernel(rows, w_value, w_mix, w_gate, w_state, decay, turn, in_re, in_im, init, notes, hr_o, hi_o, cr_o, ci_o, pr_o, pi_o, br_o, bi_o, source_o, gate_o, input_o, consts, message):
    parts, n, share = rows.shape[0], rows.shape[1] - 8, rows.shape[2]
    per = n // CHUNKS
    channels = w_value.shape[1]
    row, col = iota((n, n), 0), iota((n, n), 1)
    ordered = col == (row % CHUNKS) * per + row // CHUNKS
    tail = rows[0, n : n + 8, 0:n].astype(F32)
    intervals = (tail[3:4] + tail[4:5]) + tail[5:6]
    steps = jnp.sum(jnp.where(ordered, intervals, 0.0), axis=1, keepdims=True)
    total = jnp.sum(intervals, axis=1, keepdims=True)
    order = jnp.where(ordered, 1.0, 0.0).astype(BF16)

    squares = 0.0
    for k in range(parts):
        x = rows[k, 0:n, :].astype(F32)
        squares = squares + jnp.sum(x * x, axis=1, keepdims=True)
    inv_rms = lax.rsqrt(squares / D + EPSILON)
    first = second = 0.0
    for k in range(parts):
        tail = rows[k, n : n + 8, :].astype(F32)
        gain = (tail[0:1] + tail[1:2]) + tail[2:3]
        normed = ((rows[k, 0:n, :].astype(F32) * inv_rms) * gain).astype(BF16)
        at = slice(k * share, k * share + share)
        first = first + dot(normed, jnp.concatenate([w_value[at, :], w_mix[at, :]], axis=1))
        second = second + dot(normed, jnp.concatenate([w_gate[at, :], w_state[at, :]], axis=1))
    first = dot(order, first.astype(BF16))
    second = dot(order, second.astype(BF16))
    source = (first[:, :channels] * first[:, channels:]).astype(BF16).astype(F32)
    source_o[...] = source
    gate_o[...] = second[:, :channels]
    input_o[...] = second[:, channels:]
    state = second[:, channels:].astype(BF16)
    state = jnp.concatenate([state, state], axis=1)

    groups, states = decay.shape[1], decay.shape[2]
    wide = channels // groups
    pairs = groups // 2
    consts[32:40, :] = notes[...]
    edges = []
    for d in range(2):
        backward = d == 1
        rates, turns = decay[d], turn[d]
        inverse = 1.0 / (rates * rates + turns * turns)
        inv_re = jnp.broadcast_to((-rates * inverse)[:, None, :], (groups, wide, states)).reshape(channels, states)
        inv_im = jnp.broadcast_to((-turns * inverse)[:, None, :], (groups, wide, states)).reshape(channels, states)
        at = slice(d * channels, d * channels + channels)
        scaled_re, scaled_im = cmul(in_re[at, :], in_im[at, :], inv_re, inv_im)
        scaled_re, scaled_im = doubled(scaled_re), doubled(scaled_im)
        for q in range(pairs):
            tile = d * pairs + q
            lanes = slice(tile * 128, tile * 128 + 128)
            rate, turning = row_of(decay, d, q), row_of(turn, d, q)
            consts[tile : tile + 1, :] = rate
            consts[8 + tile : 9 + tile, :] = turning
            consts[16 + tile : 17 + tile, :] = jnp.concatenate([init[d, 0, 2 * q : 2 * q + 1, :], init[d, 0, 2 * q + 1 : 2 * q + 2, :]], axis=1)
            consts[24 + tile : 25 + tile, :] = jnp.concatenate([init[d, 1, 2 * q : 2 * q + 1, :], init[d, 1, 2 * q + 1 : 2 * q + 2, :]], axis=1)
            mine = iota((channels, 128), 0) // wide == 2 * q + iota((channels, 128), 1) // states
            re_hi, re_lo = halves(jnp.where(mine, scaled_re, 0.0))
            im_hi, im_lo = halves(jnp.where(mine, scaled_im, 0.0))
            matrix = jnp.concatenate([jnp.concatenate([re_hi, re_lo], axis=0), jnp.concatenate([im_hi, im_lo], axis=0)], axis=1)
            driven = dot(state, matrix)
            damping = -rate * steps
            s, c = sin_cos((0.5 * turning) * steps)
            magnitude = jnp.exp(damping)
            twice = 2.0 * s * s
            cosine = 1.0 - twice
            fr = magnitude * cosine
            fi = magnitude * (2.0 * s * c)
            lift = exp_less_one(damping) * cosine - twice
            push_re, push_im = cmul(lift, fi, driven[:, :128], driven[:, 128:])
            cr = ci = hr = hi = None
            for i in reversed(range(per)) if backward else range(per):
                at = slice(i * CHUNKS, i * CHUNKS + CHUNKS)
                r, m = fr[at], fi[at]
                if cr is None:
                    cr, ci, hr, hi = r, m, push_re[at], push_im[at]
                else:
                    cr, ci = cmul(r, m, cr, ci)
                    ar, ai = cmul(r, m, hr, hi)
                    hr, hi = ar + push_re[at], ai + push_im[at]
                pr_o[at, lanes] = cr
                pi_o[at, lanes] = ci
                hr_o[at, lanes] = hr
                hi_o[at, lanes] = hi
            br, bi, lr, li = scan_chunks(cr, ci, hr, hi, backward)
            br_o[:, lanes] = one_later(br, backward, 1.0)
            bi_o[:, lanes] = one_later(bi, backward, 0.0)
            cr_o[:, lanes] = one_later(lr, backward, 0.0)
            ci_o[:, lanes] = one_later(li, backward, 0.0)
            edge = 0 if backward else CHUNKS - 1
            edges.append((lr[edge : edge + 1], li[edge : edge + 1]))
    for k in range(message.shape[0]):
        for tile, (r, m) in enumerate(edges):
            message[k, tile : tile + 1, :] = r
            message[k, 8 + tile : 9 + tile, :] = m
        message[k, 16:17, :] = jnp.broadcast_to(total, (1, 128))
        message[k, 17:18, :] = source[0:1]
        message[k, 18:19, :] = source[n - 1 : n]
        message[k, 19:24, :] = jnp.zeros((5, 128), F32)


def plane_kernel(got, consts, inner, message):
    size = got.shape[0]
    here, plane = lax.axis_index(SP[1:]), lax.axis_index(SP[0])
    rate, turning = consts[0:8, :], consts[8:16, :]
    forward = iota((8, 128), 0) < 4
    hr = hi = spent = jnp.zeros((8, 128), F32)
    ir = ii = before = hr
    for k in range(size):
        m = size - 1 - k
        mine = (forward & (here == k)) | (jnp.logical_not(forward) & (here == m))
        ir = jnp.where(mine, hr, ir)
        ii = jnp.where(mine, hi, ii)
        before = jnp.where(mine, spent, before)
        elapsed = jnp.where(forward, got[k, 16:17, :], got[m, 16:17, :])
        ar, ai = moved(elapsed, rate, turning)
        ar, ai = cmul(ar, ai, hr, hi)
        hr = ar + jnp.where(forward, got[k, 0:8, :], got[m, 0:8, :])
        hi = ai + jnp.where(forward, got[k, 8:16, :], got[m, 8:16, :])
        spent = spent + elapsed
    wr, wi = moved(before, rate, turning)
    inner[0:8, :] = ir
    inner[8:16, :] = ii
    inner[16:24, :] = wr
    inner[24:32, :] = wi
    previous = following = jnp.zeros((1, 128), F32)
    for k in range(size):
        previous = jnp.where(here - 1 == k, got[k, 18:19, :], previous)
        following = jnp.where(here + 1 == k, got[k, 17:18, :], following)
    inner[32:40, :] = jnp.broadcast_to(previous, (8, 128))
    inner[40:48, :] = jnp.broadcast_to(following, (8, 128))
    swapped = pltpu.roll(hi, 4, 0)
    later = jnp.where(forward, hr, swapped)
    earlier = jnp.where(forward, swapped, hr)
    row = iota((8, 128), 0)
    high = spent.astype(BF16).astype(F32)
    mid = (spent - high).astype(BF16).astype(F32)
    note = jnp.where(row == 0, high, jnp.where(row == 1, mid, jnp.where(row == 2, spent - high - mid, 0.0)))
    note_later = jnp.where(row == 3, got[size - 1, 18:19, :], note)
    note_earlier = jnp.where(row == 3, got[0, 17:18, :], note)
    later = jnp.concatenate([later, note_later], axis=0)
    earlier = jnp.concatenate([earlier, note_earlier], axis=0)
    for k in range(message.shape[0]):
        message[k] = jnp.where(plane < k, later, earlier).astype(BF16)


def finish_kernel(got, inner, consts, hr_i, hi_i, cr_i, ci_i, pr, pi, br, bi, rd_re, rd_im, source, gate, state, proj_conv, proj_state, out):
    size = got.shape[0]
    here, plane = lax.axis_index(SP[1:]), lax.axis_index(SP[0])
    last = lax.axis_size(SP[1:]) - 1
    rate, turning = consts[0:8, :], consts[8:16, :]
    forward = iota((8, 128), 0) < 4
    hr, hi = consts[16:24, :], consts[24:32, :]
    arrived = [got[k].astype(F32) for k in range(size)]
    times = [(x[8:9] + x[9:10]) + x[10:11] for x in arrived]
    for k in range(size):
        m = size - 1 - k
        active = (forward & (plane > k)) | (jnp.logical_not(forward) & (plane < m))
        elapsed = jnp.where(forward, times[k], times[m])
        ar, ai = moved(elapsed, rate, turning)
        ar, ai = cmul(ar, ai, hr, hi)
        a, b = arrived[k][0:8], arrived[m][0:8]
        hr = jnp.where(active, ar + jnp.where(forward, a, b), hr)
        hi = jnp.where(active, ai + pltpu.roll(jnp.where(forward, b, a), 4, 0), hi)
    ar, ai = cmul(inner[16:24, :], inner[24:32, :], hr, hi)
    inc_re = ar + inner[0:8, :]
    inc_im = ai + inner[8:16, :]
    n, width = hr_i.shape
    per = n // CHUNKS
    channels = rd_re.shape[0] // 2
    states = rd_re.shape[1]
    pairs = width // 256
    block = channels // pairs
    wide = block // 2
    responses = []
    for q in range(pairs):
        mine = iota((block, 128), 0) // wide == iota((block, 128), 1) // states
        full, matrix = [], []
        for d in range(2):
            tile = d * pairs + q
            lanes = slice(tile * 128, tile * 128 + 128)
            er, ei = cmul(br[:, lanes], bi[:, lanes], inc_re[tile : tile + 1], inc_im[tile : tile + 1])
            er = jnp.concatenate([er + cr_i[:, lanes]] * per, axis=0)
            ei = jnp.concatenate([ei + ci_i[:, lanes]] * per, axis=0)
            ar, ai = cmul(pr[:, lanes], pi[:, lanes], er, ei)
            full += [ar + hr_i[:, lanes], ai + hi_i[:, lanes]]
            at = slice(d * channels + q * block, d * channels + (q + 1) * block)
            matrix += [jnp.where(mine, doubled(rd_re[at, :]), 0.0), jnp.where(mine, -doubled(rd_im[at, :]), 0.0)]
        high, low = halves(jnp.concatenate(full, axis=1))
        r_hi, r_lo = halves(jnp.concatenate(matrix, axis=1))
        across = ((1,), (1,))
        responses.append((dot(low, r_hi, across) + dot(high, r_lo, across)) + dot(high, r_hi, across))
    response = state[...] * consts[35:36, :] + jnp.concatenate(responses, axis=1)
    state_out = jax.nn.gelu(response).astype(BF16)
    previous, following = inner[32:33, :], inner[40:41, :]
    for k in range(size):
        previous = jnp.where((here == 0) & (plane - 1 == k), arrived[k][11:12], previous)
        following = jnp.where((here == last) & (plane + 1 == k), arrived[k][11:12], following)
    x = source[...]
    row = iota((CHUNKS, x.shape[1]), 0)
    head = jnp.where(row == 0, previous, pltpu.roll(x[n - CHUNKS :], 1, 0))
    foot = jnp.where(row == CHUNKS - 1, following, pltpu.roll(x[:CHUNKS], CHUNKS - 1, 0))
    before = jnp.concatenate([head, x[: n - CHUNKS]], axis=0)
    after = jnp.concatenate([x[CHUNKS:], foot], axis=0)
    filtered = consts[32:33, :] * before + consts[33:34, :] * x + consts[34:35, :] * after
    conv_out = (gate[...] * filtered).astype(BF16)
    row, col = iota((n, n), 0), iota((n, n), 1)
    order = jnp.where(row == (col % CHUNKS) * per + col // CHUNKS, 1.0, 0.0).astype(BF16)
    conv_out = dot(order, conv_out).astype(BF16)
    state_out = dot(order, state_out).astype(BF16)
    share = out.shape[2]
    for k in range(out.shape[0]):
        at = slice(k * share, k * share + share)
        out[k] = (dot(conv_out, proj_conv[:, at]) + dot(state_out, proj_state[:, at])).astype(BF16)


def exchange(x, axis):
    return lax.all_to_all(x, axis, split_axis=0, concat_axis=0, tiled=True)


VMEM = pl.BlockSpec(memory_space=pltpu.VMEM)


def call(kernel, shapes, *args, name=None):
    return pl.pallas_call(
        kernel,
        out_shape=[jax.ShapeDtypeStruct(s, d) for s, d in shapes],
        in_specs=[VMEM] * len(args),
        out_specs=[VMEM] * len(shapes),
        compiler_params=pltpu.CompilerParams(vmem_limit_bytes=24 * 2**20),
        name=name,
    )(*args)


def per_device(
    stream,
    norm_gain,
    w_value,
    w_mix,
    w_gate,
    w_state,
    conv_taps,
    skip_gain,
    decay_rate,
    turn_rate,
    input_real,
    input_imag,
    read_real,
    read_imag,
    initial_state,
    intervals,
    proj_conv,
    proj_state,
):
    n, share = stream.shape
    parts = lax.axis_size("tp")
    inner_axes = SP[1:]
    inside = lax.axis_size(inner_axes)
    planes = lax.axis_size(SP[0])
    channels = w_value.shape[1]
    width = decay_rate.size
    packed, notes = pl.pallas_call(
        pack_kernel,
        out_shape=[jax.ShapeDtypeStruct((parts, n + 8, share), BF16), jax.ShapeDtypeStruct((8, channels), F32)],
        in_specs=[VMEM] * 5,
        out_specs=[VMEM] * 2,
        scratch_shapes=[pltpu.SemaphoreType.DMA((parts,))],
        compiler_params=pltpu.CompilerParams(vmem_limit_bytes=4 * 2**20),
        cost_estimate=pl.CostEstimate(flops=10**9, bytes_accessed=3 * 10**8, transcendentals=0),
        name="pack",
    )(stream, norm_gain.reshape(1, -1), intervals.reshape(1, n), conv_taps, skip_gain.reshape(1, -1))
    rows = exchange(packed, "tp")

    states = ((n, width), F32)
    chunks = ((CHUNKS, width), F32)
    mixed = ((n, channels), F32)
    hr, hi, cr, ci, pr, pi, br, bi, source, gate, state, consts, message = call(
        local_kernel,
        [states, states, chunks, chunks, states, states, chunks, chunks, mixed, mixed, mixed]
        + [((40, channels), F32), ((inside, 24, 128), F32)],
        rows, w_value, w_mix, w_gate, w_state, decay_rate, turn_rate,
        jnp.swapaxes(input_real, 2, 3).reshape(2 * channels, -1),
        jnp.swapaxes(input_imag, 2, 3).reshape(2 * channels, -1),
        initial_state, notes,
        name="local",
    )
    inner, message = call(
        plane_kernel,
        [((48, 128), F32), ((planes, 16, 128), BF16)],
        exchange(message, inner_axes), consts,
        name="plane",
    )
    got = exchange(message, SP[0])
    (partial,) = call(
        finish_kernel,
        [((parts, n, share), BF16)],
        got, inner, consts, hr, hi, cr, ci, pr, pi, br, bi,
        read_real.reshape(2 * channels, -1), read_imag.reshape(2 * channels, -1), source, gate, state,
        proj_conv, proj_state,
        name="finish",
    )
    arrived = exchange(partial, "tp")
    return arrived.astype(F32).sum(axis=0).astype(BF16)


def solution(mesh):
    finer = Mesh(mesh.devices.reshape(16, 4, 2, mesh.shape["tp"]), ("sp_0", "sp_1", "sp_2", "tp"))
    return jax.shard_map(
        per_device,
        mesh=finer,
        in_specs=(
            P(SP, "tp"),
            P("tp"),
            P(None, "tp"),
            P(None, "tp"),
            P(None, "tp"),
            P(None, "tp"),
            P(None, "tp"),
            P("tp"),
            P(None, "tp", None),
            P(None, "tp", None),
            P(None, "tp", None, None),
            P(None, "tp", None, None),
            P(None, "tp", None, None),
            P(None, "tp", None, None),
            P(None, None, "tp", None),
            P(SP),
            P("tp", None),
            P("tp", None),
        ),
        out_specs=P(SP, "tp"),
        check_vma=False,
    )
```

```python
import jax
import jax.numpy as jnp
from jax import lax
from jax.experimental import pallas as pl
from jax.experimental.pallas import tpu as pltpu
from jax.sharding import Mesh
from jax.sharding import PartitionSpec as P

D = 2048
SP = ("sp_0", "sp_1", "sp_2")
EPSILON = 1e-06
F32 = jnp.float32
BF16 = jnp.bfloat16
CHUNKS = 8


def turned(half_turn, elapsed):
    half = half_turn * elapsed
    turns = jnp.round(half * 0.3183098861837907)
    rest = jnp.clip((half - turns * 3.140625) - turns * 9.67653589793e-4, -1.6, 1.6)
    square = rest * rest
    sine = rest + rest * (square * (-0.16666659712791443 + square * (0.008333086036145687 + square * (-0.0001981096138479188 + square * 2.6085685931320768e-06))))
    cosine = 1.0 + square * (-0.4999993145465851 + square * (0.04166397079825401 + square * (-0.0013855763245373964 + square * 2.3190419597085565e-05)))
    double = sine + sine
    fall = double * sine
    return double * cosine, 1.0 - fall, fall


def turned_briefly(rate, elapsed):
    turns = rate * elapsed
    rest = turns - jnp.round(turns)
    square = rest * rest
    sine = rest * (4.442883014678955 + square * (-7.308244228363037 + square * (3.606335163116455 + square * (-0.846008837223053 + square * 0.10963883250951767))))
    cosine = 1.4142135381698608 + square * (-6.978850841522217 + square * (5.7394561767578125 + square * (-1.8835265636444092 + square * 0.3106144070625305)))
    fall = sine * sine
    return sine * cosine, 1.0 - fall, fall


def damped(half_rate, elapsed):
    x = half_rate * elapsed
    root = jnp.exp(-x)
    magnitude = root * root
    square = x * x
    series = root * (x * (-2.0 - square * (1 / 3 + square * (1 / 60))))
    return magnitude, jnp.where(x < 0.25, series, magnitude - 1.0)


def moved(elapsed, rate, half_turn):
    magnitude = jnp.exp(-rate * elapsed)
    sine, cosine, _ = turned(half_turn, elapsed)
    return magnitude * cosine, magnitude * sine


def cmul(ar, ai, br, bi):
    return ar * br - ai * bi, ar * bi + ai * br


def iota(shape, dim):
    return lax.broadcasted_iota(jnp.int32, shape, dim)


def dot(a, b, dims=((1,), (0,))):
    return lax.dot_general(a, b, (dims, ((), ())), preferred_element_type=F32)


def halves(x):
    high = x.astype(BF16)
    return high, (x - high.astype(F32)).astype(BF16)


def scan_chunks(fr, fi, lr, li, backward):
    rows = iota(fr.shape, 0)
    for k in (1, 2, 4):
        shift = CHUNKS - k if backward else k
        outside = rows >= CHUNKS - k if backward else rows < k
        sfr = jnp.where(outside, 1.0, pltpu.roll(fr, shift, 0))
        sfi = jnp.where(outside, 0.0, pltpu.roll(fi, shift, 0))
        if lr is not None:
            slr = jnp.where(outside, 0.0, pltpu.roll(lr, shift, 0))
            sli = jnp.where(outside, 0.0, pltpu.roll(li, shift, 0))
            ar, ai = cmul(fr, fi, slr, sli)
            lr, li = lr + ar, li + ai
        fr, fi = cmul(fr, fi, sfr, sfi)
    return fr, fi, lr, li


def one_later(x, backward, fill):
    rows = iota(x.shape, 0)
    if backward:
        return jnp.where(rows == CHUNKS - 1, fill, pltpu.roll(x, CHUNKS - 1, 0))
    return jnp.where(rows == 0, fill, pltpu.roll(x, 1, 0))


def lead_kernel(out):
    out[...] = jnp.zeros(out.shape, F32)


def pack_kernel(stream, gain, intervals, taps, skip, blank, out, notes):
    n, share = stream.shape
    row = iota((8, share), 0)
    tail = jnp.zeros((8, share), F32)
    for at, x in enumerate((gain[...], jnp.concatenate([intervals[...]] * (share // n), axis=1))):
        high = x.astype(BF16).astype(F32)
        mid = (x - high).astype(BF16).astype(F32)
        for p, piece in enumerate((high, mid, x - high - mid)):
            tail = jnp.where(row == 3 * at + p, piece, tail)
    tail = tail.astype(BF16)
    for k in range(out.shape[0]):
        out[k, 0:n, :] = stream[...]
        out[k, n : n + 8, :] = tail
    notes[...] = blank[...]
    notes[0:3, :] = taps[...]
    notes[3:4, :] = skip[...]


def row_of(ref, d, q):
    return jnp.concatenate([ref[d, 2 * q : 2 * q + 1, :], ref[d, 2 * q + 1 : 2 * q + 2, :]], axis=1)


def doubled(x):
    return jnp.concatenate([x, x], axis=1)


def local_kernel(rows, w_value, w_mix, w_gate, w_state, decay, turn, in_re, in_im, init, notes, ur_o, ui_o, cr_o, ci_o, fr_o, fi_o, br_o, bi_o, source_o, gate_o, input_o, consts, message, lift_s, er_s, ei_s):
    parts, n, share = rows.shape[0], rows.shape[1] - 8, rows.shape[2]
    per = n // CHUNKS
    channels = w_value.shape[1]
    groups, states = decay.shape[1], decay.shape[2]
    wide = channels // groups
    pairs = groups // 2
    tiles = 2 * pairs
    row, col = iota((n, n), 0), iota((n, n), 1)
    ordered = col == (row % CHUNKS) * per + row // CHUNKS
    tail = rows[0, n : n + 8, 0:n].astype(F32)
    intervals = (tail[3:4] + tail[4:5]) + tail[5:6]
    steps = jnp.sum(jnp.where(ordered, intervals, 0.0), axis=1, keepdims=True)
    total = jnp.sum(intervals, axis=1, keepdims=True)
    elapsed = sum(steps[i * CHUNKS : i * CHUNKS + CHUNKS] for i in range(per))
    order = jnp.where(ordered, 1.0, 0.0).astype(BF16)
    consts[32:40, :] = notes[...]

    def lanes_of(tile):
        return slice(tile * 128, tile * 128 + 128)

    def chunk_rows(tile):
        return [slice(i * CHUNKS, i * CHUNKS + CHUNKS) for i in (reversed(range(per)) if tile >= pairs else range(per))]

    def tabulate(tile):
        d, q = tile // pairs, tile % pairs
        lanes = lanes_of(tile)
        rate, half_turn = row_of(decay, d, q), 0.5 * row_of(turn, d, q)
        consts[tile : tile + 1, :] = rate
        consts[8 + tile : 9 + tile, :] = half_turn
        for part in range(2):
            pair = [init[d, part, 2 * q + k : 2 * q + k + 1, :] for k in range(2)]
            consts[16 + 8 * part + tile : 17 + 8 * part + tile, :] = jnp.concatenate(pair, axis=1)
        sine, cosine, fall = turned_briefly(half_turn * 0.3183098861837907, steps)
        magnitude, less_one = damped(0.5 * rate, steps)
        fr_o[:, lanes] = magnitude * cosine
        fi_o[:, lanes] = magnitude * sine
        lift_s[:, lanes] = less_one * cosine - fall
        er, ei = moved(elapsed, rate, half_turn)
        er_s[:, lanes] = er
        ei_s[:, lanes] = ei
        br, bi, _, _ = scan_chunks(er, ei, None, None, tile >= pairs)
        br_o[:, lanes] = one_later(br, tile >= pairs, 1.0)
        bi_o[:, lanes] = one_later(bi, tile >= pairs, 0.0)

    squares = 0.0
    for k in range(parts):
        x = rows[k, 0:n, :].astype(F32)
        squares = squares + jnp.sum(x * x, axis=1, keepdims=True)
    inv_rms = lax.rsqrt(squares / D + EPSILON)
    first = second = 0.0
    for k in range(parts):
        tail = rows[k, n : n + 8, :].astype(F32)
        gain = (tail[0:1] + tail[1:2]) + tail[2:3]
        normed = ((rows[k, 0:n, :].astype(F32) * inv_rms) * gain).astype(BF16)
        at = slice(k * share, k * share + share)
        first = first + dot(normed, jnp.concatenate([w_value[at, :], w_mix[at, :]], axis=1))
        second = second + dot(normed, jnp.concatenate([w_gate[at, :], w_state[at, :]], axis=1))
        for tile in range(k * tiles // parts, (k + 1) * tiles // parts):
            tabulate(tile)
    first = dot(order, first.astype(BF16))
    second = dot(order, second.astype(BF16))
    source = (first[:, :channels] * first[:, channels:]).astype(BF16).astype(F32)
    source_o[...] = source
    gate_o[...] = second[:, :channels]
    input_o[...] = second[:, channels:]
    state = second[:, channels:].astype(BF16)

    block = 2 * wide
    edges = []
    for d in range(2):
        backward = d == 1
        rates, turns = decay[d], turn[d]
        inverse = 1.0 / (rates * rates + turns * turns)
        inv_re = jnp.broadcast_to((-rates * inverse)[:, None, :], (groups, wide, states)).reshape(channels, states)
        inv_im = jnp.broadcast_to((-turns * inverse)[:, None, :], (groups, wide, states)).reshape(channels, states)
        at = slice(d * channels, d * channels + channels)
        scaled_re, scaled_im = cmul(in_re[at, :], in_im[at, :], inv_re, inv_im)
        scaled = (doubled(scaled_re), doubled(scaled_im))
        mine = iota((block, 128), 0) // wide == iota((block, 128), 1) // states
        for q in range(pairs):
            tile = d * pairs + q
            lanes = lanes_of(tile)
            some = slice(q * block, q * block + block)
            matrix = jnp.concatenate([jnp.concatenate(halves(jnp.where(mine, x[some], 0.0)), axis=0) for x in scaled], axis=1)
            driven = dot(jnp.concatenate([state[:, some], state[:, some]], axis=1), matrix)
            fr, fi = fr_o[:, lanes], fi_o[:, lanes]
            push_re, push_im = cmul(lift_s[:, lanes], fi, driven[:, :128], driven[:, 128:])
            ur_o[:, lanes] = push_re
            ui_o[:, lanes] = push_im
            hr = hi = None
            for at in chunk_rows(tile):
                if hr is None:
                    hr, hi = push_re[at], push_im[at]
                else:
                    ar, ai = cmul(fr[at], fi[at], hr, hi)
                    hr, hi = ar + push_re[at], ai + push_im[at]
            _, _, lr, li = scan_chunks(er_s[:, lanes], ei_s[:, lanes], hr, hi, backward)
            cr_o[:, lanes] = one_later(lr, backward, 0.0)
            ci_o[:, lanes] = one_later(li, backward, 0.0)
            edge = 0 if backward else CHUNKS - 1
            edges.append((lr[edge : edge + 1], li[edge : edge + 1]))
    for k in range(message.shape[0]):
        for tile, (r, m) in enumerate(edges):
            message[k, tile : tile + 1, :] = r
            message[k, 8 + tile : 9 + tile, :] = m
        message[k, 16:17, :] = jnp.broadcast_to(total, (1, 128))
        message[k, 17:18, :] = source[0:1]
        message[k, 18:19, :] = source[n - 1 : n]
        message[k, 19:24, :] = jnp.zeros((5, 128), F32)


def plane_kernel(got, consts, inner, message):
    size = got.shape[0]
    here, plane = lax.axis_index(SP[1:]), lax.axis_index(SP[0])
    rate, turning = consts[0:8, :], consts[8:16, :]
    forward = iota((8, 128), 0) < 4
    hr = hi = spent = jnp.zeros((8, 128), F32)
    ir = ii = before = hr
    for k in range(size):
        m = size - 1 - k
        mine = (forward & (here == k)) | (jnp.logical_not(forward) & (here == m))
        ir = jnp.where(mine, hr, ir)
        ii = jnp.where(mine, hi, ii)
        before = jnp.where(mine, spent, before)
        elapsed = jnp.where(forward, got[k, 16:17, :], got[m, 16:17, :])
        ar, ai = moved(elapsed, rate, turning)
        ar, ai = cmul(ar, ai, hr, hi)
        hr = ar + jnp.where(forward, got[k, 0:8, :], got[m, 0:8, :])
        hi = ai + jnp.where(forward, got[k, 8:16, :], got[m, 8:16, :])
        spent = spent + elapsed
    wr, wi = moved(before, rate, turning)
    inner[0:8, :] = ir
    inner[8:16, :] = ii
    inner[16:24, :] = wr
    inner[24:32, :] = wi
    previous = following = jnp.zeros((1, 128), F32)
    for k in range(size):
        previous = jnp.where(here - 1 == k, got[k, 18:19, :], previous)
        following = jnp.where(here + 1 == k, got[k, 17:18, :], following)
    inner[32:40, :] = jnp.broadcast_to(previous, (8, 128))
    inner[40:48, :] = jnp.broadcast_to(following, (8, 128))
    swapped = pltpu.roll(hi, 4, 0)
    later = jnp.where(forward, hr, swapped)
    earlier = jnp.where(forward, swapped, hr)
    row = iota((8, 128), 0)
    high = spent.astype(BF16).astype(F32)
    mid = (spent - high).astype(BF16).astype(F32)
    note = jnp.where(row == 0, high, jnp.where(row == 1, mid, jnp.where(row == 2, spent - high - mid, 0.0)))
    note_later = jnp.where(row == 3, got[size - 1, 18:19, :], note)
    note_earlier = jnp.where(row == 3, got[0, 17:18, :], note)
    later = jnp.concatenate([later, note_later], axis=0)
    earlier = jnp.concatenate([earlier, note_earlier], axis=0)
    for k in range(message.shape[0]):
        message[k] = jnp.where(plane < k, later, earlier).astype(BF16)


def finish_kernel(got, inner, consts, ur, ui, cr_i, ci_i, fr, fi, br, bi, rd_re, rd_im, source, gate, state, proj_conv, proj_state, out):
    size = got.shape[0]
    here, plane = lax.axis_index(SP[1:]), lax.axis_index(SP[0])
    last = lax.axis_size(SP[1:]) - 1
    rate, turning = consts[0:8, :], consts[8:16, :]
    forward = iota((8, 128), 0) < 4
    hr, hi = consts[16:24, :], consts[24:32, :]
    arrived = [got[k].astype(F32) for k in range(size)]
    times = [(x[8:9] + x[9:10]) + x[10:11] for x in arrived]
    for k in range(size):
        m = size - 1 - k
        active = (forward & (plane > k)) | (jnp.logical_not(forward) & (plane < m))
        elapsed = jnp.where(forward, times[k], times[m])
        ar, ai = moved(elapsed, rate, turning)
        ar, ai = cmul(ar, ai, hr, hi)
        a, b = arrived[k][0:8], arrived[m][0:8]
        hr = jnp.where(active, ar + jnp.where(forward, a, b), hr)
        hi = jnp.where(active, ai + pltpu.roll(jnp.where(forward, b, a), 4, 0), hi)
    ar, ai = cmul(inner[16:24, :], inner[24:32, :], hr, hi)
    inc_re = ar + inner[0:8, :]
    inc_im = ai + inner[8:16, :]
    n, width = ur.shape
    per = n // CHUNKS
    channels = rd_re.shape[0] // 2
    states = rd_re.shape[1]
    pairs = width // 256
    block = channels // pairs
    wide = block // 2
    responses = []
    for q in range(pairs):
        mine = iota((block, 128), 0) // wide == iota((block, 128), 1) // states
        full, matrix = [], []
        for d in range(2):
            tile = d * pairs + q
            lanes = slice(tile * 128, tile * 128 + 128)
            er, ei = cmul(br[:, lanes], bi[:, lanes], inc_re[tile : tile + 1], inc_im[tile : tile + 1])
            hr, hi = er + cr_i[:, lanes], ei + ci_i[:, lanes]
            history = [None] * per
            for i in reversed(range(per)) if d == 1 else range(per):
                at = slice(i * CHUNKS, i * CHUNKS + CHUNKS)
                ar, ai = cmul(fr[at, lanes], fi[at, lanes], hr, hi)
                hr, hi = ar + ur[at, lanes], ai + ui[at, lanes]
                history[i] = (hr, hi)
            full += [jnp.concatenate([x[part] for x in history], axis=0) for part in range(2)]
            at = slice(d * channels + q * block, d * channels + (q + 1) * block)
            matrix += [jnp.where(mine, doubled(rd_re[at, :]), 0.0), jnp.where(mine, -doubled(rd_im[at, :]), 0.0)]
        high, low = halves(jnp.concatenate(full, axis=1))
        r_hi, r_lo = halves(jnp.concatenate(matrix, axis=1))
        across = ((1,), (1,))
        responses.append((dot(low, r_hi, across) + dot(high, r_lo, across)) + dot(high, r_hi, across))
    response = state[...] * consts[35:36, :] + jnp.concatenate(responses, axis=1)
    state_out = jax.nn.gelu(response).astype(BF16)
    previous, following = inner[32:33, :], inner[40:41, :]
    for k in range(size):
        previous = jnp.where((here == 0) & (plane - 1 == k), arrived[k][11:12], previous)
        following = jnp.where((here == last) & (plane + 1 == k), arrived[k][11:12], following)
    x = source[...]
    row = iota((CHUNKS, x.shape[1]), 0)
    head = jnp.where(row == 0, previous, pltpu.roll(x[n - CHUNKS :], 1, 0))
    foot = jnp.where(row == CHUNKS - 1, following, pltpu.roll(x[:CHUNKS], CHUNKS - 1, 0))
    before = jnp.concatenate([head, x[: n - CHUNKS]], axis=0)
    after = jnp.concatenate([x[CHUNKS:], foot], axis=0)
    filtered = consts[32:33, :] * before + consts[33:34, :] * x + consts[34:35, :] * after
    conv_out = (gate[...] * filtered).astype(BF16)
    row, col = iota((n, n), 0), iota((n, n), 1)
    order = jnp.where(row == (col % CHUNKS) * per + col // CHUNKS, 1.0, 0.0).astype(BF16)
    conv_out = dot(order, conv_out).astype(BF16)
    state_out = dot(order, state_out).astype(BF16)
    share = out.shape[2]
    for k in range(out.shape[0]):
        at = slice(k * share, k * share + share)
        out[k] = (dot(conv_out, proj_conv[:, at]) + dot(state_out, proj_state[:, at])).astype(BF16)


def exchange(x, axis):
    return lax.all_to_all(x, axis, split_axis=0, concat_axis=0, tiled=True)


VMEM = pl.BlockSpec(memory_space=pltpu.VMEM)


def call(kernel, shapes, *args, scratch=(), bytes_moved=10**6, name=None):
    return pl.pallas_call(
        kernel,
        out_shape=[jax.ShapeDtypeStruct(s, d) for s, d in shapes],
        in_specs=[VMEM] * len(args),
        out_specs=[VMEM] * len(shapes),
        scratch_shapes=scratch,
        compiler_params=pltpu.CompilerParams(vmem_limit_bytes=24 * 2**20),
        cost_estimate=pl.CostEstimate(flops=10**9, bytes_accessed=bytes_moved, transcendentals=0),
        name=name,
    )(*args)


def per_device(
    stream,
    norm_gain,
    w_value,
    w_mix,
    w_gate,
    w_state,
    conv_taps,
    skip_gain,
    decay_rate,
    turn_rate,
    input_real,
    input_imag,
    read_real,
    read_imag,
    initial_state,
    intervals,
    proj_conv,
    proj_state,
):
    n, share = stream.shape
    parts = lax.axis_size("tp")
    inner_axes = SP[1:]
    inside = lax.axis_size(inner_axes)
    planes = lax.axis_size(SP[0])
    channels = w_value.shape[1]
    width = decay_rate.size
    (blank,) = call(lead_kernel, [((8, channels), F32)], bytes_moved=3 * 10**8, name="lead")
    packed, notes = call(
        pack_kernel,
        [((parts, n + 8, share), BF16), ((8, channels), F32)],
        stream, norm_gain.reshape(1, -1), intervals.reshape(1, n), conv_taps, skip_gain.reshape(1, -1), blank,
        bytes_moved=3 * 10**8,
        name="pack",
    )
    rows = exchange(packed, "tp")

    states = ((n, width), F32)
    chunks = ((CHUNKS, width), F32)
    mixed = ((n, channels), F32)
    ur, ui, cr, ci, fr, fi, br, bi, source, gate, state, consts, message = call(
        local_kernel,
        [states, states, chunks, chunks, states, states, chunks, chunks, mixed, mixed, mixed]
        + [((40, channels), F32), ((inside, 24, 128), F32)],
        rows, w_value, w_mix, w_gate, w_state, decay_rate, turn_rate,
        jnp.swapaxes(input_real, 2, 3).reshape(2 * channels, -1),
        jnp.swapaxes(input_imag, 2, 3).reshape(2 * channels, -1),
        initial_state, notes,
        scratch=[pltpu.VMEM((n, width), F32)] + [pltpu.VMEM((CHUNKS, width), F32)] * 2,
        name="local",
    )
    inner, message = call(
        plane_kernel,
        [((48, 128), F32), ((planes, 16, 128), BF16)],
        exchange(message, inner_axes), consts,
        name="plane",
    )
    got = exchange(message, SP[0])
    (partial,) = call(
        finish_kernel,
        [((parts, n, share), BF16)],
        got, inner, consts, ur, ui, cr, ci, fr, fi, br, bi,
        read_real.reshape(2 * channels, -1), read_imag.reshape(2 * channels, -1), source, gate, state,
        proj_conv, proj_state,
        name="finish",
    )
    arrived = exchange(partial, "tp")
    return arrived.astype(F32).sum(axis=0).astype(BF16)


def solution(mesh):
    finer = Mesh(mesh.devices.reshape(16, 4, 2, mesh.shape["tp"]), ("sp_0", "sp_1", "sp_2", "tp"))
    return jax.shard_map(
        per_device,
        mesh=finer,
        in_specs=(
            P(SP, "tp"),
            P("tp"),
            P(None, "tp"),
            P(None, "tp"),
            P(None, "tp"),
            P(None, "tp"),
            P(None, "tp"),
            P("tp"),
            P(None, "tp", None),
            P(None, "tp", None),
            P(None, "tp", None, None),
            P(None, "tp", None, None),
            P(None, "tp", None, None),
            P(None, "tp", None, None),
            P(None, None, "tp", None),
            P(SP),
            P("tp", None),
            P("tp", None),
        ),
        out_specs=P(SP, "tp"),
        check_vma=False,
    )
```

```python
import jax
import jax.numpy as jnp
from jax import lax
from jax.experimental import pallas as pl
from jax.experimental.pallas import tpu as pltpu
from jax.sharding import Mesh
from jax.sharding import PartitionSpec as P

D = 2048
SP = ("sp_0", "sp_1", "sp_2")
EPSILON = 1e-06
F32 = jnp.float32
BF16 = jnp.bfloat16
CHUNKS = 8


def turned(half_turn, elapsed):
    half = half_turn * elapsed
    turns = jnp.round(half * 0.3183098861837907)
    rest = jnp.clip((half - turns * 3.140625) - turns * 9.67653589793e-4, -1.6, 1.6)
    square = rest * rest
    sine = rest + rest * (square * (-0.16666659712791443 + square * (0.008333086036145687 + square * (-0.0001981096138479188 + square * 2.6085685931320768e-06))))
    cosine = 1.0 + square * (-0.4999993145465851 + square * (0.04166397079825401 + square * (-0.0013855763245373964 + square * 2.3190419597085565e-05)))
    double = sine + sine
    fall = double * sine
    return double * cosine, 1.0 - fall, fall


def turned_briefly(rate, elapsed):
    turns = rate * elapsed
    rest = turns - jnp.round(turns)
    square = rest * rest
    sine = rest * (4.442883014678955 + square * (-7.308244228363037 + square * (3.606335163116455 + square * (-0.846008837223053 + square * 0.10963883250951767))))
    cosine = 1.4142135381698608 + square * (-6.978850841522217 + square * (5.7394561767578125 + square * (-1.8835265636444092 + square * 0.3106144070625305)))
    fall = sine * sine
    return sine * cosine, 1.0 - fall, fall


def damped(half_rate, elapsed):
    x = half_rate * elapsed
    root = jnp.exp(-x)
    magnitude = root * root
    square = x * x
    series = root * (x * (-2.0 - square * (1 / 3 + square * (1 / 60))))
    return magnitude, jnp.where(x < 0.25, series, magnitude - 1.0)


def moved(elapsed, rate, half_turn):
    magnitude = jnp.exp(-rate * elapsed)
    sine, cosine, _ = turned(half_turn, elapsed)
    return magnitude * cosine, magnitude * sine


def cmul(ar, ai, br, bi):
    return ar * br - ai * bi, ar * bi + ai * br


def iota(shape, dim):
    return lax.broadcasted_iota(jnp.int32, shape, dim)


def dot(a, b, dims=((1,), (0,))):
    return lax.dot_general(a, b, (dims, ((), ())), preferred_element_type=F32)


def halves(x):
    high = x.astype(BF16)
    return high, (x - high.astype(F32)).astype(BF16)


def scan_chunks(fr, fi, lr, li, backward):
    rows = iota(fr.shape, 0)
    for k in (1, 2, 4):
        shift = CHUNKS - k if backward else k
        outside = rows >= CHUNKS - k if backward else rows < k
        sfr = jnp.where(outside, 1.0, pltpu.roll(fr, shift, 0))
        sfi = jnp.where(outside, 0.0, pltpu.roll(fi, shift, 0))
        if lr is not None:
            slr = jnp.where(outside, 0.0, pltpu.roll(lr, shift, 0))
            sli = jnp.where(outside, 0.0, pltpu.roll(li, shift, 0))
            ar, ai = cmul(fr, fi, slr, sli)
            lr, li = lr + ar, li + ai
        fr, fi = cmul(fr, fi, sfr, sfi)
    return fr, fi, lr, li


def one_later(x, backward, fill):
    rows = iota(x.shape, 0)
    if backward:
        return jnp.where(rows == CHUNKS - 1, fill, pltpu.roll(x, CHUNKS - 1, 0))
    return jnp.where(rows == 0, fill, pltpu.roll(x, 1, 0))


def lead_kernel(out):
    out[...] = jnp.zeros(out.shape, F32)


def pack_kernel(stream, gain, intervals, taps, skip, blank, out, notes):
    n, share = stream.shape
    row = iota((8, share), 0)
    tail = jnp.zeros((8, share), F32)
    for at, x in enumerate((gain[...], jnp.concatenate([intervals[...]] * (share // n), axis=1))):
        high = x.astype(BF16).astype(F32)
        mid = (x - high).astype(BF16).astype(F32)
        for p, piece in enumerate((high, mid, x - high - mid)):
            tail = jnp.where(row == 3 * at + p, piece, tail)
    tail = tail.astype(BF16)
    for k in range(out.shape[0]):
        out[k, 0:n, :] = stream[...]
        out[k, n : n + 8, :] = tail
    notes[...] = blank[...]
    notes[0:3, :] = taps[...]
    notes[3:4, :] = skip[...]


def row_of(ref, d, q):
    return jnp.concatenate([ref[d, 2 * q : 2 * q + 1, :], ref[d, 2 * q + 1 : 2 * q + 2, :]], axis=1)


def doubled(x):
    return jnp.concatenate([x, x], axis=1)


def local_kernel(rows, w_value, w_mix, w_gate, w_state, decay, turn, in_re, in_im, init, notes, ur_o, ui_o, cr_o, ci_o, fr_o, fi_o, br_o, bi_o, source_o, gate_o, input_o, consts, message, lift_s, er_s, ei_s):
    parts, n, share = rows.shape[0], rows.shape[1] - 8, rows.shape[2]
    per = n // CHUNKS
    channels = w_value.shape[1]
    groups, states = decay.shape[1], decay.shape[2]
    wide = channels // groups
    pairs = groups // 2
    tiles = 2 * pairs
    row, col = iota((n, n), 0), iota((n, n), 1)
    ordered = col == (row % CHUNKS) * per + row // CHUNKS
    tail = rows[0, n : n + 8, 0:n].astype(F32)
    intervals = (tail[3:4] + tail[4:5]) + tail[5:6]
    steps = jnp.sum(jnp.where(ordered, intervals, 0.0), axis=1, keepdims=True)
    total = jnp.sum(intervals, axis=1, keepdims=True)
    elapsed = sum(steps[i * CHUNKS : i * CHUNKS + CHUNKS] for i in range(per))
    order = jnp.where(ordered, 1.0, 0.0).astype(BF16)
    consts[32:40, :] = notes[...]

    def lanes_of(tile):
        return slice(tile * 128, tile * 128 + 128)

    def chunk_rows(tile):
        return [slice(i * CHUNKS, i * CHUNKS + CHUNKS) for i in (reversed(range(per)) if tile >= pairs else range(per))]

    def tabulate(tile):
        d, q = tile // pairs, tile % pairs
        lanes = lanes_of(tile)
        rate, half_turn = row_of(decay, d, q), 0.5 * row_of(turn, d, q)
        consts[tile : tile + 1, :] = rate
        consts[8 + tile : 9 + tile, :] = half_turn
        for part in range(2):
            pair = [init[d, part, 2 * q + k : 2 * q + k + 1, :] for k in range(2)]
            consts[16 + 8 * part + tile : 17 + 8 * part + tile, :] = jnp.concatenate(pair, axis=1)
        sine, cosine, fall = turned_briefly(half_turn * 0.3183098861837907, steps)
        magnitude, less_one = damped(0.5 * rate, steps)
        fr_o[:, lanes] = magnitude * cosine
        fi_o[:, lanes] = magnitude * sine
        lift_s[:, lanes] = less_one * cosine - fall
        er, ei = moved(elapsed, rate, half_turn)
        er_s[:, lanes] = er
        ei_s[:, lanes] = ei
        br, bi, _, _ = scan_chunks(er, ei, None, None, tile >= pairs)
        br_o[:, lanes] = one_later(br, tile >= pairs, 1.0)
        bi_o[:, lanes] = one_later(bi, tile >= pairs, 0.0)

    squares = 0.0
    for k in range(parts):
        x = rows[k, 0:n, :].astype(F32)
        squares = squares + jnp.sum(x * x, axis=1, keepdims=True)
    inv_rms = lax.rsqrt(squares / D + EPSILON)
    first = second = 0.0
    for k in range(parts):
        tail = rows[k, n : n + 8, :].astype(F32)
        gain = (tail[0:1] + tail[1:2]) + tail[2:3]
        normed = ((rows[k, 0:n, :].astype(F32) * inv_rms) * gain).astype(BF16)
        at = slice(k * share, k * share + share)
        first = first + dot(normed, jnp.concatenate([w_value[at, :], w_mix[at, :]], axis=1))
        second = second + dot(normed, jnp.concatenate([w_gate[at, :], w_state[at, :]], axis=1))
        for tile in range(k * tiles // parts, (k + 1) * tiles // parts):
            tabulate(tile)
    first = dot(order, first.astype(BF16))
    second = dot(order, second.astype(BF16))
    source = (first[:, :channels] * first[:, channels:]).astype(BF16).astype(F32)
    source_o[...] = source
    gate_o[...] = second[:, :channels]
    input_o[...] = second[:, channels:]
    state = second[:, channels:].astype(BF16)

    block = 2 * wide
    edges = []
    for d in range(2):
        backward = d == 1
        rates, turns = decay[d], turn[d]
        inverse = 1.0 / (rates * rates + turns * turns)
        inv_re = jnp.broadcast_to((-rates * inverse)[:, None, :], (groups, wide, states)).reshape(channels, states)
        inv_im = jnp.broadcast_to((-turns * inverse)[:, None, :], (groups, wide, states)).reshape(channels, states)
        at = slice(d * channels, d * channels + channels)
        scaled_re, scaled_im = cmul(in_re[at, :], in_im[at, :], inv_re, inv_im)
        scaled = (doubled(scaled_re), doubled(scaled_im))
        mine = iota((block, 128), 0) // wide == iota((block, 128), 1) // states
        for q in range(pairs):
            tile = d * pairs + q
            lanes = lanes_of(tile)
            some = slice(q * block, q * block + block)
            matrix = jnp.concatenate([jnp.concatenate(halves(jnp.where(mine, x[some], 0.0)), axis=0) for x in scaled], axis=1)
            driven = dot(jnp.concatenate([state[:, some], state[:, some]], axis=1), matrix)
            fr, fi = fr_o[:, lanes], fi_o[:, lanes]
            push_re, push_im = cmul(lift_s[:, lanes], fi, driven[:, :128], driven[:, 128:])
            ur_o[:, lanes] = push_re
            ui_o[:, lanes] = push_im
            hr = hi = None
            for at in chunk_rows(tile):
                if hr is None:
                    hr, hi = push_re[at], push_im[at]
                else:
                    ar, ai = cmul(fr[at], fi[at], hr, hi)
                    hr, hi = ar + push_re[at], ai + push_im[at]
            _, _, lr, li = scan_chunks(er_s[:, lanes], ei_s[:, lanes], hr, hi, backward)
            cr_o[:, lanes] = one_later(lr, backward, 0.0)
            ci_o[:, lanes] = one_later(li, backward, 0.0)
            edge = 0 if backward else CHUNKS - 1
            edges.append((lr[edge : edge + 1], li[edge : edge + 1]))
    high = total.astype(BF16).astype(F32)
    mid = (total - high).astype(BF16).astype(F32)
    lines = [r for r, m in edges] + [m for r, m in edges]
    lines += [jnp.broadcast_to(x, (1, 128)) for x in (high, mid, total - high - mid)]
    lines += [source[0:1], source[n - 1 : n], jnp.zeros((3, 128), F32)]
    lines = jnp.concatenate(lines, axis=0).astype(BF16)
    for k in range(message.shape[0]):
        message[k] = lines


def plane_kernel(got, consts, inner, message):
    size = got.shape[0]
    came = [got[k].astype(F32) for k in range(size)]
    times = [(x[16:17] + x[17:18]) + x[18:19] for x in came]
    here, plane = lax.axis_index(SP[1:]), lax.axis_index(SP[0])
    rate, turning = consts[0:8, :], consts[8:16, :]
    forward = iota((8, 128), 0) < 4
    hr = hi = spent = jnp.zeros((8, 128), F32)
    ir = ii = before = hr
    for k in range(size):
        m = size - 1 - k
        mine = (forward & (here == k)) | (jnp.logical_not(forward) & (here == m))
        ir = jnp.where(mine, hr, ir)
        ii = jnp.where(mine, hi, ii)
        before = jnp.where(mine, spent, before)
        elapsed = jnp.where(forward, times[k], times[m])
        ar, ai = moved(elapsed, rate, turning)
        ar, ai = cmul(ar, ai, hr, hi)
        hr = ar + jnp.where(forward, came[k][0:8], came[m][0:8])
        hi = ai + jnp.where(forward, came[k][8:16], came[m][8:16])
        spent = spent + elapsed
    wr, wi = moved(before, rate, turning)
    inner[0:8, :] = ir
    inner[8:16, :] = ii
    inner[16:24, :] = wr
    inner[24:32, :] = wi
    previous = following = jnp.zeros((1, 128), F32)
    for k in range(size):
        previous = jnp.where(here - 1 == k, came[k][20:21], previous)
        following = jnp.where(here + 1 == k, came[k][19:20], following)
    inner[32:40, :] = jnp.broadcast_to(previous, (8, 128))
    inner[40:48, :] = jnp.broadcast_to(following, (8, 128))
    high = spent[0:1].astype(BF16).astype(F32)
    mid = (spent[0:1] - high).astype(BF16).astype(F32)
    note = [high, mid, spent[0:1] - high - mid]
    note_later = jnp.concatenate(note + [came[size - 1][20:21]], axis=0)
    note_earlier = jnp.concatenate(note + [came[0][19:20]], axis=0)
    later = jnp.concatenate([hr[0:4], hi[0:4], note_later], axis=1)
    earlier = jnp.concatenate([hr[4:8], hi[4:8], note_earlier], axis=1)
    for k in range(message.shape[0]):
        message[k] = jnp.where(plane < k, later, earlier).astype(BF16)


def finish_kernel(got, inner, consts, ur, ui, cr_i, ci_i, fr, fi, br, bi, rd_re, rd_im, source, gate, state, proj_conv, proj_state, out):
    size = got.shape[0]
    here, plane = lax.axis_index(SP[1:]), lax.axis_index(SP[0])
    last = lax.axis_size(SP[1:]) - 1
    rate, turning = consts[0:8, :], consts[8:16, :]
    forward = iota((8, 128), 0) < 4
    hr, hi = consts[16:24, :], consts[24:32, :]
    arrived = [got[k].astype(F32) for k in range(size)]
    times = [(x[0:1, 256:] + x[1:2, 256:]) + x[2:3, 256:] for x in arrived]
    for k in range(size):
        m = size - 1 - k
        active = (forward & (plane > k)) | (jnp.logical_not(forward) & (plane < m))
        elapsed = jnp.where(forward, times[k], times[m])
        ar, ai = moved(elapsed, rate, turning)
        ar, ai = cmul(ar, ai, hr, hi)
        hr = jnp.where(active, ar + jnp.concatenate([arrived[k][:, :128], arrived[m][:, :128]], axis=0), hr)
        hi = jnp.where(active, ai + jnp.concatenate([arrived[k][:, 128:256], arrived[m][:, 128:256]], axis=0), hi)
    ar, ai = cmul(inner[16:24, :], inner[24:32, :], hr, hi)
    inc_re = ar + inner[0:8, :]
    inc_im = ai + inner[8:16, :]
    n, width = ur.shape
    per = n // CHUNKS
    channels = rd_re.shape[0] // 2
    states = rd_re.shape[1]
    pairs = width // 256
    block = channels // pairs
    wide = block // 2
    responses = []
    for q in range(pairs):
        mine = iota((block, 128), 0) // wide == iota((block, 128), 1) // states
        full, matrix = [], []
        for d in range(2):
            tile = d * pairs + q
            lanes = slice(tile * 128, tile * 128 + 128)
            er, ei = cmul(br[:, lanes], bi[:, lanes], inc_re[tile : tile + 1], inc_im[tile : tile + 1])
            hr, hi = er + cr_i[:, lanes], ei + ci_i[:, lanes]
            history = [None] * per
            for i in reversed(range(per)) if d == 1 else range(per):
                at = slice(i * CHUNKS, i * CHUNKS + CHUNKS)
                ar, ai = cmul(fr[at, lanes], fi[at, lanes], hr, hi)
                hr, hi = ar + ur[at, lanes], ai + ui[at, lanes]
                history[i] = (hr, hi)
            full += [jnp.concatenate([x[part] for x in history], axis=0) for part in range(2)]
            at = slice(d * channels + q * block, d * channels + (q + 1) * block)
            matrix += [jnp.where(mine, doubled(rd_re[at, :]), 0.0), jnp.where(mine, -doubled(rd_im[at, :]), 0.0)]
        high, low = halves(jnp.concatenate(full, axis=1))
        r_hi, r_lo = halves(jnp.concatenate(matrix, axis=1))
        across = ((1,), (1,))
        responses.append((dot(low, r_hi, across) + dot(high, r_lo, across)) + dot(high, r_hi, across))
    response = state[...] * consts[35:36, :] + jnp.concatenate(responses, axis=1)
    state_out = jax.nn.gelu(response).astype(BF16)
    previous, following = inner[32:33, :], inner[40:41, :]
    for k in range(size):
        previous = jnp.where((here == 0) & (plane - 1 == k), arrived[k][3:4, 256:], previous)
        following = jnp.where((here == last) & (plane + 1 == k), arrived[k][3:4, 256:], following)
    x = source[...]
    row = iota((CHUNKS, x.shape[1]), 0)
    head = jnp.where(row == 0, previous, pltpu.roll(x[n - CHUNKS :], 1, 0))
    foot = jnp.where(row == CHUNKS - 1, following, pltpu.roll(x[:CHUNKS], CHUNKS - 1, 0))
    before = jnp.concatenate([head, x[: n - CHUNKS]], axis=0)
    after = jnp.concatenate([x[CHUNKS:], foot], axis=0)
    filtered = consts[32:33, :] * before + consts[33:34, :] * x + consts[34:35, :] * after
    conv_out = (gate[...] * filtered).astype(BF16)
    row, col = iota((n, n), 0), iota((n, n), 1)
    order = jnp.where(row == (col % CHUNKS) * per + col // CHUNKS, 1.0, 0.0).astype(BF16)
    conv_out = dot(order, conv_out).astype(BF16)
    state_out = dot(order, state_out).astype(BF16)
    share = out.shape[2]
    for k in range(out.shape[0]):
        at = slice(k * share, k * share + share)
        out[k] = (dot(conv_out, proj_conv[:, at]) + dot(state_out, proj_state[:, at])).astype(BF16)


def exchange(x, axis):
    return lax.all_to_all(x, axis, split_axis=0, concat_axis=0, tiled=True)


VMEM = pl.BlockSpec(memory_space=pltpu.VMEM)


def call(kernel, shapes, *args, scratch=(), bytes_moved=10**6, name=None):
    return pl.pallas_call(
        kernel,
        out_shape=[jax.ShapeDtypeStruct(s, d) for s, d in shapes],
        in_specs=[VMEM] * len(args),
        out_specs=[VMEM] * len(shapes),
        scratch_shapes=scratch,
        compiler_params=pltpu.CompilerParams(vmem_limit_bytes=24 * 2**20),
        cost_estimate=pl.CostEstimate(flops=10**9, bytes_accessed=bytes_moved, transcendentals=0),
        name=name,
    )(*args)


def per_device(
    stream,
    norm_gain,
    w_value,
    w_mix,
    w_gate,
    w_state,
    conv_taps,
    skip_gain,
    decay_rate,
    turn_rate,
    input_real,
    input_imag,
    read_real,
    read_imag,
    initial_state,
    intervals,
    proj_conv,
    proj_state,
):
    n, share = stream.shape
    parts = lax.axis_size("tp")
    inner_axes = SP[1:]
    inside = lax.axis_size(inner_axes)
    planes = lax.axis_size(SP[0])
    channels = w_value.shape[1]
    width = decay_rate.size
    (blank,) = call(lead_kernel, [((8, channels), F32)], bytes_moved=3 * 10**8, name="lead")
    packed, notes = call(
        pack_kernel,
        [((parts, n + 8, share), BF16), ((8, channels), F32)],
        stream, norm_gain.reshape(1, -1), intervals.reshape(1, n), conv_taps, skip_gain.reshape(1, -1), blank,
        bytes_moved=3 * 10**8,
        name="pack",
    )
    rows = exchange(packed, "tp")

    states = ((n, width), F32)
    chunks = ((CHUNKS, width), F32)
    mixed = ((n, channels), F32)
    ur, ui, cr, ci, fr, fi, br, bi, source, gate, state, consts, message = call(
        local_kernel,
        [states, states, chunks, chunks, states, states, chunks, chunks, mixed, mixed, mixed]
        + [((40, channels), F32), ((inside, 24, 128), BF16)],
        rows, w_value, w_mix, w_gate, w_state, decay_rate, turn_rate,
        jnp.swapaxes(input_real, 2, 3).reshape(2 * channels, -1),
        jnp.swapaxes(input_imag, 2, 3).reshape(2 * channels, -1),
        initial_state, notes,
        scratch=[pltpu.VMEM((n, width), F32)] + [pltpu.VMEM((CHUNKS, width), F32)] * 2,
        name="local",
    )
    inner, message = call(
        plane_kernel,
        [((48, 128), F32), ((planes, 4, 384), BF16)],
        exchange(message, inner_axes), consts,
        name="plane",
    )
    got = exchange(message, SP[0])
    (partial,) = call(
        finish_kernel,
        [((parts, n, share), BF16)],
        got, inner, consts, ur, ui, cr, ci, fr, fi, br, bi,
        read_real.reshape(2 * channels, -1), read_imag.reshape(2 * channels, -1), source, gate, state,
        proj_conv, proj_state,
        name="finish",
    )
    arrived = exchange(partial, "tp")
    return arrived.astype(F32).sum(axis=0).astype(BF16)


def solution(mesh):
    finer = Mesh(mesh.devices.reshape(16, 4, 2, mesh.shape["tp"]), ("sp_0", "sp_1", "sp_2", "tp"))
    return jax.shard_map(
        per_device,
        mesh=finer,
        in_specs=(
            P(SP, "tp"),
            P("tp"),
            P(None, "tp"),
            P(None, "tp"),
            P(None, "tp"),
            P(None, "tp"),
            P(None, "tp"),
            P("tp"),
            P(None, "tp", None),
            P(None, "tp", None),
            P(None, "tp", None, None),
            P(None, "tp", None, None),
            P(None, "tp", None, None),
            P(None, "tp", None, None),
            P(None, None, "tp", None),
            P(SP),
            P("tp", None),
            P("tp", None),
        ),
        out_specs=P(SP, "tp"),
        check_vma=False,
    )
```

```python
import jax
import jax.numpy as jnp
from jax import lax
from jax.experimental import pallas as pl
from jax.experimental.pallas import tpu as pltpu
from jax.sharding import Mesh
from jax.sharding import PartitionSpec as P

D = 2048
SP = ("sp_0", "sp_1", "sp_2")
EPSILON = 1e-06
F32 = jnp.float32
BF16 = jnp.bfloat16
CHUNKS = 8
LONGEST = 1e30


def turned(half_turn, elapsed):
    half = half_turn * elapsed
    turns = jnp.round(half * 0.3183098861837907)
    rest = jnp.clip((half - turns * 3.140625) - turns * 9.67653589793e-4, -1.6, 1.6)
    square = rest * rest
    sine = rest + rest * (square * (-0.16666659712791443 + square * (0.008333086036145687 + square * (-0.0001981096138479188 + square * 2.6085685931320768e-06))))
    cosine = 1.0 + square * (-0.4999993145465851 + square * (0.04166397079825401 + square * (-0.0013855763245373964 + square * 2.3190419597085565e-05)))
    double = sine + sine
    fall = double * sine
    return double * cosine, 1.0 - fall, fall


def turned_briefly(rate, elapsed):
    turns = rate * elapsed
    rest = turns - jnp.round(turns)
    square = rest * rest
    sine = rest * (4.442883014678955 + square * (-7.308244228363037 + square * (3.606335163116455 + square * (-0.846008837223053 + square * 0.10963883250951767))))
    cosine = 1.4142135381698608 + square * (-6.978850841522217 + square * (5.7394561767578125 + square * (-1.8835265636444092 + square * 0.3106144070625305)))
    fall = sine * sine
    return sine * cosine, 1.0 - fall, fall


def damped(half_rate, elapsed):
    x = half_rate * elapsed
    root = jnp.exp(-x)
    magnitude = root * root
    square = x * x
    series = root * (x * (-2.0 - square * (1 / 3 + square * (1 / 60))))
    return magnitude, jnp.where(x < 0.25, series, magnitude - 1.0)


def moved(elapsed, rate, half_turn):
    magnitude = jnp.exp(-rate * elapsed)
    sine, cosine, _ = turned(half_turn, elapsed)
    return magnitude * cosine, magnitude * sine


def cmul(ar, ai, br, bi):
    return ar * br - ai * bi, ar * bi + ai * br


def iota(shape, dim):
    return lax.broadcasted_iota(jnp.int32, shape, dim)


def dot(a, b, dims=((1,), (0,))):
    return lax.dot_general(a, b, (dims, ((), ())), preferred_element_type=F32)


def halves(x):
    high = x.astype(BF16)
    return high, (x - high.astype(F32)).astype(BF16)


def scan_chunks(fr, fi, lr, li, backward):
    rows = iota(fr.shape, 0)
    for k in (1, 2, 4):
        shift = CHUNKS - k if backward else k
        outside = rows >= CHUNKS - k if backward else rows < k
        sfr = jnp.where(outside, 1.0, pltpu.roll(fr, shift, 0))
        sfi = jnp.where(outside, 0.0, pltpu.roll(fi, shift, 0))
        if lr is not None:
            slr = jnp.where(outside, 0.0, pltpu.roll(lr, shift, 0))
            sli = jnp.where(outside, 0.0, pltpu.roll(li, shift, 0))
            ar, ai = cmul(fr, fi, slr, sli)
            lr, li = lr + ar, li + ai
        fr, fi = cmul(fr, fi, sfr, sfi)
    return fr, fi, lr, li


def one_later(x, backward, fill):
    rows = iota(x.shape, 0)
    if backward:
        return jnp.where(rows == CHUNKS - 1, fill, pltpu.roll(x, CHUNKS - 1, 0))
    return jnp.where(rows == 0, fill, pltpu.roll(x, 1, 0))


def lead_kernel(out):
    out[...] = jnp.zeros(out.shape, F32)


def pack_kernel(stream, gain, intervals, taps, skip, blank, out, notes):
    n, share = stream.shape
    row = iota((8, share), 0)
    tail = jnp.zeros((8, share), F32)
    for at, x in enumerate((gain[...], jnp.concatenate([intervals[...]] * (share // n), axis=1))):
        high = x.astype(BF16).astype(F32)
        mid = (x - high).astype(BF16).astype(F32)
        for p, piece in enumerate((high, mid, x - high - mid)):
            tail = jnp.where(row == 3 * at + p, piece, tail)
    tail = tail.astype(BF16)
    for k in range(out.shape[0]):
        out[k, 0:n, :] = stream[...]
        out[k, n : n + 8, :] = tail
    notes[...] = blank[...]
    notes[0:3, :] = taps[...]
    notes[3:4, :] = skip[...]


def row_of(ref, d, q):
    return jnp.concatenate([ref[d, 2 * q : 2 * q + 1, :], ref[d, 2 * q + 1 : 2 * q + 2, :]], axis=1)


def doubled(x):
    return jnp.concatenate([x, x], axis=1)


def local_kernel(rows, w_value, w_mix, w_gate, w_state, decay, turn, in_re, in_im, init, notes, ur_o, ui_o, cr_o, ci_o, fr_o, fi_o, br_o, bi_o, source_o, gate_o, input_o, consts, message, lift_s, er_s, ei_s):
    parts, n, share = rows.shape[0], rows.shape[1] - 8, rows.shape[2]
    per = n // CHUNKS
    channels = w_value.shape[1]
    groups, states = decay.shape[1], decay.shape[2]
    wide = channels // groups
    pairs = groups // 2
    tiles = 2 * pairs
    row, col = iota((n, n), 0), iota((n, n), 1)
    ordered = col == (row % CHUNKS) * per + row // CHUNKS
    tail = rows[0, n : n + 8, 0:n].astype(F32)
    intervals = (tail[3:4] + tail[4:5]) + tail[5:6]
    steps = jnp.sum(jnp.where(ordered, intervals, 0.0), axis=1, keepdims=True)
    total = jnp.minimum(jnp.sum(intervals, axis=1, keepdims=True), LONGEST)
    elapsed = jnp.minimum(sum(steps[i * CHUNKS : i * CHUNKS + CHUNKS] for i in range(per)), LONGEST)
    order = jnp.where(ordered, 1.0, 0.0).astype(BF16)
    consts[32:40, :] = notes[...]

    def lanes_of(tile):
        return slice(tile * 128, tile * 128 + 128)

    def chunk_rows(tile):
        return [slice(i * CHUNKS, i * CHUNKS + CHUNKS) for i in (reversed(range(per)) if tile >= pairs else range(per))]

    def tabulate(tile):
        d, q = tile // pairs, tile % pairs
        lanes = lanes_of(tile)
        rate, half_turn = row_of(decay, d, q), 0.5 * row_of(turn, d, q)
        consts[tile : tile + 1, :] = rate
        consts[8 + tile : 9 + tile, :] = half_turn
        for part in range(2):
            pair = [init[d, part, 2 * q + k : 2 * q + k + 1, :] for k in range(2)]
            consts[16 + 8 * part + tile : 17 + 8 * part + tile, :] = jnp.concatenate(pair, axis=1)
        sine, cosine, fall = turned_briefly(half_turn * 0.3183098861837907, steps)
        magnitude, less_one = damped(0.5 * rate, steps)
        fr_o[:, lanes] = magnitude * cosine
        fi_o[:, lanes] = magnitude * sine
        lift_s[:, lanes] = less_one * cosine - fall
        er, ei = moved(elapsed, rate, half_turn)
        er_s[:, lanes] = er
        ei_s[:, lanes] = ei
        br, bi, _, _ = scan_chunks(er, ei, None, None, tile >= pairs)
        br_o[:, lanes] = one_later(br, tile >= pairs, 1.0)
        bi_o[:, lanes] = one_later(bi, tile >= pairs, 0.0)

    squares = 0.0
    for k in range(parts):
        x = rows[k, 0:n, :].astype(F32)
        squares = squares + jnp.sum(x * x, axis=1, keepdims=True)
    inv_rms = lax.rsqrt(squares / D + EPSILON)
    first = second = 0.0
    for k in range(parts):
        tail = rows[k, n : n + 8, :].astype(F32)
        gain = (tail[0:1] + tail[1:2]) + tail[2:3]
        normed = ((rows[k, 0:n, :].astype(F32) * inv_rms) * gain).astype(BF16)
        at = slice(k * share, k * share + share)
        first = first + dot(normed, jnp.concatenate([w_value[at, :], w_mix[at, :]], axis=1))
        second = second + dot(normed, jnp.concatenate([w_gate[at, :], w_state[at, :]], axis=1))
        for tile in range(k * tiles // parts, (k + 1) * tiles // parts):
            tabulate(tile)
    first = dot(order, first.astype(BF16))
    second = dot(order, second.astype(BF16))
    source = (first[:, :channels] * first[:, channels:]).astype(BF16).astype(F32)
    source_o[...] = source
    gate_o[...] = second[:, :channels]
    input_o[...] = second[:, channels:]
    state = second[:, channels:].astype(BF16)

    block = 2 * wide
    edges = []
    for d in range(2):
        backward = d == 1
        rates, turns = decay[d], turn[d]
        inverse = 1.0 / (rates * rates + turns * turns)
        inv_re = jnp.broadcast_to((-rates * inverse)[:, None, :], (groups, wide, states)).reshape(channels, states)
        inv_im = jnp.broadcast_to((-turns * inverse)[:, None, :], (groups, wide, states)).reshape(channels, states)
        at = slice(d * channels, d * channels + channels)
        scaled_re, scaled_im = cmul(in_re[at, :], in_im[at, :], inv_re, inv_im)
        scaled = (doubled(scaled_re), doubled(scaled_im))
        mine = iota((block, 128), 0) // wide == iota((block, 128), 1) // states
        for q in range(pairs):
            tile = d * pairs + q
            lanes = lanes_of(tile)
            some = slice(q * block, q * block + block)
            matrix = jnp.concatenate([jnp.concatenate(halves(jnp.where(mine, x[some], 0.0)), axis=0) for x in scaled], axis=1)
            driven = dot(jnp.concatenate([state[:, some], state[:, some]], axis=1), matrix)
            fr, fi = fr_o[:, lanes], fi_o[:, lanes]
            push_re, push_im = cmul(lift_s[:, lanes], fi, driven[:, :128], driven[:, 128:])
            ur_o[:, lanes] = push_re
            ui_o[:, lanes] = push_im
            hr = hi = None
            for at in chunk_rows(tile):
                if hr is None:
                    hr, hi = push_re[at], push_im[at]
                else:
                    ar, ai = cmul(fr[at], fi[at], hr, hi)
                    hr, hi = ar + push_re[at], ai + push_im[at]
            _, _, lr, li = scan_chunks(er_s[:, lanes], ei_s[:, lanes], hr, hi, backward)
            cr_o[:, lanes] = one_later(lr, backward, 0.0)
            ci_o[:, lanes] = one_later(li, backward, 0.0)
            edge = 0 if backward else CHUNKS - 1
            edges.append((lr[edge : edge + 1], li[edge : edge + 1]))
    high = total.astype(BF16).astype(F32)
    mid = (total - high).astype(BF16).astype(F32)
    lines = [r for r, m in edges] + [m for r, m in edges]
    lines += [jnp.broadcast_to(x, (1, 128)) for x in (high, mid, total - high - mid)]
    lines += [source[0:1], source[n - 1 : n], jnp.zeros((3, 128), F32)]
    lines = jnp.concatenate(lines, axis=0).astype(BF16)
    for k in range(message.shape[0]):
        message[k] = lines


def plane_kernel(got, consts, inner, message):
    size = got.shape[0]
    came = [got[k].astype(F32) for k in range(size)]
    times = [(x[16:17] + x[17:18]) + x[18:19] for x in came]
    here, plane = lax.axis_index(SP[1:]), lax.axis_index(SP[0])
    rate, turning = consts[0:8, :], consts[8:16, :]
    forward = iota((8, 128), 0) < 4
    hr = hi = spent = jnp.zeros((8, 128), F32)
    ir = ii = before = hr
    for k in range(size):
        m = size - 1 - k
        mine = (forward & (here == k)) | (jnp.logical_not(forward) & (here == m))
        ir = jnp.where(mine, hr, ir)
        ii = jnp.where(mine, hi, ii)
        before = jnp.where(mine, spent, before)
        elapsed = jnp.where(forward, times[k], times[m])
        ar, ai = moved(elapsed, rate, turning)
        ar, ai = cmul(ar, ai, hr, hi)
        hr = ar + jnp.where(forward, came[k][0:8], came[m][0:8])
        hi = ai + jnp.where(forward, came[k][8:16], came[m][8:16])
        spent = spent + elapsed
    wr, wi = moved(before, rate, turning)
    inner[0:8, :] = ir
    inner[8:16, :] = ii
    inner[16:24, :] = wr
    inner[24:32, :] = wi
    previous = following = jnp.zeros((1, 128), F32)
    for k in range(size):
        previous = jnp.where(here - 1 == k, came[k][20:21], previous)
        following = jnp.where(here + 1 == k, came[k][19:20], following)
    inner[32:40, :] = jnp.broadcast_to(previous, (8, 128))
    inner[40:48, :] = jnp.broadcast_to(following, (8, 128))
    high = spent[0:1].astype(BF16).astype(F32)
    mid = (spent[0:1] - high).astype(BF16).astype(F32)
    note = [high, mid, spent[0:1] - high - mid]
    note_later = jnp.concatenate(note + [came[size - 1][20:21]], axis=0)
    note_earlier = jnp.concatenate(note + [came[0][19:20]], axis=0)
    later = jnp.concatenate([hr[0:4], hi[0:4], note_later], axis=1)
    earlier = jnp.concatenate([hr[4:8], hi[4:8], note_earlier], axis=1)
    for k in range(message.shape[0]):
        message[k] = jnp.where(plane < k, later, earlier).astype(BF16)


def finish_kernel(got, inner, consts, ur, ui, cr_i, ci_i, fr, fi, br, bi, rd_re, rd_im, source, gate, state, proj_conv, proj_state, out):
    size = got.shape[0]
    here, plane = lax.axis_index(SP[1:]), lax.axis_index(SP[0])
    last = lax.axis_size(SP[1:]) - 1
    rate, turning = consts[0:8, :], consts[8:16, :]
    forward = iota((8, 128), 0) < 4
    hr, hi = consts[16:24, :], consts[24:32, :]
    arrived = [got[k].astype(F32) for k in range(size)]
    times = [(x[0:1, 256:] + x[1:2, 256:]) + x[2:3, 256:] for x in arrived]
    for k in range(size):
        m = size - 1 - k
        active = (forward & (plane > k)) | (jnp.logical_not(forward) & (plane < m))
        elapsed = jnp.where(forward, times[k], times[m])
        ar, ai = moved(elapsed, rate, turning)
        ar, ai = cmul(ar, ai, hr, hi)
        hr = jnp.where(active, ar + jnp.concatenate([arrived[k][:, :128], arrived[m][:, :128]], axis=0), hr)
        hi = jnp.where(active, ai + jnp.concatenate([arrived[k][:, 128:256], arrived[m][:, 128:256]], axis=0), hi)
    ar, ai = cmul(inner[16:24, :], inner[24:32, :], hr, hi)
    inc_re = ar + inner[0:8, :]
    inc_im = ai + inner[8:16, :]
    n, width = ur.shape
    per = n // CHUNKS
    channels = rd_re.shape[0] // 2
    states = rd_re.shape[1]
    pairs = width // 256
    block = channels // pairs
    wide = block // 2
    responses = []
    for q in range(pairs):
        mine = iota((block, 128), 0) // wide == iota((block, 128), 1) // states
        full, matrix = [], []
        for d in range(2):
            tile = d * pairs + q
            lanes = slice(tile * 128, tile * 128 + 128)
            er, ei = cmul(br[:, lanes], bi[:, lanes], inc_re[tile : tile + 1], inc_im[tile : tile + 1])
            hr, hi = er + cr_i[:, lanes], ei + ci_i[:, lanes]
            history = [None] * per
            for i in reversed(range(per)) if d == 1 else range(per):
                at = slice(i * CHUNKS, i * CHUNKS + CHUNKS)
                ar, ai = cmul(fr[at, lanes], fi[at, lanes], hr, hi)
                hr, hi = ar + ur[at, lanes], ai + ui[at, lanes]
                history[i] = (hr, hi)
            full += [jnp.concatenate([x[part] for x in history], axis=0) for part in range(2)]
            at = slice(d * channels + q * block, d * channels + (q + 1) * block)
            matrix += [jnp.where(mine, doubled(rd_re[at, :]), 0.0), jnp.where(mine, -doubled(rd_im[at, :]), 0.0)]
        high, low = halves(jnp.concatenate(full, axis=1))
        r_hi, r_lo = halves(jnp.concatenate(matrix, axis=1))
        across = ((1,), (1,))
        stacked = dot(jnp.concatenate([high, low], axis=0), r_hi, across)
        responses.append((stacked[n:] + dot(high, r_lo, across)) + stacked[:n])
    response = state[...] * consts[35:36, :] + jnp.concatenate(responses, axis=1)
    state_out = jax.nn.gelu(response).astype(BF16)
    previous, following = inner[32:33, :], inner[40:41, :]
    for k in range(size):
        previous = jnp.where((here == 0) & (plane - 1 == k), arrived[k][3:4, 256:], previous)
        following = jnp.where((here == last) & (plane + 1 == k), arrived[k][3:4, 256:], following)
    x = source[...]
    row = iota((CHUNKS, x.shape[1]), 0)
    head = jnp.where(row == 0, previous, pltpu.roll(x[n - CHUNKS :], 1, 0))
    foot = jnp.where(row == CHUNKS - 1, following, pltpu.roll(x[:CHUNKS], CHUNKS - 1, 0))
    before = jnp.concatenate([head, x[: n - CHUNKS]], axis=0)
    after = jnp.concatenate([x[CHUNKS:], foot], axis=0)
    filtered = consts[32:33, :] * before + consts[33:34, :] * x + consts[34:35, :] * after
    conv_out = (gate[...] * filtered).astype(BF16)
    row, col = iota((n, n), 0), iota((n, n), 1)
    order = jnp.where(row == (col % CHUNKS) * per + col // CHUNKS, 1.0, 0.0).astype(BF16)
    conv_out = dot(order, conv_out).astype(BF16)
    state_out = dot(order, state_out).astype(BF16)
    share = out.shape[2]
    for k in range(out.shape[0]):
        at = slice(k * share, k * share + share)
        out[k] = (dot(conv_out, proj_conv[:, at]) + dot(state_out, proj_state[:, at])).astype(BF16)


def exchange(x, axis):
    return lax.all_to_all(x, axis, split_axis=0, concat_axis=0, tiled=True)


VMEM = pl.BlockSpec(memory_space=pltpu.VMEM)


def call(kernel, shapes, *args, scratch=(), bytes_moved=10**6, name=None):
    return pl.pallas_call(
        kernel,
        out_shape=[jax.ShapeDtypeStruct(s, d) for s, d in shapes],
        in_specs=[VMEM] * len(args),
        out_specs=[VMEM] * len(shapes),
        scratch_shapes=scratch,
        compiler_params=pltpu.CompilerParams(vmem_limit_bytes=24 * 2**20),
        cost_estimate=pl.CostEstimate(flops=10**9, bytes_accessed=bytes_moved, transcendentals=0),
        name=name,
    )(*args)


def per_device(
    stream,
    norm_gain,
    w_value,
    w_mix,
    w_gate,
    w_state,
    conv_taps,
    skip_gain,
    decay_rate,
    turn_rate,
    input_real,
    input_imag,
    read_real,
    read_imag,
    initial_state,
    intervals,
    proj_conv,
    proj_state,
):
    n, share = stream.shape
    parts = lax.axis_size("tp")
    inner_axes = SP[1:]
    inside = lax.axis_size(inner_axes)
    planes = lax.axis_size(SP[0])
    channels = w_value.shape[1]
    width = decay_rate.size
    (blank,) = call(lead_kernel, [((8, channels), F32)], bytes_moved=3 * 10**8, name="lead")
    packed, notes = call(
        pack_kernel,
        [((parts, n + 8, share), BF16), ((8, channels), F32)],
        stream, norm_gain.reshape(1, -1), intervals.reshape(1, n), conv_taps, skip_gain.reshape(1, -1), blank,
        bytes_moved=3 * 10**8,
        name="pack",
    )
    rows = exchange(packed, "tp")

    states = ((n, width), F32)
    chunks = ((CHUNKS, width), F32)
    mixed = ((n, channels), F32)
    ur, ui, cr, ci, fr, fi, br, bi, source, gate, state, consts, message = call(
        local_kernel,
        [states, states, chunks, chunks, states, states, chunks, chunks, mixed, mixed, mixed]
        + [((40, channels), F32), ((inside, 24, 128), BF16)],
        rows, w_value, w_mix, w_gate, w_state, decay_rate, turn_rate,
        jnp.swapaxes(input_real, 2, 3).reshape(2 * channels, -1),
        jnp.swapaxes(input_imag, 2, 3).reshape(2 * channels, -1),
        initial_state, notes,
        scratch=[pltpu.VMEM((n, width), F32)] + [pltpu.VMEM((CHUNKS, width), F32)] * 2,
        name="local",
    )
    inner, message = call(
        plane_kernel,
        [((48, 128), F32), ((planes, 4, 384), BF16)],
        exchange(message, inner_axes), consts,
        name="plane",
    )
    got = exchange(message, SP[0])
    (partial,) = call(
        finish_kernel,
        [((parts, n, share), BF16)],
        got, inner, consts, ur, ui, cr, ci, fr, fi, br, bi,
        read_real.reshape(2 * channels, -1), read_imag.reshape(2 * channels, -1), source, gate, state,
        proj_conv, proj_state,
        name="finish",
    )
    arrived = exchange(partial, "tp")
    return arrived.astype(F32).sum(axis=0).astype(BF16)


def solution(mesh):
    finer = Mesh(mesh.devices.reshape(16, 4, 2, mesh.shape["tp"]), ("sp_0", "sp_1", "sp_2", "tp"))
    return jax.shard_map(
        per_device,
        mesh=finer,
        in_specs=(
            P(SP, "tp"),
            P("tp"),
            P(None, "tp"),
            P(None, "tp"),
            P(None, "tp"),
            P(None, "tp"),
            P(None, "tp"),
            P("tp"),
            P(None, "tp", None),
            P(None, "tp", None),
            P(None, "tp", None, None),
            P(None, "tp", None, None),
            P(None, "tp", None, None),
            P(None, "tp", None, None),
            P(None, None, "tp", None),
            P(SP),
            P("tp", None),
            P("tp", None),
        ),
        out_specs=P(SP, "tp"),
        check_vma=False,
    )
```

```python
import jax
import jax.numpy as jnp
from jax import lax
from jax.experimental import pallas as pl
from jax.experimental.pallas import tpu as pltpu
from jax.sharding import Mesh
from jax.sharding import PartitionSpec as P

D = 2048
SP = ("sp_0", "sp_1", "sp_2")
EPSILON = 1e-06
F32 = jnp.float32
BF16 = jnp.bfloat16
CHUNKS = 8
LONGEST = 1e30
LOG2E = 1.4426950408889634


def turned(half_turn, elapsed):
    half = half_turn * elapsed
    turns = jnp.round(half * 0.3183098861837907)
    rest = jnp.clip((half - turns * 3.140625) - turns * 9.67653589793e-4, -1.6, 1.6)
    square = rest * rest
    sine = rest + rest * (square * (-0.16666659712791443 + square * (0.008333086036145687 + square * (-0.0001981096138479188 + square * 2.6085685931320768e-06))))
    cosine = 1.0 + square * (-0.4999993145465851 + square * (0.04166397079825401 + square * (-0.0013855763245373964 + square * 2.3190419597085565e-05)))
    double = sine + sine
    fall = double * sine
    return double * cosine, 1.0 - fall, fall


def turned_briefly(rate, elapsed):
    turns = rate * elapsed
    rest = turns - jnp.round(turns)
    square = rest * rest
    sine = rest * (4.442883014678955 + square * (-7.308244228363037 + square * (3.606335163116455 + square * (-0.846008837223053 + square * 0.10963883250951767))))
    cosine = 1.4142135381698608 + square * (-6.978850841522217 + square * (5.7394561767578125 + square * (-1.8835265636444092 + square * 0.3106144070625305)))
    fall = sine * sine
    return sine * cosine, 1.0 - fall, fall


def damped(half_rate, elapsed):
    x = half_rate * elapsed
    root = jnp.exp2(x * -LOG2E)
    magnitude = root * root
    square = x * x
    series = root * (x * (-2.0 - square * (1 / 3 + square * (1 / 60))))
    return magnitude, jnp.where(x < 0.25, series, magnitude - 1.0)


def moved(elapsed, rate, half_turn):
    magnitude = jnp.exp2((rate * -LOG2E) * elapsed)
    sine, cosine, _ = turned(half_turn, elapsed)
    return magnitude * cosine, magnitude * sine


def cmul(ar, ai, br, bi):
    return ar * br - ai * bi, ar * bi + ai * br


def iota(shape, dim):
    return lax.broadcasted_iota(jnp.int32, shape, dim)


def dot(a, b, dims=((1,), (0,))):
    return lax.dot_general(a, b, (dims, ((), ())), preferred_element_type=F32)


def halves(x):
    high = x.astype(BF16)
    return high, (x - high.astype(F32)).astype(BF16)


def scan_chunks(fr, fi, lr, li, backward):
    rows = iota(fr.shape, 0)
    for k in (1, 2, 4):
        shift = CHUNKS - k if backward else k
        outside = rows >= CHUNKS - k if backward else rows < k
        sfr = jnp.where(outside, 1.0, pltpu.roll(fr, shift, 0))
        sfi = jnp.where(outside, 0.0, pltpu.roll(fi, shift, 0))
        if lr is not None:
            slr = jnp.where(outside, 0.0, pltpu.roll(lr, shift, 0))
            sli = jnp.where(outside, 0.0, pltpu.roll(li, shift, 0))
            ar, ai = cmul(fr, fi, slr, sli)
            lr, li = lr + ar, li + ai
        fr, fi = cmul(fr, fi, sfr, sfi)
    return fr, fi, lr, li


def one_later(x, backward, fill):
    rows = iota(x.shape, 0)
    if backward:
        return jnp.where(rows == CHUNKS - 1, fill, pltpu.roll(x, CHUNKS - 1, 0))
    return jnp.where(rows == 0, fill, pltpu.roll(x, 1, 0))


def lead_kernel(out):
    out[...] = jnp.zeros(out.shape, F32)


def pack_kernel(stream, gain, intervals, taps, skip, blank, out, notes):
    n, share = stream.shape
    row = iota((8, share), 0)
    tail = jnp.zeros((8, share), F32)
    for at, x in enumerate((gain[...], jnp.concatenate([intervals[...]] * (share // n), axis=1))):
        high = x.astype(BF16).astype(F32)
        mid = (x - high).astype(BF16).astype(F32)
        for p, piece in enumerate((high, mid, x - high - mid)):
            tail = jnp.where(row == 3 * at + p, piece, tail)
    tail = tail.astype(BF16)
    for k in range(out.shape[0]):
        out[k, 0:n, :] = stream[...]
        out[k, n : n + 8, :] = tail
    notes[...] = blank[...]
    notes[0:3, :] = taps[...]
    notes[3:4, :] = skip[...]


def row_of(ref, d, q):
    return jnp.concatenate([ref[d, 2 * q : 2 * q + 1, :], ref[d, 2 * q + 1 : 2 * q + 2, :]], axis=1)


def doubled(x):
    return jnp.concatenate([x, x], axis=1)


def local_kernel(rows, w_value, w_mix, w_gate, w_state, decay, turn, in_re, in_im, init, notes, ur_o, ui_o, cr_o, ci_o, fr_o, fi_o, br_o, bi_o, source_o, gate_o, input_o, consts, message, lift_s, er_s, ei_s):
    parts, n, share = rows.shape[0], rows.shape[1] - 8, rows.shape[2]
    per = n // CHUNKS
    channels = w_value.shape[1]
    groups, states = decay.shape[1], decay.shape[2]
    wide = channels // groups
    pairs = groups // 2
    tiles = 2 * pairs
    row, col = iota((n, n), 0), iota((n, n), 1)
    ordered = col == (row % CHUNKS) * per + row // CHUNKS
    tail = rows[0, n : n + 8, 0:n].astype(F32)
    intervals = (tail[3:4] + tail[4:5]) + tail[5:6]
    steps = jnp.sum(jnp.where(ordered, intervals, 0.0), axis=1, keepdims=True)
    total = jnp.minimum(jnp.sum(intervals, axis=1, keepdims=True), LONGEST)
    elapsed = jnp.minimum(sum(steps[i * CHUNKS : i * CHUNKS + CHUNKS] for i in range(per)), LONGEST)
    order = jnp.where(ordered, 1.0, 0.0).astype(BF16)
    consts[32:40, :] = notes[...]

    def lanes_of(tile):
        return slice(tile * 128, tile * 128 + 128)

    def chunk_rows(tile):
        return [slice(i * CHUNKS, i * CHUNKS + CHUNKS) for i in (reversed(range(per)) if tile >= pairs else range(per))]

    def tabulate(tile):
        d, q = tile // pairs, tile % pairs
        lanes = lanes_of(tile)
        rate, half_turn = row_of(decay, d, q), 0.5 * row_of(turn, d, q)
        consts[tile : tile + 1, :] = rate
        consts[8 + tile : 9 + tile, :] = half_turn
        for part in range(2):
            pair = [init[d, part, 2 * q + k : 2 * q + k + 1, :] for k in range(2)]
            consts[16 + 8 * part + tile : 17 + 8 * part + tile, :] = jnp.concatenate(pair, axis=1)
        sine, cosine, fall = turned_briefly(half_turn * 0.3183098861837907, steps)
        magnitude, less_one = damped(0.5 * rate, steps)
        fr_o[:, lanes] = magnitude * cosine
        fi_o[:, lanes] = magnitude * sine
        lift_s[:, lanes] = less_one * cosine - fall
        er, ei = moved(elapsed, rate, half_turn)
        er_s[:, lanes] = er
        ei_s[:, lanes] = ei
        br, bi, _, _ = scan_chunks(er, ei, None, None, tile >= pairs)
        br_o[:, lanes] = one_later(br, tile >= pairs, 1.0)
        bi_o[:, lanes] = one_later(bi, tile >= pairs, 0.0)

    squares = 0.0
    for k in range(parts):
        x = rows[k, 0:n, :].astype(F32)
        squares = squares + jnp.sum(x * x, axis=1, keepdims=True)
    inv_rms = lax.rsqrt(squares / D + EPSILON)
    first = second = 0.0
    for k in range(parts):
        tail = rows[k, n : n + 8, :].astype(F32)
        gain = (tail[0:1] + tail[1:2]) + tail[2:3]
        normed = ((rows[k, 0:n, :].astype(F32) * inv_rms) * gain).astype(BF16)
        at = slice(k * share, k * share + share)
        first = first + dot(normed, jnp.concatenate([w_value[at, :], w_mix[at, :]], axis=1))
        second = second + dot(normed, jnp.concatenate([w_gate[at, :], w_state[at, :]], axis=1))
        for tile in range(k * tiles // parts, (k + 1) * tiles // parts):
            tabulate(tile)
    first = dot(order, first.astype(BF16))
    second = dot(order, second.astype(BF16))
    source = (first[:, :channels] * first[:, channels:]).astype(BF16).astype(F32)
    source_o[...] = source
    gate_o[...] = second[:, :channels]
    input_o[...] = second[:, channels:]
    state = second[:, channels:].astype(BF16)

    block = 2 * wide
    edges = []
    for d in range(2):
        backward = d == 1
        rates, turns = decay[d], turn[d]
        inverse = 1.0 / (rates * rates + turns * turns)
        inv_re = jnp.broadcast_to((-rates * inverse)[:, None, :], (groups, wide, states)).reshape(channels, states)
        inv_im = jnp.broadcast_to((-turns * inverse)[:, None, :], (groups, wide, states)).reshape(channels, states)
        at = slice(d * channels, d * channels + channels)
        scaled_re, scaled_im = cmul(in_re[at, :], in_im[at, :], inv_re, inv_im)
        scaled = (doubled(scaled_re), doubled(scaled_im))
        mine = iota((block, 128), 0) // wide == iota((block, 128), 1) // states
        for q in range(pairs):
            tile = d * pairs + q
            lanes = lanes_of(tile)
            some = slice(q * block, q * block + block)
            matrix = jnp.concatenate([jnp.concatenate(halves(jnp.where(mine, x[some], 0.0)), axis=0) for x in scaled], axis=1)
            driven = dot(jnp.concatenate([state[:, some], state[:, some]], axis=1), matrix)
            fr, fi = fr_o[:, lanes], fi_o[:, lanes]
            push_re, push_im = cmul(lift_s[:, lanes], fi, driven[:, :128], driven[:, 128:])
            ur_o[:, lanes] = push_re
            ui_o[:, lanes] = push_im
            hr = hi = None
            for at in chunk_rows(tile):
                if hr is None:
                    hr, hi = push_re[at], push_im[at]
                else:
                    ar, ai = cmul(fr[at], fi[at], hr, hi)
                    hr, hi = ar + push_re[at], ai + push_im[at]
            _, _, lr, li = scan_chunks(er_s[:, lanes], ei_s[:, lanes], hr, hi, backward)
            cr_o[:, lanes] = one_later(lr, backward, 0.0)
            ci_o[:, lanes] = one_later(li, backward, 0.0)
            edge = 0 if backward else CHUNKS - 1
            edges.append((lr[edge : edge + 1], li[edge : edge + 1]))
    high = total.astype(BF16).astype(F32)
    mid = (total - high).astype(BF16).astype(F32)
    lines = [r for r, m in edges] + [m for r, m in edges]
    lines += [jnp.broadcast_to(x, (1, 128)) for x in (high, mid, total - high - mid)]
    lines += [source[0:1], source[n - 1 : n], jnp.zeros((3, 128), F32)]
    lines = jnp.concatenate(lines, axis=0).astype(BF16)
    for k in range(message.shape[0]):
        message[k] = lines


def plane_kernel(got, consts, inner, message):
    size = got.shape[0]
    came = [got[k].astype(F32) for k in range(size)]
    times = [(x[16:17] + x[17:18]) + x[18:19] for x in came]
    here, plane = lax.axis_index(SP[1:]), lax.axis_index(SP[0])
    rate, turning = consts[0:8, :], consts[8:16, :]
    forward = iota((8, 128), 0) < 4
    hr = hi = spent = jnp.zeros((8, 128), F32)
    ir = ii = before = hr
    for k in range(size):
        m = size - 1 - k
        mine = (forward & (here == k)) | (jnp.logical_not(forward) & (here == m))
        ir = jnp.where(mine, hr, ir)
        ii = jnp.where(mine, hi, ii)
        before = jnp.where(mine, spent, before)
        elapsed = jnp.where(forward, times[k], times[m])
        ar, ai = moved(elapsed, rate, turning)
        ar, ai = cmul(ar, ai, hr, hi)
        hr = ar + jnp.where(forward, came[k][0:8], came[m][0:8])
        hi = ai + jnp.where(forward, came[k][8:16], came[m][8:16])
        spent = spent + elapsed
    wr, wi = moved(before, rate, turning)
    inner[0:8, :] = ir
    inner[8:16, :] = ii
    inner[16:24, :] = wr
    inner[24:32, :] = wi
    previous = following = jnp.zeros((1, 128), F32)
    for k in range(size):
        previous = jnp.where(here - 1 == k, came[k][20:21], previous)
        following = jnp.where(here + 1 == k, came[k][19:20], following)
    inner[32:40, :] = jnp.broadcast_to(previous, (8, 128))
    inner[40:48, :] = jnp.broadcast_to(following, (8, 128))
    high = spent[0:1].astype(BF16).astype(F32)
    mid = (spent[0:1] - high).astype(BF16).astype(F32)
    note = [high, mid, spent[0:1] - high - mid]
    note_later = jnp.concatenate(note + [came[size - 1][20:21]], axis=0)
    note_earlier = jnp.concatenate(note + [came[0][19:20]], axis=0)
    later = jnp.concatenate([hr[0:4], hi[0:4], note_later], axis=1)
    earlier = jnp.concatenate([hr[4:8], hi[4:8], note_earlier], axis=1)
    for k in range(message.shape[0]):
        message[k] = jnp.where(plane < k, later, earlier).astype(BF16)


def finish_kernel(got, inner, consts, ur, ui, cr_i, ci_i, fr, fi, br, bi, rd_re, rd_im, source, gate, state, proj_conv, proj_state, out):
    size = got.shape[0]
    here, plane = lax.axis_index(SP[1:]), lax.axis_index(SP[0])
    last = lax.axis_size(SP[1:]) - 1
    rate, turning = consts[0:8, :], consts[8:16, :]
    forward = iota((8, 128), 0) < 4
    hr, hi = consts[16:24, :], consts[24:32, :]
    arrived = [got[k].astype(F32) for k in range(size)]
    times = [(x[0:1, 256:] + x[1:2, 256:]) + x[2:3, 256:] for x in arrived]
    for k in range(size):
        m = size - 1 - k
        active = (forward & (plane > k)) | (jnp.logical_not(forward) & (plane < m))
        elapsed = jnp.where(forward, times[k], times[m])
        ar, ai = moved(elapsed, rate, turning)
        ar, ai = cmul(ar, ai, hr, hi)
        hr = jnp.where(active, ar + jnp.concatenate([arrived[k][:, :128], arrived[m][:, :128]], axis=0), hr)
        hi = jnp.where(active, ai + jnp.concatenate([arrived[k][:, 128:256], arrived[m][:, 128:256]], axis=0), hi)
    ar, ai = cmul(inner[16:24, :], inner[24:32, :], hr, hi)
    inc_re = ar + inner[0:8, :]
    inc_im = ai + inner[8:16, :]
    n, width = ur.shape
    per = n // CHUNKS
    channels = rd_re.shape[0] // 2
    states = rd_re.shape[1]
    pairs = width // 256
    block = channels // pairs
    wide = block // 2
    responses = []
    for q in range(pairs):
        mine = iota((block, 128), 0) // wide == iota((block, 128), 1) // states
        full, matrix = [], []
        for d in range(2):
            tile = d * pairs + q
            lanes = slice(tile * 128, tile * 128 + 128)
            er, ei = cmul(br[:, lanes], bi[:, lanes], inc_re[tile : tile + 1], inc_im[tile : tile + 1])
            hr, hi = er + cr_i[:, lanes], ei + ci_i[:, lanes]
            history = [None] * per
            for i in reversed(range(per)) if d == 1 else range(per):
                at = slice(i * CHUNKS, i * CHUNKS + CHUNKS)
                ar, ai = cmul(fr[at, lanes], fi[at, lanes], hr, hi)
                hr, hi = ar + ur[at, lanes], ai + ui[at, lanes]
                history[i] = (hr, hi)
            full += [jnp.concatenate([x[part] for x in history], axis=0) for part in range(2)]
            at = slice(d * channels + q * block, d * channels + (q + 1) * block)
            matrix += [jnp.where(mine, doubled(rd_re[at, :]), 0.0), jnp.where(mine, -doubled(rd_im[at, :]), 0.0)]
        high, low = halves(jnp.concatenate(full, axis=1))
        r_hi, r_lo = halves(jnp.concatenate(matrix, axis=1))
        across = ((1,), (1,))
        stacked = dot(jnp.concatenate([high, low], axis=0), r_hi, across)
        responses.append((stacked[n:] + dot(high, r_lo, across)) + stacked[:n])
    response = state[...] * consts[35:36, :] + jnp.concatenate(responses, axis=1)
    state_out = jax.nn.gelu(response).astype(BF16)
    previous, following = inner[32:33, :], inner[40:41, :]
    for k in range(size):
        previous = jnp.where((here == 0) & (plane - 1 == k), arrived[k][3:4, 256:], previous)
        following = jnp.where((here == last) & (plane + 1 == k), arrived[k][3:4, 256:], following)
    x = source[...]
    row = iota((CHUNKS, x.shape[1]), 0)
    head = jnp.where(row == 0, previous, pltpu.roll(x[n - CHUNKS :], 1, 0))
    foot = jnp.where(row == CHUNKS - 1, following, pltpu.roll(x[:CHUNKS], CHUNKS - 1, 0))
    before = jnp.concatenate([head, x[: n - CHUNKS]], axis=0)
    after = jnp.concatenate([x[CHUNKS:], foot], axis=0)
    filtered = consts[32:33, :] * before + consts[33:34, :] * x + consts[34:35, :] * after
    conv_out = (gate[...] * filtered).astype(BF16)
    row, col = iota((n, n), 0), iota((n, n), 1)
    order = jnp.where(row == (col % CHUNKS) * per + col // CHUNKS, 1.0, 0.0).astype(BF16)
    conv_out = dot(order, conv_out).astype(BF16)
    state_out = dot(order, state_out).astype(BF16)
    both = jnp.concatenate([conv_out, state_out], axis=1)
    share = out.shape[2]
    for k in range(out.shape[0]):
        at = slice(k * share, k * share + share)
        out[k] = dot(both, jnp.concatenate([proj_conv[:, at], proj_state[:, at]], axis=0)).astype(BF16)


def exchange(x, axis):
    return lax.all_to_all(x, axis, split_axis=0, concat_axis=0, tiled=True)


VMEM = pl.BlockSpec(memory_space=pltpu.VMEM)


def call(kernel, shapes, *args, scratch=(), bytes_moved=10**6, name=None):
    return pl.pallas_call(
        kernel,
        out_shape=[jax.ShapeDtypeStruct(s, d) for s, d in shapes],
        in_specs=[VMEM] * len(args),
        out_specs=[VMEM] * len(shapes),
        scratch_shapes=scratch,
        compiler_params=pltpu.CompilerParams(vmem_limit_bytes=24 * 2**20),
        cost_estimate=pl.CostEstimate(flops=10**9, bytes_accessed=bytes_moved, transcendentals=0),
        name=name,
    )(*args)


def per_device(
    stream,
    norm_gain,
    w_value,
    w_mix,
    w_gate,
    w_state,
    conv_taps,
    skip_gain,
    decay_rate,
    turn_rate,
    input_real,
    input_imag,
    read_real,
    read_imag,
    initial_state,
    intervals,
    proj_conv,
    proj_state,
):
    n, share = stream.shape
    parts = lax.axis_size("tp")
    inner_axes = SP[1:]
    inside = lax.axis_size(inner_axes)
    planes = lax.axis_size(SP[0])
    channels = w_value.shape[1]
    width = decay_rate.size
    (blank,) = call(lead_kernel, [((8, channels), F32)], bytes_moved=3 * 10**8, name="lead")
    packed, notes = call(
        pack_kernel,
        [((parts, n + 8, share), BF16), ((8, channels), F32)],
        stream, norm_gain.reshape(1, -1), intervals.reshape(1, n), conv_taps, skip_gain.reshape(1, -1), blank,
        bytes_moved=3 * 10**8,
        name="pack",
    )
    rows = exchange(packed, "tp")

    states = ((n, width), F32)
    chunks = ((CHUNKS, width), F32)
    mixed = ((n, channels), F32)
    ur, ui, cr, ci, fr, fi, br, bi, source, gate, state, consts, message = call(
        local_kernel,
        [states, states, chunks, chunks, states, states, chunks, chunks, mixed, mixed, mixed]
        + [((40, channels), F32), ((inside, 24, 128), BF16)],
        rows, w_value, w_mix, w_gate, w_state, decay_rate, turn_rate,
        jnp.swapaxes(input_real, 2, 3).reshape(2 * channels, -1),
        jnp.swapaxes(input_imag, 2, 3).reshape(2 * channels, -1),
        initial_state, notes,
        scratch=[pltpu.VMEM((n, width), F32)] + [pltpu.VMEM((CHUNKS, width), F32)] * 2,
        name="local",
    )
    inner, message = call(
        plane_kernel,
        [((48, 128), F32), ((planes, 4, 384), BF16)],
        exchange(message, inner_axes), consts,
        name="plane",
    )
    got = exchange(message, SP[0])
    (partial,) = call(
        finish_kernel,
        [((parts, n, share), BF16)],
        got, inner, consts, ur, ui, cr, ci, fr, fi, br, bi,
        read_real.reshape(2 * channels, -1), read_imag.reshape(2 * channels, -1), source, gate, state,
        proj_conv, proj_state,
        name="finish",
    )
    arrived = exchange(partial, "tp")
    return arrived.astype(F32).sum(axis=0).astype(BF16)


def solution(mesh):
    finer = Mesh(mesh.devices.reshape(16, 4, 2, mesh.shape["tp"]), ("sp_0", "sp_1", "sp_2", "tp"))
    return jax.shard_map(
        per_device,
        mesh=finer,
        in_specs=(
            P(SP, "tp"),
            P("tp"),
            P(None, "tp"),
            P(None, "tp"),
            P(None, "tp"),
            P(None, "tp"),
            P(None, "tp"),
            P("tp"),
            P(None, "tp", None),
            P(None, "tp", None),
            P(None, "tp", None, None),
            P(None, "tp", None, None),
            P(None, "tp", None, None),
            P(None, "tp", None, None),
            P(None, None, "tp", None),
            P(SP),
            P("tp", None),
            P("tp", None),
        ),
        out_specs=P(SP, "tp"),
        check_vma=False,
    )
```

```python
import jax
import jax.numpy as jnp
from jax import lax
from jax.experimental import pallas as pl
from jax.experimental.pallas import tpu as pltpu
from jax.sharding import Mesh
from jax.sharding import PartitionSpec as P

D = 2048
SP = ("sp_0", "sp_1", "sp_2")
EPSILON = 1e-06
F32 = jnp.float32
BF16 = jnp.bfloat16
CHUNKS = 8
LONGEST = 1e30
LOG2E = 1.4426950408889634


def turned(half_turn, elapsed):
    half = half_turn * elapsed
    turns = jnp.round(half * 0.3183098861837907)
    rest = jnp.clip((half - turns * 3.140625) - turns * 9.67653589793e-4, -1.6, 1.6)
    square = rest * rest
    sine = rest + rest * (square * (-0.16666659712791443 + square * (0.008333086036145687 + square * (-0.0001981096138479188 + square * 2.6085685931320768e-06))))
    cosine = 1.0 + square * (-0.4999993145465851 + square * (0.04166397079825401 + square * (-0.0013855763245373964 + square * 2.3190419597085565e-05)))
    double = sine + sine
    fall = double * sine
    return double * cosine, 1.0 - fall, fall


def turned_briefly(rate, elapsed):
    turns = rate * elapsed
    rest = turns - jnp.round(turns)
    square = rest * rest
    sine = rest * (4.442883014678955 + square * (-7.308244228363037 + square * (3.606335163116455 + square * (-0.846008837223053 + square * 0.10963883250951767))))
    cosine = 1.4142135381698608 + square * (-6.978850841522217 + square * (5.7394561767578125 + square * (-1.8835265636444092 + square * 0.3106144070625305)))
    fall = sine * sine
    return sine * cosine, 1.0 - fall, fall


def damped(half_rate, elapsed):
    x = half_rate * elapsed
    root = jnp.exp2(x * -LOG2E)
    magnitude = root * root
    square = x * x
    series = root * (x * (-2.0 - square * (1 / 3 + square * (1 / 60))))
    return magnitude, jnp.where(x < 0.25, series, magnitude - 1.0)


def moved(elapsed, rate, half_turn):
    magnitude = jnp.exp2((rate * -LOG2E) * elapsed)
    sine, cosine, _ = turned(half_turn, elapsed)
    return magnitude * cosine, magnitude * sine


def cmul(ar, ai, br, bi):
    return ar * br - ai * bi, ar * bi + ai * br


def iota(shape, dim):
    return lax.broadcasted_iota(jnp.int32, shape, dim)


def dot(a, b, dims=((1,), (0,))):
    return lax.dot_general(a, b, (dims, ((), ())), preferred_element_type=F32)


def halves(x):
    high = x.astype(BF16)
    return high, (x - high.astype(F32)).astype(BF16)


def scan_chunks(fr, fi, lr, li, backward):
    rows = iota(fr.shape, 0)
    for k in (1, 2, 4):
        shift = CHUNKS - k if backward else k
        outside = rows >= CHUNKS - k if backward else rows < k
        sfr = jnp.where(outside, 1.0, pltpu.roll(fr, shift, 0))
        sfi = jnp.where(outside, 0.0, pltpu.roll(fi, shift, 0))
        if lr is not None:
            slr = jnp.where(outside, 0.0, pltpu.roll(lr, shift, 0))
            sli = jnp.where(outside, 0.0, pltpu.roll(li, shift, 0))
            ar, ai = cmul(fr, fi, slr, sli)
            lr, li = lr + ar, li + ai
        fr, fi = cmul(fr, fi, sfr, sfi)
    return fr, fi, lr, li


def one_later(x, backward, fill):
    rows = iota(x.shape, 0)
    if backward:
        return jnp.where(rows == CHUNKS - 1, fill, pltpu.roll(x, CHUNKS - 1, 0))
    return jnp.where(rows == 0, fill, pltpu.roll(x, 1, 0))


def lead_kernel(out):
    out[...] = jnp.zeros(out.shape, F32)


def pack_kernel(stream, gain, intervals, taps, skip, blank, out, notes):
    n, share = stream.shape
    row = iota((8, share), 0)
    tail = jnp.zeros((8, share), F32)
    for at, x in enumerate((gain[...], jnp.concatenate([intervals[...]] * (share // n), axis=1))):
        high = x.astype(BF16).astype(F32)
        mid = (x - high).astype(BF16).astype(F32)
        for p, piece in enumerate((high, mid, x - high - mid)):
            tail = jnp.where(row == 3 * at + p, piece, tail)
    tail = tail.astype(BF16)
    for k in range(out.shape[0]):
        out[k, 0:n, :] = stream[...]
        out[k, n : n + 8, :] = tail
    notes[...] = blank[...]
    notes[0:3, :] = taps[...]
    notes[3:4, :] = skip[...]


def row_of(ref, d, q):
    return jnp.concatenate([ref[d, 2 * q : 2 * q + 1, :], ref[d, 2 * q + 1 : 2 * q + 2, :]], axis=1)


def doubled(x):
    return jnp.concatenate([x, x], axis=1)


def local_kernel(rows, w_value, w_mix, w_gate, w_state, decay, turn, in_re, in_im, init, notes, ur_o, ui_o, cr_o, ci_o, fr_o, fi_o, br_o, bi_o, source_o, gate_o, input_o, consts, message, lift_s, er_s, ei_s):
    parts, n, share = rows.shape[0], rows.shape[1] - 8, rows.shape[2]
    per = n // CHUNKS
    channels = w_value.shape[1]
    groups, states = decay.shape[1], decay.shape[2]
    wide = channels // groups
    pairs = groups // 2
    tiles = 2 * pairs
    row, col = iota((n, n), 0), iota((n, n), 1)
    ordered = col == (row % CHUNKS) * per + row // CHUNKS
    tail = rows[0, n : n + 8, 0:n].astype(F32)
    intervals = (tail[3:4] + tail[4:5]) + tail[5:6]
    steps = jnp.sum(jnp.where(ordered, intervals, 0.0), axis=1, keepdims=True)
    total = jnp.minimum(jnp.sum(intervals, axis=1, keepdims=True), LONGEST)
    elapsed = jnp.minimum(sum(steps[i * CHUNKS : i * CHUNKS + CHUNKS] for i in range(per)), LONGEST)
    order = jnp.where(ordered, 1.0, 0.0).astype(BF16)
    consts[32:40, :] = notes[...]

    def lanes_of(tile):
        return slice(tile * 128, tile * 128 + 128)

    def chunk_rows(tile):
        return [slice(i * CHUNKS, i * CHUNKS + CHUNKS) for i in (reversed(range(per)) if tile >= pairs else range(per))]

    def tabulate(tile):
        d, q = tile // pairs, tile % pairs
        lanes = lanes_of(tile)
        rate, half_turn = row_of(decay, d, q), 0.5 * row_of(turn, d, q)
        consts[tile : tile + 1, :] = rate
        consts[8 + tile : 9 + tile, :] = half_turn
        for part in range(2):
            pair = [init[d, part, 2 * q + k : 2 * q + k + 1, :] for k in range(2)]
            consts[16 + 8 * part + tile : 17 + 8 * part + tile, :] = jnp.concatenate(pair, axis=1)
        sine, cosine, fall = turned_briefly(half_turn * 0.3183098861837907, steps)
        magnitude, less_one = damped(0.5 * rate, steps)
        fr_o[:, lanes] = magnitude * cosine
        fi_o[:, lanes] = magnitude * sine
        lift_s[:, lanes] = less_one * cosine - fall
        er, ei = moved(elapsed, rate, half_turn)
        er_s[:, lanes] = er
        ei_s[:, lanes] = ei
        br, bi, _, _ = scan_chunks(er, ei, None, None, tile >= pairs)
        br_o[:, lanes] = one_later(br, tile >= pairs, 1.0)
        bi_o[:, lanes] = one_later(bi, tile >= pairs, 0.0)

    squares = 0.0
    for k in range(parts):
        x = rows[k, 0:n, :].astype(F32)
        squares = squares + x * x
    squares = jnp.sum(squares, axis=1, keepdims=True)
    inv_rms = lax.rsqrt(squares / D + EPSILON)
    first = second = 0.0
    for k in range(parts):
        tail = rows[k, n : n + 8, :].astype(F32)
        gain = (tail[0:1] + tail[1:2]) + tail[2:3]
        normed = ((rows[k, 0:n, :].astype(F32) * inv_rms) * gain).astype(BF16)
        at = slice(k * share, k * share + share)
        first = first + dot(normed, jnp.concatenate([w_value[at, :], w_mix[at, :]], axis=1))
        second = second + dot(normed, jnp.concatenate([w_gate[at, :], w_state[at, :]], axis=1))
        for tile in range(k * tiles // parts, (k + 1) * tiles // parts):
            tabulate(tile)
    first = dot(order, first.astype(BF16))
    second = dot(order, second.astype(BF16))
    source = (first[:, :channels] * first[:, channels:]).astype(BF16).astype(F32)
    source_o[...] = source
    gate_o[...] = second[:, :channels]
    input_o[...] = second[:, channels:]
    state = second[:, channels:].astype(BF16)

    block = 2 * wide
    edges = []
    for d in range(2):
        backward = d == 1
        rates, turns = decay[d], turn[d]
        inverse = 1.0 / (rates * rates + turns * turns)
        inv_re = jnp.broadcast_to((-rates * inverse)[:, None, :], (groups, wide, states)).reshape(channels, states)
        inv_im = jnp.broadcast_to((-turns * inverse)[:, None, :], (groups, wide, states)).reshape(channels, states)
        at = slice(d * channels, d * channels + channels)
        scaled_re, scaled_im = cmul(in_re[at, :], in_im[at, :], inv_re, inv_im)
        scaled = (doubled(scaled_re), doubled(scaled_im))
        mine = iota((block, 128), 0) // wide == iota((block, 128), 1) // states
        for q in range(pairs):
            tile = d * pairs + q
            lanes = lanes_of(tile)
            some = slice(q * block, q * block + block)
            matrix = jnp.concatenate([jnp.concatenate(halves(jnp.where(mine, x[some], 0.0)), axis=0) for x in scaled], axis=1)
            driven = dot(jnp.concatenate([state[:, some], state[:, some]], axis=1), matrix)
            fr, fi = fr_o[:, lanes], fi_o[:, lanes]
            push_re, push_im = cmul(lift_s[:, lanes], fi, driven[:, :128], driven[:, 128:])
            ur_o[:, lanes] = push_re
            ui_o[:, lanes] = push_im
            hr = hi = None
            for at in chunk_rows(tile):
                if hr is None:
                    hr, hi = push_re[at], push_im[at]
                else:
                    ar, ai = cmul(fr[at], fi[at], hr, hi)
                    hr, hi = ar + push_re[at], ai + push_im[at]
            _, _, lr, li = scan_chunks(er_s[:, lanes], ei_s[:, lanes], hr, hi, backward)
            cr_o[:, lanes] = one_later(lr, backward, 0.0)
            ci_o[:, lanes] = one_later(li, backward, 0.0)
            edge = 0 if backward else CHUNKS - 1
            edges.append((lr[edge : edge + 1], li[edge : edge + 1]))
    high = total.astype(BF16).astype(F32)
    mid = (total - high).astype(BF16).astype(F32)
    lines = [r for r, m in edges] + [m for r, m in edges]
    lines += [jnp.broadcast_to(x, (1, 128)) for x in (high, mid, total - high - mid)]
    lines += [source[0:1], source[n - 1 : n], jnp.zeros((3, 128), F32)]
    lines = jnp.concatenate(lines, axis=0).astype(BF16)
    for k in range(message.shape[0]):
        message[k] = lines


def plane_kernel(got, consts, inner, message):
    size = got.shape[0]
    came = [got[k].astype(F32) for k in range(size)]
    times = [(x[16:17] + x[17:18]) + x[18:19] for x in came]
    here, plane = lax.axis_index(SP[1:]), lax.axis_index(SP[0])
    rate, turning = consts[0:8, :], consts[8:16, :]
    forward = iota((8, 128), 0) < 4
    hr = hi = spent = jnp.zeros((8, 128), F32)
    ir = ii = before = hr
    for k in range(size):
        m = size - 1 - k
        mine = (forward & (here == k)) | (jnp.logical_not(forward) & (here == m))
        ir = jnp.where(mine, hr, ir)
        ii = jnp.where(mine, hi, ii)
        before = jnp.where(mine, spent, before)
        elapsed = jnp.where(forward, times[k], times[m])
        ar, ai = moved(elapsed, rate, turning)
        ar, ai = cmul(ar, ai, hr, hi)
        hr = ar + jnp.where(forward, came[k][0:8], came[m][0:8])
        hi = ai + jnp.where(forward, came[k][8:16], came[m][8:16])
        spent = spent + elapsed
    wr, wi = moved(before, rate, turning)
    inner[0:8, :] = ir
    inner[8:16, :] = ii
    inner[16:24, :] = wr
    inner[24:32, :] = wi
    previous = following = jnp.zeros((1, 128), F32)
    for k in range(size):
        previous = jnp.where(here - 1 == k, came[k][20:21], previous)
        following = jnp.where(here + 1 == k, came[k][19:20], following)
    inner[32:40, :] = jnp.broadcast_to(previous, (8, 128))
    inner[40:48, :] = jnp.broadcast_to(following, (8, 128))
    high = spent[0:1].astype(BF16).astype(F32)
    mid = (spent[0:1] - high).astype(BF16).astype(F32)
    note = [high, mid, spent[0:1] - high - mid]
    note_later = jnp.concatenate(note + [came[size - 1][20:21]], axis=0)
    note_earlier = jnp.concatenate(note + [came[0][19:20]], axis=0)
    later = jnp.concatenate([hr[0:4], hi[0:4], note_later], axis=1)
    earlier = jnp.concatenate([hr[4:8], hi[4:8], note_earlier], axis=1)
    for k in range(message.shape[0]):
        message[k] = jnp.where(plane < k, later, earlier).astype(BF16)


def finish_kernel(got, inner, consts, ur, ui, cr_i, ci_i, fr, fi, br, bi, rd_re, rd_im, source, gate, state, proj_conv, proj_state, out):
    size = got.shape[0]
    here, plane = lax.axis_index(SP[1:]), lax.axis_index(SP[0])
    last = lax.axis_size(SP[1:]) - 1
    rate, turning = consts[0:8, :], consts[8:16, :]
    forward = iota((8, 128), 0) < 4
    hr, hi = consts[16:24, :], consts[24:32, :]
    arrived = [got[k].astype(F32) for k in range(size)]
    times = [(x[0:1, 256:] + x[1:2, 256:]) + x[2:3, 256:] for x in arrived]
    for k in range(size):
        m = size - 1 - k
        active = (forward & (plane > k)) | (jnp.logical_not(forward) & (plane < m))
        elapsed = jnp.where(forward, times[k], times[m])
        ar, ai = moved(elapsed, rate, turning)
        ar, ai = cmul(ar, ai, hr, hi)
        hr = jnp.where(active, ar + jnp.concatenate([arrived[k][:, :128], arrived[m][:, :128]], axis=0), hr)
        hi = jnp.where(active, ai + jnp.concatenate([arrived[k][:, 128:256], arrived[m][:, 128:256]], axis=0), hi)
    ar, ai = cmul(inner[16:24, :], inner[24:32, :], hr, hi)
    inc_re = ar + inner[0:8, :]
    inc_im = ai + inner[8:16, :]
    n, width = ur.shape
    per = n // CHUNKS
    channels = rd_re.shape[0] // 2
    states = rd_re.shape[1]
    pairs = width // 256
    block = channels // pairs
    wide = block // 2
    responses = []
    for q in range(pairs):
        mine = iota((block, 128), 0) // wide == iota((block, 128), 1) // states
        full, matrix = [], []
        for d in range(2):
            tile = d * pairs + q
            lanes = slice(tile * 128, tile * 128 + 128)
            er, ei = cmul(br[:, lanes], bi[:, lanes], inc_re[tile : tile + 1], inc_im[tile : tile + 1])
            hr, hi = er + cr_i[:, lanes], ei + ci_i[:, lanes]
            history = [None] * per
            for i in reversed(range(per)) if d == 1 else range(per):
                at = slice(i * CHUNKS, i * CHUNKS + CHUNKS)
                ar, ai = cmul(fr[at, lanes], fi[at, lanes], hr, hi)
                hr, hi = ar + ur[at, lanes], ai + ui[at, lanes]
                history[i] = (hr, hi)
            full += [jnp.concatenate([x[part] for x in history], axis=0) for part in range(2)]
            at = slice(d * channels + q * block, d * channels + (q + 1) * block)
            matrix += [jnp.where(mine, doubled(rd_re[at, :]), 0.0), jnp.where(mine, -doubled(rd_im[at, :]), 0.0)]
        high, low = halves(jnp.concatenate(full, axis=1))
        r_hi, r_lo = halves(jnp.concatenate(matrix, axis=1))
        across = ((1,), (1,))
        stacked = dot(jnp.concatenate([high, low], axis=0), r_hi, across)
        responses.append((stacked[n:] + dot(high, r_lo, across)) + stacked[:n])
    response = state[...] * consts[35:36, :] + jnp.concatenate(responses, axis=1)
    state_out = jax.nn.gelu(response).astype(BF16)
    previous, following = inner[32:33, :], inner[40:41, :]
    for k in range(size):
        previous = jnp.where((here == 0) & (plane - 1 == k), arrived[k][3:4, 256:], previous)
        following = jnp.where((here == last) & (plane + 1 == k), arrived[k][3:4, 256:], following)
    x = source[...]
    row = iota((CHUNKS, x.shape[1]), 0)
    head = jnp.where(row == 0, previous, pltpu.roll(x[n - CHUNKS :], 1, 0))
    foot = jnp.where(row == CHUNKS - 1, following, pltpu.roll(x[:CHUNKS], CHUNKS - 1, 0))
    before = jnp.concatenate([head, x[: n - CHUNKS]], axis=0)
    after = jnp.concatenate([x[CHUNKS:], foot], axis=0)
    filtered = consts[32:33, :] * before + consts[33:34, :] * x + consts[34:35, :] * after
    conv_out = (gate[...] * filtered).astype(BF16)
    row, col = iota((n, n), 0), iota((n, n), 1)
    order = jnp.where(row == (col % CHUNKS) * per + col // CHUNKS, 1.0, 0.0).astype(BF16)
    conv_out = dot(order, conv_out).astype(BF16)
    state_out = dot(order, state_out).astype(BF16)
    both = jnp.concatenate([conv_out, state_out], axis=1)
    share = out.shape[2]
    for k in range(out.shape[0]):
        at = slice(k * share, k * share + share)
        out[k] = dot(both, jnp.concatenate([proj_conv[:, at], proj_state[:, at]], axis=0)).astype(BF16)


def exchange(x, axis):
    return lax.all_to_all(x, axis, split_axis=0, concat_axis=0, tiled=True)


VMEM = pl.BlockSpec(memory_space=pltpu.VMEM)


def call(kernel, shapes, *args, scratch=(), bytes_moved=10**6, name=None):
    return pl.pallas_call(
        kernel,
        out_shape=[jax.ShapeDtypeStruct(s, d) for s, d in shapes],
        in_specs=[VMEM] * len(args),
        out_specs=[VMEM] * len(shapes),
        scratch_shapes=scratch,
        compiler_params=pltpu.CompilerParams(vmem_limit_bytes=24 * 2**20),
        cost_estimate=pl.CostEstimate(flops=10**9, bytes_accessed=bytes_moved, transcendentals=0),
        name=name,
    )(*args)


def per_device(
    stream,
    norm_gain,
    w_value,
    w_mix,
    w_gate,
    w_state,
    conv_taps,
    skip_gain,
    decay_rate,
    turn_rate,
    input_real,
    input_imag,
    read_real,
    read_imag,
    initial_state,
    intervals,
    proj_conv,
    proj_state,
):
    n, share = stream.shape
    parts = lax.axis_size("tp")
    inner_axes = SP[1:]
    inside = lax.axis_size(inner_axes)
    planes = lax.axis_size(SP[0])
    channels = w_value.shape[1]
    width = decay_rate.size
    (blank,) = call(lead_kernel, [((8, channels), F32)], bytes_moved=3 * 10**8, name="lead")
    packed, notes = call(
        pack_kernel,
        [((parts, n + 8, share), BF16), ((8, channels), F32)],
        stream, norm_gain.reshape(1, -1), intervals.reshape(1, n), conv_taps, skip_gain.reshape(1, -1), blank,
        bytes_moved=3 * 10**8,
        name="pack",
    )
    rows = exchange(packed, "tp")

    states = ((n, width), F32)
    chunks = ((CHUNKS, width), F32)
    mixed = ((n, channels), F32)
    ur, ui, cr, ci, fr, fi, br, bi, source, gate, state, consts, message = call(
        local_kernel,
        [states, states, chunks, chunks, states, states, chunks, chunks, mixed, mixed, mixed]
        + [((40, channels), F32), ((inside, 24, 128), BF16)],
        rows, w_value, w_mix, w_gate, w_state, decay_rate, turn_rate,
        jnp.swapaxes(input_real, 2, 3).reshape(2 * channels, -1),
        jnp.swapaxes(input_imag, 2, 3).reshape(2 * channels, -1),
        initial_state, notes,
        scratch=[pltpu.VMEM((n, width), F32)] + [pltpu.VMEM((CHUNKS, width), F32)] * 2,
        name="local",
    )
    inner, message = call(
        plane_kernel,
        [((48, 128), F32), ((planes, 4, 384), BF16)],
        exchange(message, inner_axes), consts,
        name="plane",
    )
    got = exchange(message, SP[0])
    (partial,) = call(
        finish_kernel,
        [((parts, n, share), BF16)],
        got, inner, consts, ur, ui, cr, ci, fr, fi, br, bi,
        read_real.reshape(2 * channels, -1), read_imag.reshape(2 * channels, -1), source, gate, state,
        proj_conv, proj_state,
        name="finish",
    )
    arrived = exchange(partial, "tp")
    return arrived.astype(F32).sum(axis=0).astype(BF16)


def solution(mesh):
    finer = Mesh(mesh.devices.reshape(16, 4, 2, mesh.shape["tp"]), ("sp_0", "sp_1", "sp_2", "tp"))
    return jax.shard_map(
        per_device,
        mesh=finer,
        in_specs=(
            P(SP, "tp"),
            P("tp"),
            P(None, "tp"),
            P(None, "tp"),
            P(None, "tp"),
            P(None, "tp"),
            P(None, "tp"),
            P("tp"),
            P(None, "tp", None),
            P(None, "tp", None),
            P(None, "tp", None, None),
            P(None, "tp", None, None),
            P(None, "tp", None, None),
            P(None, "tp", None, None),
            P(None, None, "tp", None),
            P(SP),
            P("tp", None),
            P("tp", None),
        ),
        out_specs=P(SP, "tp"),
        check_vma=False,
    )
```

```python
import jax
import jax.numpy as jnp
from jax import lax
from jax.experimental import pallas as pl
from jax.experimental.pallas import tpu as pltpu
from jax.sharding import Mesh
from jax.sharding import PartitionSpec as P

D = 2048
SP = ("sp_0", "sp_1", "sp_2")
EPSILON = 1e-06
F32 = jnp.float32
BF16 = jnp.bfloat16
CHUNKS = 8
LONGEST = 1e30
LOG2E = 1.4426950408889634


def turned(half_turn, elapsed):
    half = half_turn * elapsed
    turns = jnp.round(half * 0.3183098861837907)
    rest = jnp.clip((half - turns * 3.140625) - turns * 9.67653589793e-4, -1.6, 1.6)
    square = rest * rest
    sine = rest + rest * (square * (-0.16666659712791443 + square * (0.008333086036145687 + square * (-0.0001981096138479188 + square * 2.6085685931320768e-06))))
    cosine = 1.0 + square * (-0.4999993145465851 + square * (0.04166397079825401 + square * (-0.0013855763245373964 + square * 2.3190419597085565e-05)))
    double = sine + sine
    fall = double * sine
    return double * cosine, 1.0 - fall, fall


def turned_briefly(rate, elapsed):
    turns = rate * elapsed
    rest = turns - jnp.round(turns)
    square = rest * rest
    sine = rest * (4.442883014678955 + square * (-7.308244228363037 + square * (3.606335163116455 + square * (-0.846008837223053 + square * 0.10963883250951767))))
    cosine = 1.4142135381698608 + square * (-6.978850841522217 + square * (5.7394561767578125 + square * (-1.8835265636444092 + square * 0.3106144070625305)))
    fall = sine * sine
    return sine * cosine, 1.0 - fall, fall


def damped(half_rate, elapsed):
    x = (half_rate * -LOG2E) * elapsed
    root = jnp.exp2(x)
    magnitude = root * root
    square = x * x
    series = root * (x * (1.3862943611198906 + square * (0.11100821732964315 + square * 0.002666711628)))
    return magnitude, jnp.where(x > -0.36, series, magnitude - 1.0)


def moved(elapsed, rate, half_turn):
    magnitude = jnp.exp2((rate * -LOG2E) * elapsed)
    sine, cosine, _ = turned(half_turn, elapsed)
    return magnitude * cosine, magnitude * sine


def cmul(ar, ai, br, bi):
    return ar * br - ai * bi, ar * bi + ai * br


def iota(shape, dim):
    return lax.broadcasted_iota(jnp.int32, shape, dim)


def dot(a, b, dims=((1,), (0,))):
    return lax.dot_general(a, b, (dims, ((), ())), preferred_element_type=F32)


def halves(x):
    high = x.astype(BF16)
    return high, (x - high.astype(F32)).astype(BF16)


def scan_chunks(fr, fi, lr, li, backward):
    rows = iota(fr.shape, 0)
    for k in (1, 2, 4):
        shift = CHUNKS - k if backward else k
        outside = rows >= CHUNKS - k if backward else rows < k
        sfr = jnp.where(outside, 1.0, pltpu.roll(fr, shift, 0))
        sfi = jnp.where(outside, 0.0, pltpu.roll(fi, shift, 0))
        if lr is not None:
            slr = jnp.where(outside, 0.0, pltpu.roll(lr, shift, 0))
            sli = jnp.where(outside, 0.0, pltpu.roll(li, shift, 0))
            ar, ai = cmul(fr, fi, slr, sli)
            lr, li = lr + ar, li + ai
        fr, fi = cmul(fr, fi, sfr, sfi)
    return fr, fi, lr, li


def one_later(x, backward, fill):
    rows = iota(x.shape, 0)
    if backward:
        return jnp.where(rows == CHUNKS - 1, fill, pltpu.roll(x, CHUNKS - 1, 0))
    return jnp.where(rows == 0, fill, pltpu.roll(x, 1, 0))


def lead_kernel(out):
    out[...] = jnp.zeros(out.shape, F32)


def pack_kernel(stream, gain, intervals, taps, skip, blank, out, notes):
    n, share = stream.shape
    row = iota((8, share), 0)
    tail = jnp.zeros((8, share), F32)
    for at, x in enumerate((gain[...], jnp.concatenate([intervals[...]] * (share // n), axis=1))):
        high = x.astype(BF16).astype(F32)
        mid = (x - high).astype(BF16).astype(F32)
        for p, piece in enumerate((high, mid, x - high - mid)):
            tail = jnp.where(row == 3 * at + p, piece, tail)
    tail = tail.astype(BF16)
    for k in range(out.shape[0]):
        out[k, 0:n, :] = stream[...]
        out[k, n : n + 8, :] = tail
    notes[...] = blank[...]
    notes[0:3, :] = taps[...]
    notes[3:4, :] = skip[...]


def row_of(ref, d, q):
    return jnp.concatenate([ref[d, 2 * q : 2 * q + 1, :], ref[d, 2 * q + 1 : 2 * q + 2, :]], axis=1)


def doubled(x):
    return jnp.concatenate([x, x], axis=1)


def local_kernel(rows, w_value, w_mix, w_gate, w_state, decay, turn, in_re, in_im, init, notes, ur_o, ui_o, cr_o, ci_o, fr_o, fi_o, br_o, bi_o, source_o, gate_o, input_o, consts, message, lift_s, er_s, ei_s):
    parts, n, share = rows.shape[0], rows.shape[1] - 8, rows.shape[2]
    per = n // CHUNKS
    channels = w_value.shape[1]
    groups, states = decay.shape[1], decay.shape[2]
    wide = channels // groups
    pairs = groups // 2
    tiles = 2 * pairs
    row, col = iota((n, n), 0), iota((n, n), 1)
    ordered = col == (row % CHUNKS) * per + row // CHUNKS
    tail = rows[0, n : n + 8, 0:n].astype(F32)
    intervals = (tail[3:4] + tail[4:5]) + tail[5:6]
    steps = jnp.sum(jnp.where(ordered, intervals, 0.0), axis=1, keepdims=True)
    total = jnp.minimum(jnp.sum(intervals, axis=1, keepdims=True), LONGEST)
    elapsed = jnp.minimum(sum(steps[i * CHUNKS : i * CHUNKS + CHUNKS] for i in range(per)), LONGEST)
    order = jnp.where(ordered, 1.0, 0.0).astype(BF16)
    consts[32:40, :] = notes[...]

    def lanes_of(tile):
        return slice(tile * 128, tile * 128 + 128)

    def chunk_rows(tile):
        return [slice(i * CHUNKS, i * CHUNKS + CHUNKS) for i in (reversed(range(per)) if tile >= pairs else range(per))]

    def tabulate(tile):
        d, q = tile // pairs, tile % pairs
        lanes = lanes_of(tile)
        rate, half_turn = row_of(decay, d, q), 0.5 * row_of(turn, d, q)
        consts[tile : tile + 1, :] = rate
        consts[8 + tile : 9 + tile, :] = half_turn
        for part in range(2):
            pair = [init[d, part, 2 * q + k : 2 * q + k + 1, :] for k in range(2)]
            consts[16 + 8 * part + tile : 17 + 8 * part + tile, :] = jnp.concatenate(pair, axis=1)
        sine, cosine, fall = turned_briefly(half_turn * 0.3183098861837907, steps)
        magnitude, less_one = damped(0.5 * rate, steps)
        fr_o[:, lanes] = magnitude * cosine
        fi_o[:, lanes] = magnitude * sine
        lift_s[:, lanes] = less_one * cosine - fall
        er, ei = moved(elapsed, rate, half_turn)
        er_s[:, lanes] = er
        ei_s[:, lanes] = ei
        br, bi, _, _ = scan_chunks(er, ei, None, None, tile >= pairs)
        br_o[:, lanes] = one_later(br, tile >= pairs, 1.0)
        bi_o[:, lanes] = one_later(bi, tile >= pairs, 0.0)

    squares = 0.0
    for k in range(parts):
        x = rows[k, 0:n, :].astype(F32)
        squares = squares + x * x
    squares = jnp.sum(squares, axis=1, keepdims=True)
    inv_rms = lax.rsqrt(squares / D + EPSILON)
    first = second = 0.0
    for k in range(parts):
        tail = rows[k, n : n + 8, :].astype(F32)
        gain = (tail[0:1] + tail[1:2]) + tail[2:3]
        normed = ((rows[k, 0:n, :].astype(F32) * inv_rms) * gain).astype(BF16)
        at = slice(k * share, k * share + share)
        first = first + dot(normed, jnp.concatenate([w_value[at, :], w_mix[at, :]], axis=1))
        second = second + dot(normed, jnp.concatenate([w_gate[at, :], w_state[at, :]], axis=1))
        for tile in range(k * tiles // parts, (k + 1) * tiles // parts):
            tabulate(tile)
    first = dot(order, first.astype(BF16))
    second = dot(order, second.astype(BF16))
    source = (first[:, :channels] * first[:, channels:]).astype(BF16).astype(F32)
    source_o[...] = source
    gate_o[...] = second[:, :channels]
    input_o[...] = second[:, channels:]
    state = second[:, channels:].astype(BF16)

    block = 2 * wide
    edges = []
    for d in range(2):
        backward = d == 1
        rates, turns = decay[d], turn[d]
        inverse = 1.0 / (rates * rates + turns * turns)
        inv_re = jnp.broadcast_to((-rates * inverse)[:, None, :], (groups, wide, states)).reshape(channels, states)
        inv_im = jnp.broadcast_to((-turns * inverse)[:, None, :], (groups, wide, states)).reshape(channels, states)
        at = slice(d * channels, d * channels + channels)
        scaled_re, scaled_im = cmul(in_re[at, :], in_im[at, :], inv_re, inv_im)
        scaled = (doubled(scaled_re), doubled(scaled_im))
        mine = iota((block, 128), 0) // wide == iota((block, 128), 1) // states
        for q in range(pairs):
            tile = d * pairs + q
            lanes = lanes_of(tile)
            some = slice(q * block, q * block + block)
            matrix = jnp.concatenate([jnp.concatenate(halves(jnp.where(mine, x[some], 0.0)), axis=0) for x in scaled], axis=1)
            driven = dot(jnp.concatenate([state[:, some], state[:, some]], axis=1), matrix)
            fr, fi = fr_o[:, lanes], fi_o[:, lanes]
            push_re, push_im = cmul(lift_s[:, lanes], fi, driven[:, :128], driven[:, 128:])
            ur_o[:, lanes] = push_re
            ui_o[:, lanes] = push_im
            hr = hi = None
            for at in chunk_rows(tile):
                if hr is None:
                    hr, hi = push_re[at], push_im[at]
                else:
                    ar, ai = cmul(fr[at], fi[at], hr, hi)
                    hr, hi = ar + push_re[at], ai + push_im[at]
            _, _, lr, li = scan_chunks(er_s[:, lanes], ei_s[:, lanes], hr, hi, backward)
            cr_o[:, lanes] = one_later(lr, backward, 0.0)
            ci_o[:, lanes] = one_later(li, backward, 0.0)
            edge = 0 if backward else CHUNKS - 1
            edges.append((lr[edge : edge + 1], li[edge : edge + 1]))
    high = total.astype(BF16).astype(F32)
    mid = (total - high).astype(BF16).astype(F32)
    lines = [r for r, m in edges] + [m for r, m in edges]
    lines += [jnp.broadcast_to(x, (1, 128)) for x in (high, mid, total - high - mid)]
    lines += [source[0:1], source[n - 1 : n], jnp.zeros((3, 128), F32)]
    lines = jnp.concatenate(lines, axis=0).astype(BF16)
    for k in range(message.shape[0]):
        message[k] = lines


def plane_kernel(got, consts, inner, message):
    size = got.shape[0]
    came = [got[k].astype(F32) for k in range(size)]
    times = [(x[16:17] + x[17:18]) + x[18:19] for x in came]
    here, plane = lax.axis_index(SP[1:]), lax.axis_index(SP[0])
    rate, turning = consts[0:8, :], consts[8:16, :]
    forward = iota((8, 128), 0) < 4
    hr = hi = spent = jnp.zeros((8, 128), F32)
    ir = ii = before = hr
    for k in range(size):
        m = size - 1 - k
        mine = (forward & (here == k)) | (jnp.logical_not(forward) & (here == m))
        ir = jnp.where(mine, hr, ir)
        ii = jnp.where(mine, hi, ii)
        before = jnp.where(mine, spent, before)
        elapsed = jnp.where(forward, times[k], times[m])
        ar, ai = moved(elapsed, rate, turning)
        ar, ai = cmul(ar, ai, hr, hi)
        hr = ar + jnp.where(forward, came[k][0:8], came[m][0:8])
        hi = ai + jnp.where(forward, came[k][8:16], came[m][8:16])
        spent = spent + elapsed
    wr, wi = moved(before, rate, turning)
    inner[0:8, :] = ir
    inner[8:16, :] = ii
    inner[16:24, :] = wr
    inner[24:32, :] = wi
    previous = following = jnp.zeros((1, 128), F32)
    for k in range(size):
        previous = jnp.where(here - 1 == k, came[k][20:21], previous)
        following = jnp.where(here + 1 == k, came[k][19:20], following)
    inner[32:40, :] = jnp.broadcast_to(previous, (8, 128))
    inner[40:48, :] = jnp.broadcast_to(following, (8, 128))
    high = spent[0:1].astype(BF16).astype(F32)
    mid = (spent[0:1] - high).astype(BF16).astype(F32)
    note = [high, mid, spent[0:1] - high - mid]
    note_later = jnp.concatenate(note + [came[size - 1][20:21]], axis=0)
    note_earlier = jnp.concatenate(note + [came[0][19:20]], axis=0)
    later = jnp.concatenate([hr[0:4], hi[0:4], note_later], axis=1)
    earlier = jnp.concatenate([hr[4:8], hi[4:8], note_earlier], axis=1)
    for k in range(message.shape[0]):
        message[k] = jnp.where(plane < k, later, earlier).astype(BF16)


def finish_kernel(got, inner, consts, ur, ui, cr_i, ci_i, fr, fi, br, bi, rd_re, rd_im, source, gate, state, proj_conv, proj_state, out):
    size = got.shape[0]
    here, plane = lax.axis_index(SP[1:]), lax.axis_index(SP[0])
    last = lax.axis_size(SP[1:]) - 1
    rate, turning = consts[0:8, :], consts[8:16, :]
    forward = iota((8, 128), 0) < 4
    hr, hi = consts[16:24, :], consts[24:32, :]
    arrived = [got[k].astype(F32) for k in range(size)]
    times = [(x[0:1, 256:] + x[1:2, 256:]) + x[2:3, 256:] for x in arrived]
    for k in range(size):
        m = size - 1 - k
        active = (forward & (plane > k)) | (jnp.logical_not(forward) & (plane < m))
        elapsed = jnp.where(forward, times[k], times[m])
        ar, ai = moved(elapsed, rate, turning)
        ar, ai = cmul(ar, ai, hr, hi)
        hr = jnp.where(active, ar + jnp.concatenate([arrived[k][:, :128], arrived[m][:, :128]], axis=0), hr)
        hi = jnp.where(active, ai + jnp.concatenate([arrived[k][:, 128:256], arrived[m][:, 128:256]], axis=0), hi)
    ar, ai = cmul(inner[16:24, :], inner[24:32, :], hr, hi)
    inc_re = ar + inner[0:8, :]
    inc_im = ai + inner[8:16, :]
    n, width = ur.shape
    per = n // CHUNKS
    channels = rd_re.shape[0] // 2
    states = rd_re.shape[1]
    pairs = width // 256
    block = channels // pairs
    wide = block // 2
    responses = []
    for q in range(pairs):
        mine = iota((block, 128), 0) // wide == iota((block, 128), 1) // states
        full, matrix = [], []
        for d in range(2):
            tile = d * pairs + q
            lanes = slice(tile * 128, tile * 128 + 128)
            er, ei = cmul(br[:, lanes], bi[:, lanes], inc_re[tile : tile + 1], inc_im[tile : tile + 1])
            hr, hi = er + cr_i[:, lanes], ei + ci_i[:, lanes]
            history = [None] * per
            for i in reversed(range(per)) if d == 1 else range(per):
                at = slice(i * CHUNKS, i * CHUNKS + CHUNKS)
                ar, ai = cmul(fr[at, lanes], fi[at, lanes], hr, hi)
                hr, hi = ar + ur[at, lanes], ai + ui[at, lanes]
                history[i] = (hr, hi)
            full += [jnp.concatenate([x[part] for x in history], axis=0) for part in range(2)]
            at = slice(d * channels + q * block, d * channels + (q + 1) * block)
            matrix += [jnp.where(mine, doubled(rd_re[at, :]), 0.0), jnp.where(mine, -doubled(rd_im[at, :]), 0.0)]
        high, low = halves(jnp.concatenate(full, axis=1))
        r_hi, r_lo = halves(jnp.concatenate(matrix, axis=1))
        across = ((1,), (1,))
        stacked = dot(jnp.concatenate([high, low], axis=0), r_hi, across)
        responses.append((stacked[n:] + dot(high, r_lo, across)) + stacked[:n])
    response = state[...] * consts[35:36, :] + jnp.concatenate(responses, axis=1)
    state_out = jax.nn.gelu(response).astype(BF16)
    previous, following = inner[32:33, :], inner[40:41, :]
    for k in range(size):
        previous = jnp.where((here == 0) & (plane - 1 == k), arrived[k][3:4, 256:], previous)
        following = jnp.where((here == last) & (plane + 1 == k), arrived[k][3:4, 256:], following)
    x = source[...]
    row = iota((CHUNKS, x.shape[1]), 0)
    head = jnp.where(row == 0, previous, pltpu.roll(x[n - CHUNKS :], 1, 0))
    foot = jnp.where(row == CHUNKS - 1, following, pltpu.roll(x[:CHUNKS], CHUNKS - 1, 0))
    before = jnp.concatenate([head, x[: n - CHUNKS]], axis=0)
    after = jnp.concatenate([x[CHUNKS:], foot], axis=0)
    filtered = consts[32:33, :] * before + consts[33:34, :] * x + consts[34:35, :] * after
    conv_out = (gate[...] * filtered).astype(BF16)
    row, col = iota((n, n), 0), iota((n, n), 1)
    order = jnp.where(row == (col % CHUNKS) * per + col // CHUNKS, 1.0, 0.0).astype(BF16)
    conv_out = dot(order, conv_out).astype(BF16)
    state_out = dot(order, state_out).astype(BF16)
    both = jnp.concatenate([conv_out, state_out], axis=1)
    share = out.shape[2]
    for k in range(out.shape[0]):
        at = slice(k * share, k * share + share)
        out[k] = dot(both, jnp.concatenate([proj_conv[:, at], proj_state[:, at]], axis=0)).astype(BF16)


def exchange(x, axis):
    return lax.all_to_all(x, axis, split_axis=0, concat_axis=0, tiled=True)


VMEM = pl.BlockSpec(memory_space=pltpu.VMEM)


def call(kernel, shapes, *args, scratch=(), bytes_moved=10**6, name=None):
    return pl.pallas_call(
        kernel,
        out_shape=[jax.ShapeDtypeStruct(s, d) for s, d in shapes],
        in_specs=[VMEM] * len(args),
        out_specs=[VMEM] * len(shapes),
        scratch_shapes=scratch,
        compiler_params=pltpu.CompilerParams(vmem_limit_bytes=24 * 2**20),
        cost_estimate=pl.CostEstimate(flops=10**9, bytes_accessed=bytes_moved, transcendentals=0),
        name=name,
    )(*args)


def per_device(
    stream,
    norm_gain,
    w_value,
    w_mix,
    w_gate,
    w_state,
    conv_taps,
    skip_gain,
    decay_rate,
    turn_rate,
    input_real,
    input_imag,
    read_real,
    read_imag,
    initial_state,
    intervals,
    proj_conv,
    proj_state,
):
    n, share = stream.shape
    parts = lax.axis_size("tp")
    inner_axes = SP[1:]
    inside = lax.axis_size(inner_axes)
    planes = lax.axis_size(SP[0])
    channels = w_value.shape[1]
    width = decay_rate.size
    (blank,) = call(lead_kernel, [((8, channels), F32)], bytes_moved=3 * 10**8, name="lead")
    packed, notes = call(
        pack_kernel,
        [((parts, n + 8, share), BF16), ((8, channels), F32)],
        stream, norm_gain.reshape(1, -1), intervals.reshape(1, n), conv_taps, skip_gain.reshape(1, -1), blank,
        bytes_moved=3 * 10**8,
        name="pack",
    )
    rows = exchange(packed, "tp")

    states = ((n, width), F32)
    chunks = ((CHUNKS, width), F32)
    mixed = ((n, channels), F32)
    ur, ui, cr, ci, fr, fi, br, bi, source, gate, state, consts, message = call(
        local_kernel,
        [states, states, chunks, chunks, states, states, chunks, chunks, mixed, mixed, mixed]
        + [((40, channels), F32), ((inside, 24, 128), BF16)],
        rows, w_value, w_mix, w_gate, w_state, decay_rate, turn_rate,
        jnp.swapaxes(input_real, 2, 3).reshape(2 * channels, -1),
        jnp.swapaxes(input_imag, 2, 3).reshape(2 * channels, -1),
        initial_state, notes,
        scratch=[pltpu.VMEM((n, width), F32)] + [pltpu.VMEM((CHUNKS, width), F32)] * 2,
        name="local",
    )
    inner, message = call(
        plane_kernel,
        [((48, 128), F32), ((planes, 4, 384), BF16)],
        exchange(message, inner_axes), consts,
        name="plane",
    )
    got = exchange(message, SP[0])
    (partial,) = call(
        finish_kernel,
        [((parts, n, share), BF16)],
        got, inner, consts, ur, ui, cr, ci, fr, fi, br, bi,
        read_real.reshape(2 * channels, -1), read_imag.reshape(2 * channels, -1), source, gate, state,
        proj_conv, proj_state,
        name="finish",
    )
    arrived = exchange(partial, "tp")
    return arrived.astype(F32).sum(axis=0).astype(BF16)


def solution(mesh):
    finer = Mesh(mesh.devices.reshape(16, 4, 2, mesh.shape["tp"]), ("sp_0", "sp_1", "sp_2", "tp"))
    return jax.shard_map(
        per_device,
        mesh=finer,
        in_specs=(
            P(SP, "tp"),
            P("tp"),
            P(None, "tp"),
            P(None, "tp"),
            P(None, "tp"),
            P(None, "tp"),
            P(None, "tp"),
            P("tp"),
            P(None, "tp", None),
            P(None, "tp", None),
            P(None, "tp", None, None),
            P(None, "tp", None, None),
            P(None, "tp", None, None),
            P(None, "tp", None, None),
            P(None, None, "tp", None),
            P(SP),
            P("tp", None),
            P("tp", None),
        ),
        out_specs=P(SP, "tp"),
        check_vma=False,
    )
```
